256 devices in a mesh: sp: 32 (over z, x), tp: 8 (over y, core).
Axes of the slice: x: 4, y: 4, z: 8, core: 2. Of those that a mesh axis runs over, the one named last changes fastest.
Arguments:
- tokens: bfloat16 [2, 6144, 4096], P(None, 'sp', 'tp'), may hold values from -12 to 12
- query_weight: bfloat16 [4096, 2048], P(None, 'tp'), may hold values from -0.09375 to 0.09375
- key_weight: bfloat16 [4096, 2048], P(None, 'tp'), may hold values from -0.09375 to 0.09375
- value_weight: bfloat16 [4096, 2048], P(None, 'tp'), may hold values from -0.09375 to 0.09375
- gate_weight: bfloat16 [4096, 2048], P(None, 'tp'), may hold values from -0.09375 to 0.09375
- beta_weight: bfloat16 [4096, 16], P(None, 'tp'), may hold values from -0.09375 to 0.09375
- decay_weight: bfloat16 [4096, 16], P(None, 'tp'), may hold values from -0.09375 to 0.09375
- beta_bias: float32 [16], P('tp'), may hold values from -6 to -3
- rate_log: float32 [16], P('tp'), may hold values from -12 to -2.5
- out_gain: float32 [128], replicated, may hold values from 0.1 to 1.9
- new_query: bfloat16 [2, 16, 128], P(None, 'tp'), may hold values from -6 to 6
- new_key: bfloat16 [2, 16, 128], P(None, 'tp'), may hold values from -6 to 6
- new_value: bfloat16 [2, 16, 128], P(None, 'tp'), may hold values from -6 to 6
- new_beta: float32 [2, 16], P(None, 'tp'), may hold values from 0.1 to 0.9
- new_decay: float32 [2, 16], P(None, 'tp'), may hold values from 0.3 to 1
Outputs:
- mixed_out: bfloat16 [2, 6144, 2048], P(None, 'sp', 'tp')
- cache: bfloat16 [2, 16, 128, 128], P(None, 'tp', 'sp')
- first_out: float32 [2, 2048], P(None, 'tp')
The draws below stay inside these ranges and needn't reach their ends.
All inputs are finite; a program needn't handle non-finite values.
Results may differ from the reference program's by a relative error of at most 0.0073.
Values may be sent and summed in bfloat16 or wider, within the bound.
No kernel may reach another device: no remote copies, remote signals or barrier semaphores. Data moves between devices by JAX's collectives and lax.ppermute only.
A program may use at most 64 MiB of HBM per device.

```python
import jax
import jax.numpy as jnp
from jax import lax

D = 4096
HEADS = 16
HEAD = 128
BLOCK = 64
SEQS = 2
LEN = 6144


def draw_tokens(key, part):
    key_base, key_level, key_common = jax.random.split(key, 3)
    blocks = LEN // BLOCK
    base_draw = jax.random.truncated_normal(key_base, -4.0, 4.0, (SEQS, LEN, D), jnp.float32)
    level_log = jax.random.uniform(key_level, (SEQS, blocks, 1, 1), jnp.float32, -1.0, 1.0)
    common = jnp.zeros((1, 1, D), jnp.float32)
    row_scale = jnp.broadcast_to(jnp.exp(level_log), (SEQS, blocks, BLOCK, 1)).reshape(SEQS, LEN, 1)
    return ((base_draw + common) * row_scale).astype(jnp.bfloat16)


def draw_rate_log(key, part):
    key_slow, key_quick, key_pick = jax.random.split(key, 3)
    slow_rates = jnp.log(jax.random.uniform(key_slow, (HEADS,), jnp.float32, 0.2, 0.6) / LEN)
    quick_rates = jnp.log(jax.random.uniform(key_quick, (HEADS,), jnp.float32, 0.02, 0.06))
    slow_picks = jax.random.randint(key_pick, (HEADS,), 0, 2)
    return jnp.where(slow_picks == 1, slow_rates, quick_rates)


def block_scale(stream_key, shape, shards, low, largest):
    factor_of = 1.0
    for dim, shards_of in shards:
        heights = jax.random.uniform(jax.random.fold_in(jax.random.fold_in(stream_key, 6), dim), (shards_of,), jnp.float32, low / len(shards), largest / len(shards))
        factor_of = factor_of * jnp.repeat(jnp.exp(heights), shape[dim] // shards_of).reshape((-1,) + (1,) * (len(shape) - 1 - dim))
    return factor_of


def centred(key, shape, scale, reach, pieces=(), kind=jnp.bfloat16):
    array = scale * jax.random.normal(key, shape, jnp.float32)
    if pieces:
        array = array * block_scale(key, shape, pieces, -0.22, 0.18)
    return jnp.clip(array, -reach, reach).astype(kind)


def setup_inputs(seed: int = 0) -> dict:
    streams_of = jax.random.split(jax.random.key(seed), 16)
    return {
        "tokens": draw_tokens(jax.random.fold_in(streams_of[15], 71), 0),
        "query_weight": centred(streams_of[1], (D, HEADS * HEAD), D ** -0.5, 0.09375, ((1, 8),)),
        "key_weight": centred(streams_of[2], (D, HEADS * HEAD), D ** -0.5, 0.09375, ((1, 8),)),
        "value_weight": centred(streams_of[3], (D, HEADS * HEAD), D ** -0.5, 0.09375, ((1, 8),)),
        "gate_weight": centred(streams_of[4], (D, HEADS * HEAD), D ** -0.5, 0.09375, ((1, 8),)),
        "beta_weight": centred(streams_of[5], (D, HEADS), D ** -0.5, 0.09375, ((1, 8),)),
        "decay_weight": centred(streams_of[6], (D, HEADS), D ** -0.5, 0.09375, ((1, 8),)),
        "beta_bias": jnp.clip(-6.0 + 3.0 * jax.random.uniform(streams_of[7], (HEADS,), jnp.float32) ** block_scale(streams_of[7], (HEADS,), ((0, 8),), -0.2, 0.2), -6.0, -3.0),
        "rate_log": draw_rate_log(jax.random.fold_in(streams_of[15], 71), 0),
        "out_gain": jnp.clip(1.0 + 0.18 * jax.random.normal(streams_of[9], (HEAD,), jnp.float32), 0.1, 1.9),
        "new_query": centred(streams_of[10], (SEQS, HEADS, HEAD), 1.0, 6.0, ((1, 8),)),
        "new_key": centred(streams_of[11], (SEQS, HEADS, HEAD), 1.0, 6.0, ((1, 8),)),
        "new_value": centred(streams_of[12], (SEQS, HEADS, HEAD), 1.0, 6.0, ((1, 8),)),
        "new_beta": jnp.clip(0.1 + 0.79999997 * jax.random.uniform(streams_of[13], (SEQS, HEADS), jnp.float32) ** block_scale(streams_of[13], (SEQS, HEADS), ((1, 8),), -0.2, 0.2), 0.1, 0.9),
        "new_decay": jnp.clip(0.3 + 0.7 * jax.random.uniform(streams_of[14], (SEQS, HEADS), jnp.float32) ** block_scale(streams_of[14], (SEQS, HEADS), ((1, 8),), -0.2, 0.2), 0.3, 1.0),
    }


unit_floor = 1.0
norm_floor = 0.001
highest = lax.Precision.HIGHEST

def matmul(form, left, right):
    return jnp.einsum(form, left, right, precision=highest)

def unit_rows(values):
    return values * lax.rsqrt(lax.optimization_barrier(jnp.sum(values * values, axis=-1, keepdims=True)) + unit_floor)

def head_norm(values, out_gain):
    return values * lax.rsqrt(lax.optimization_barrier(jnp.mean(values * values, axis=-1, keepdims=True)) + norm_floor) * out_gain

def stored(values):
    return lax.optimization_barrier(values.astype(jnp.bfloat16)).astype(jnp.float32)

def unit_lower_inverse(lower_part):
    extent = lower_part.shape[-1]
    nilpotent = -lower_part
    inverse = jnp.eye(extent, dtype=jnp.float32) + nilpotent
    for _ in range(extent.bit_length() - 2):
        nilpotent = matmul('...ij,...jk->...ik', nilpotent, nilpotent)
        inverse = inverse + matmul('...ij,...jk->...ik', nilpotent, inverse)
    return inverse

def prepare(query_rows, key_rows, value_rows, beta_in, decay_in, beta_bias, rate_log, seq_count, length, head_count):
    extent = query_rows.shape[-1] // head_count
    blocks = length // BLOCK

    def by_head(values):
        shaped = values.reshape(seq_count, blocks, BLOCK, head_count, extent)
        return shaped.transpose(0, 3, 1, 2, 4).reshape(seq_count * head_count, blocks, BLOCK, extent)

    def by_scalar(values):
        shaped = values.reshape(seq_count, blocks, BLOCK, head_count)
        return shaped.transpose(0, 3, 1, 2).reshape(seq_count * head_count, blocks, BLOCK)
    queries = unit_rows(by_head(query_rows))
    key_unit = unit_rows(by_head(key_rows))
    values = by_head(value_rows)
    strength = by_scalar(jax.nn.sigmoid(beta_in + beta_bias))
    decays = by_scalar(-jnp.exp(rate_log) * jax.nn.softplus(decay_in))
    return (queries, key_unit, values, strength, decays)

def block_terms(queries, key_unit, values, strength, decays):
    extent = decays.shape[-1]
    cumulative = jnp.cumsum(decays, axis=-1)
    causal = jnp.tril(jnp.ones((extent, extent), bool))
    strict = jnp.tril(jnp.ones((extent, extent), bool), -1)
    spread = cumulative[..., :, None] - cumulative[..., None, :]
    weights = jnp.where(causal, jnp.exp(jnp.where(causal, spread, 0.0)), 0.0)
    key_beta = key_unit * strength[..., None]
    lower_part = jnp.where(strict, matmul('...td,...sd->...ts', key_beta, key_unit) * weights, 0.0)
    inverse = unit_lower_inverse(lower_part)
    update = matmul('...ts,...se->...te', inverse, values * strength[..., None])
    carry_w = matmul('...ts,...sd->...td', inverse, key_beta * jnp.exp(cumulative)[..., None])
    scores = matmul('...td,...sd->...ts', queries, key_unit) * weights
    query_decay = queries * jnp.exp(cumulative)[..., None]
    last_log = cumulative[..., -1]
    key_decay = key_unit * jnp.exp(last_log[..., None] - cumulative)[..., None]
    return (update, carry_w, query_decay, scores, key_decay, last_log)

def first_read(cache_whole, new_query, new_key, new_value, new_beta, new_decay, out_gain):
    seq_count, head_count, extent, _ = cache_whole.shape
    memory = lax.optimization_barrier(cache_whole).astype(jnp.float32)
    query_unit = unit_rows(new_query.astype(jnp.float32))
    key_unit = unit_rows(new_key.astype(jnp.float32))
    recall = matmul('shde,shd->she', memory, query_unit)
    retrieve = matmul('shde,shd->she', memory, key_unit)
    intersect = lax.optimization_barrier(jnp.sum(key_unit * query_unit, axis=-1))
    fresh_values = new_value.astype(jnp.float32) - new_decay[..., None] * retrieve
    read_heads = new_decay[..., None] * recall + (new_beta * intersect)[..., None] * fresh_values
    return head_norm(read_heads, out_gain).reshape(seq_count, head_count * extent)

def reference(tokens, query_weight, key_weight, value_weight, gate_weight, beta_weight, decay_weight, beta_bias, rate_log, out_gain, new_query, new_key, new_value, new_beta, new_decay):
    flat_rows = tokens.reshape(SEQS * LEN, D)

    def project(weight):
        return jnp.dot(flat_rows, weight, preferred_element_type=jnp.float32)
    query_rows = stored(project(query_weight))
    key_rows = stored(project(key_weight))
    value_rows = stored(project(value_weight))
    gate_rows = stored(project(gate_weight))
    beta_in = project(beta_weight)
    decay_in = project(decay_weight)
    prepared = prepare(query_rows, key_rows, value_rows, beta_in, decay_in, beta_bias, rate_log, SEQS, LEN, HEADS)
    block_data = block_terms(*prepared)

    def advance(state_now, inputs):
        update, carry_w, query_decay, scores, key_decay, last_log = inputs
        fresh_values = update - matmul('btd,bde->bte', carry_w, state_now)
        block_out = matmul('btd,bde->bte', query_decay, state_now) + matmul('bts,bse->bte', scores, fresh_values)
        state_next = state_now * jnp.exp(last_log)[:, None, None] + matmul('bsd,bse->bde', key_decay, fresh_values)
        return (state_next, block_out)
    inputs = tuple((jnp.moveaxis(member, 1, 0) for member in block_data))
    batch_size = SEQS * HEADS
    final_state, outputs = lax.scan(advance, jnp.zeros((batch_size, HEAD, HEAD), jnp.float32), inputs)
    heads_out = outputs.reshape(LEN // BLOCK, SEQS, HEADS, BLOCK, HEAD).transpose(1, 0, 3, 2, 4)
    heads_out = heads_out.reshape(SEQS, LEN, HEADS, HEAD)
    gate_values = gate_rows.reshape(SEQS, LEN, HEADS, HEAD)
    mixed_out = (head_norm(heads_out, out_gain) * jax.nn.silu(gate_values)).astype(jnp.bfloat16)
    mixed_out = mixed_out.reshape(SEQS, LEN, HEADS * HEAD)
    cache = final_state.reshape(SEQS, HEADS, HEAD, HEAD).astype(jnp.bfloat16)
    first_out = first_read(cache, new_query, new_key, new_value, new_beta, new_decay, out_gain)
    return (mixed_out, cache, first_out)
```

```python
import functools

import jax
import jax.numpy as jnp
from jax import lax
from jax.experimental import pallas as pl
from jax.experimental.pallas import tpu as pltpu
from jax.sharding import Mesh
from jax.sharding import PartitionSpec as P

NEAR = ("zl", "x")
AXES = ("zh", "zl", "x")
PACK = 16
unit_floor = 1.0
norm_floor = 0.001
bf16 = jnp.bfloat16
f32 = jnp.float32


def dot(left, right, dims=((1,), (0,))):
    return lax.dot_general(
        left.astype(bf16), right.astype(bf16), (dims, ((), ())), preferred_element_type=f32
    )


ROWS = ((1,), (1,))
COLS = ((0,), (0,))


def thirds(value):
    high = value.astype(bf16).astype(f32)
    rest = value - high
    mid = rest.astype(bf16).astype(f32)
    return high, mid, rest - mid


def iota(shape, dim):
    return lax.broadcasted_iota(jnp.int32, shape, dim)


def row_pack(values, width):
    rows = iota((PACK, width), 0)
    packed = jnp.zeros((PACK, width), f32)
    for at, value in enumerate(values):
        packed = jnp.where(rows == at, value, packed)
    return packed


def rms_scale(values, floor, mean):
    total = jnp.sum(values * values, axis=-1, keepdims=True)
    return lax.rsqrt((total / values.shape[-1] if mean else total) + floor)


def token_copies(pieces, buffer, sems):
    own, own_c, *rest = pieces
    copies = [
        [pltpu.make_async_copy(ref.at[seq], buffer.at[slot, seq], sems.at[slot]) for seq in range(2)]
        for slot, ref in enumerate((own, own_c))
    ]
    for pair in range(6):
        first, second = rest[2 * pair : 2 * pair + 2]
        slot = 2 + pair
        copies.append(
            [
                pltpu.make_async_copy(first, buffer.at[slot, 0], sems.at[slot]),
                pltpu.make_async_copy(second, buffer.at[slot, 1], sems.at[slot]),
            ]
        )
    return copies


def project_pieces(shard_of, pieces, weights, token_buffer, weight_buffers, sems, each):
    depth = token_buffer.shape[-1]
    copies = token_copies(pieces, token_buffer, sems)
    for slot in range(8):
        start = pl.multiple_of(shard_of[slot] * depth, depth)
        for weight, buffer in zip(weights, weight_buffers):
            copies[slot].append(
                pltpu.make_async_copy(
                    weight.at[pl.ds(start, depth), :], buffer.at[slot], sems.at[slot]
                )
            )
        for copy in copies[slot]:
            copy.start()
    totals = [None] * len(weights)
    for slot in range(8):
        for copy in copies[slot]:
            copy.wait()
        rows = token_buffer[slot].reshape(-1, depth)
        for at, buffer in enumerate(weight_buffers):
            part = dot(rows, buffer[slot])
            totals[at] = part if totals[at] is None else totals[at] + part
    return totals


def local_kernel(shard_of, *refs):
    pieces, refs = refs[:14], refs[14:]
    key_w, value_w, gate_w, bias_ref, rate_ref = refs[:5]
    send_ref, key_ref, fresh_ref, carry_ref, cols_ref, rows_ref = refs[5:11]
    token_buffer, key_buffer, value_buffer, gate_buffer, sems = refs[11:]
    span = token_buffer.shape[2]
    head = send_ref.shape[-1]
    key_total, value_total, gates = project_pieces(
        shard_of,
        pieces,
        (key_w, value_w, gate_w),
        token_buffer,
        (key_buffer, value_buffer, gate_buffer),
        sems,
        None,
    )
    key_rows = key_total.astype(bf16)
    value_rows = value_total.astype(bf16)
    key_ref[...] = key_rows
    strength = jax.nn.sigmoid(gates + bias_ref[...])
    decays = -jnp.exp(rate_ref[...]) * jax.nn.softplus(gates)
    wide = cols_ref.shape[1]
    pairs = []
    lanes = iota((wide, head), 1)
    causal_wide = (iota((wide, wide), 0) >= iota((wide, wide), 1)).astype(bf16)
    for seq in range(2):
        take = slice(seq * span, (seq + 1) * span)
        padded = jnp.concatenate([decays[take], jnp.zeros((wide - span, head), f32)], axis=0)
        cumulative = sum(dot(causal_wide, part) for part in thirds(padded))
        table = jnp.where((lanes == 2) | (lanes == 3), cumulative, 0.0)
        for h in range(2):
            keys = key_rows[take, h * head : (h + 1) * head].astype(f32)
            unit = jnp.concatenate(
                [rms_scale(keys, unit_floor, False), jnp.zeros((wide - span, 1), f32)], axis=0
            )
            beta = jnp.concatenate(
                [strength[take, h : h + 1], jnp.zeros((wide - span, 1), f32)], axis=0
            )
            table = jnp.where(lanes == h, beta, table)
            table = jnp.where(lanes == 4 + h, unit, table)
        cols_ref[seq] = table
        rows_ref[seq] = table.T
    t = iota((span, span), 0)
    s = iota((span, span), 1)
    lower, inverse = [], []
    for pair in range(4):
        seq, h = divmod(pair, 2)
        keys = key_rows[seq * span : (seq + 1) * span, h * head : (h + 1) * head]
        col = lambda at: cols_ref[seq, :span, at + h : at + h + 1]
        row = lambda at: rows_ref[seq, at + h : at + h + 1, :span]
        spread = jnp.where(t >= s, col(2) - row(2), 0.0)
        alike = dot(keys, keys, ROWS) * (col(0) * col(4)) * row(4) * jnp.exp(spread)
        lower.append(jnp.where(t > s, alike, 0.0))
        inverse.append(jnp.where(t // 2 == s // 2, lower[pair], 0.0))
    size = 2
    while size < span:
        mask = (t // (2 * size) == s // (2 * size)) & (t // size != s // size)
        steps = []
        for pair in range(4):
            block = jnp.where(mask, lower[pair], 0.0)
            steps.append(block - dot(block, inverse[pair]))
        for pair in range(4):
            inverse[pair] = inverse[pair] + steps[pair] - dot(inverse[pair], steps[pair])
        size *= 2
    for pair in range(4):
        seq, h = divmod(pair, 2)
        take = slice(seq * span, (seq + 1) * span)
        keys = key_rows[take, h * head : (h + 1) * head]
        values = value_rows[take, h * head : (h + 1) * head]
        col = lambda at: cols_ref[seq, :span, at + h : at + h + 1]
        row = lambda at: rows_ref[seq, at + h : at + h + 1, :span]
        fresh = col(0) * values.astype(f32) - dot(inverse[pair] * row(0), values)
        carry = (col(0) * col(4) * jnp.exp(col(2))) * keys.astype(f32) - dot(
            inverse[pair] * (row(0) * row(4) * jnp.exp(row(2))), keys
        )
        last = cols_ref[seq, span - 1 : span, 2 + h : 3 + h]
        late = col(4) * jnp.exp(last - col(2))
        reach = dot(carry * late, keys, COLS)
        gain = dot(fresh * late, keys, COLS)
        fresh_ref[pair] = fresh.astype(bf16)
        carry_ref[pair] = carry.astype(bf16)
        factor = row_pack(thirds(jnp.broadcast_to(jnp.exp(last), (1, head))), head)
        half = head // 2
        for side in range(2):
            to = 2 * pair + side
            send_ref[to, :head, :] = reach.astype(bf16)
            send_ref[to, head : head + half, :] = gain[side * half : (side + 1) * half].astype(bf16)
            send_ref[to, head + half :, :] = factor.astype(bf16)


def window_kernel(shard_of, *refs):
    pieces, refs = refs[:14], refs[14:]
    query_w, gate_w, gain_ref, key_ref, fresh_ref, carry_ref, cols_ref, rows_ref = refs[:8]
    out_ref, reach_ref, silu_ref = refs[8:11]
    token_buffer, query_buffer, gate_buffer, sems = refs[11:]
    span = token_buffer.shape[2]
    head = fresh_ref.shape[-1]
    query_total, gate_total = project_pieces(
        shard_of, pieces, (query_w, gate_w), token_buffer, (query_buffer, gate_buffer), sems, None
    )
    query_rows = query_total.astype(bf16)
    gate_rows = gate_total.astype(bf16).astype(f32)
    t = iota((span, span), 0)
    s = iota((span, span), 1)
    for pair in range(4):
        seq, h = divmod(pair, 2)
        take = slice(seq * span, (seq + 1) * span)
        part = slice(h * head, (h + 1) * head)
        col = lambda at: cols_ref[seq, :span, at + h : at + h + 1]
        row = lambda at: rows_ref[seq, at + h : at + h + 1, :span]
        queries = query_rows[take, part]
        unit = rms_scale(queries.astype(f32), unit_floor, False)
        spread = jnp.where(t >= s, col(2) - row(2), 0.0)
        scores = dot(queries, key_ref[take, part], ROWS) * unit * row(4) * jnp.exp(spread)
        scores = jnp.where(t >= s, scores, 0.0).astype(bf16)
        out_ref[pair] = dot(scores, fresh_ref[pair])
        reach = (unit * jnp.exp(col(2))) * queries.astype(f32) - dot(scores, carry_ref[pair])
        reach_ref[pair] = reach.astype(bf16)
        gate = gate_rows[take, part]
        silu_ref[pair] = gain_ref[...] * gate * jax.nn.sigmoid(gate)


def unpack_factor(block):
    block = block.astype(f32)
    return block[0:1] + block[1:2] + block[2:3]


def compose_kernel(in_ref, total_ref, maps_ref, adds_ref, factors_ref):
    count, rows, head = in_ref.shape
    body = rows - PACK

    def load(at):
        return in_ref[at, :body, :].astype(f32), unpack_factor(in_ref[at, body:, :])

    def join(first, second):
        both, factor = first
        later, later_factor = second
        tail = jnp.concatenate([factor * later[:head], later[head:]], axis=0)
        return later_factor * both - dot(both, later[:head]) + tail, factor * later_factor

    member = [load(at) for at in range(count)]
    upto = [None] * (count + 1)
    upto[1] = member[0]
    c23, c45, c67 = (join(member[at], member[at + 1]) for at in (2, 4, 6))
    upto[2] = join(member[0], member[1])
    c456 = join(c45, member[6])
    c4567 = join(c45, c67)
    upto[4] = join(upto[2], c23)
    upto[8] = join(upto[4], c4567)
    both, factor = upto[8]
    total_ref[:body, :] = both.astype(bf16)
    total_ref[body:, :] = row_pack(thirds(factor), head).astype(bf16)
    upto[3] = join(upto[2], member[2])
    upto[5] = join(upto[4], member[4])
    upto[6] = join(upto[4], c45)
    upto[7] = join(upto[4], c456)
    for at in range(1, count):
        both, factor = upto[at]
        maps_ref[at - 1] = both[:head].astype(bf16)
        adds_ref[at - 1] = both[head:]
        factors_ref[at - 1] = jnp.broadcast_to(factor, (8, head))


def spread_kernel(
    place, beta_ref, decay_ref, own, back1, back2, back3, maps_ref, adds_ref, factors_ref,
    query_ref, key_ref, value_ref, send_ref, groups_ref, wide_ref, turned_ref,
):
    rows, head = own.shape
    half = head // 2
    far, near = place[0], place[1]
    pair = near // 2
    side = near % 2
    for slot, ref in enumerate((own, back1, back2, back3)):
        groups_ref[slot] = ref[...]
    state = jnp.zeros((half, head), f32)
    begin = state
    for group in range(4):
        begin = jnp.where(far == group, state, begin)
        block = groups_ref[lax.rem(far - group + 4, 4)]
        added = block[head : head + half].astype(f32)
        if group:
            state = unpack_factor(block[head + half :]) * state - dot(state, block[:head]) + added
        else:
            state = added
    final = state.astype(bf16).astype(f32)
    wide_ref[...] = jnp.zeros((head, head), f32)
    wide_ref[pl.ds(pl.multiple_of(side * half, half), half), :] = final
    padded = wide_ref[...]
    turned_ref[...] = padded.T
    mine = turned_ref[pl.ds(pl.multiple_of(far * 32, 32), 32), :]
    query = query_ref[pl.ds(pair, 1), :]
    key = key_ref[pl.ds(pair, 1), :]
    query = query * rms_scale(query, unit_floor, False)
    key = key * rms_scale(key, unit_floor, False)
    hits = dot(row_pack(thirds(query) + thirds(key), head), padded, ROWS)
    recall = hits[0:1] + hits[1:2] + hits[2:3]
    retrieve = hits[3:4] + hits[4:5] + hits[5:6]
    intersect = jnp.sum(key * query, axis=-1, keepdims=True)
    fresh = value_ref[pl.ds(pair, 1), :] - decay_ref[pair] * retrieve
    read = decay_ref[pair] * recall + (beta_ref[pair] * intersect) * fresh
    read = jnp.where(iota((1, head), 1) // half == side, read, 0.0)
    zero = jnp.zeros((1, head), f32)
    extra = row_pack((zero, zero, zero, zero) + thirds(read), head)
    pick_row = iota((PACK, 32), 0)
    pick_col = iota((PACK, 32), 1)
    for member in range(8):
        if member:
            at = member - 1
            entry = factors_ref[at, 0:1, :] * begin - dot(begin, maps_ref[at]) + adds_ref[at]
        else:
            entry = begin
        send_ref[member, :half, :] = entry.astype(bf16)
        pick = ((pick_row < 4) & (pick_col == 4 * member + pick_row)).astype(bf16)
        send_ref[member, half:, :] = (dot(pick, mine) + extra).astype(bf16)


def finish_kernel(in_ref, out_ref, reach_ref, silu_ref, gain_ref, mixed_ref, cache_ref, read_ref):
    head = in_ref.shape[-1]
    half = head // 2
    for pair in range(4):
        seq, h = divmod(pair, 2)
        incoming = jnp.concatenate([in_ref[2 * pair, :half, :], in_ref[2 * pair + 1, :half, :]], 0)
        whole = out_ref[pair] + dot(reach_ref[pair], incoming, ROWS)
        mixed = whole * rms_scale(whole, norm_floor, True) * silu_ref[pair]
        mixed_ref[seq, :, h * head : (h + 1) * head] = mixed.astype(bf16)
        extra = in_ref[2 * pair, half:, :].astype(f32) + in_ref[2 * pair + 1, half:, :].astype(f32)
        cache_ref[seq, h] = extra[:4].astype(bf16)
        read = extra[4:5] + extra[5:6] + extra[6:7]
        read = read * rms_scale(read, norm_floor, True) * gain_ref[...]
        read_ref[seq : seq + 1, h * head : (h + 1) * head] = read


def vmem():
    return pl.BlockSpec(memory_space=pltpu.VMEM)


def smem():
    return pl.BlockSpec(memory_space=pltpu.SMEM)


def anywhere():
    return pl.BlockSpec(memory_space=pl.ANY)


def shape(dims, dtype):
    return jax.ShapeDtypeStruct(dims, dtype)


def shift(value, axis, by):
    length = lax.axis_size(axis)
    return lax.ppermute(value, axis, [(at, (at + by) % length) for at in range(length)])


def shards(
    tokens, query_weight, key_weight, value_weight, gate_weight, beta_weight, decay_weight,
    beta_bias, rate_log, out_gain, new_query, new_key, new_value, new_beta, new_decay,
):
    _, span, depth = tokens.shape
    head = out_gain.shape[0]
    half = head // 2
    wide = 256
    width = query_weight.shape[1]
    y, core = lax.axis_index("y"), lax.axis_index("c")
    first, second = tokens[0], tokens[1]
    up0 = shift(first, "y", 1)
    down1 = shift(second, "y", -1)
    up1 = shift(second, "y", 1)
    down0 = shift(first, "y", -1)
    far0 = shift(up0, "y", 1)
    far1 = shift(down1, "y", -1)
    swap = lambda value: shift(value, "c", 1)
    pieces = [tokens, swap(tokens), up0, up1, down0, down1, far0, far1]
    pieces += [swap(value) for value in (up0, up1, down0, down1, far0, far1)]
    ahead = [y, y, y + 3, y + 1, y + 2, y + 3, y + 1, y + 2]
    cores = [core, 1 - core, core, core, core, 1 - core, 1 - core, 1 - core]
    shard_of = jnp.stack([(a % 4) * 2 + c for a, c in zip(ahead, cores)]).astype(jnp.int32)
    scalars = jnp.concatenate([beta_weight, decay_weight], axis=1)
    scalars = jnp.pad(scalars, ((0, 0), (0, head - scalars.shape[1])))
    bias = jnp.pad(beta_bias, (0, head - 2))[None]
    rate = jnp.pad(rate_log, (2, head - 4))[None]
    gain = out_gain[None]

    buffers = lambda widths: [pltpu.VMEM((8, 2, span, depth), bf16)] + [
        pltpu.VMEM((8, depth, w), bf16) for w in widths
    ] + [pltpu.SemaphoreType.DMA((8,))]
    rows = head + half + PACK
    send, key_rows, fresh, carry, cols, turned = pl.pallas_call(
        local_kernel,
        name="local_terms",
        out_shape=(
            shape((8, rows, head), bf16),
            shape((2 * span, width), bf16),
            shape((4, span, head), bf16),
            shape((4, span, head), bf16),
            shape((2, wide, head), f32),
            shape((2, head, wide), f32),
        ),
        in_specs=[smem()] + [anywhere()] * 17 + [vmem()] * 2,
        out_specs=tuple(vmem() for _ in range(6)),
        scratch_shapes=buffers((width, width, head)),
    )(shard_of, *pieces, key_weight, value_weight, scalars, bias, rate)

    arrived = lax.all_to_all(send, NEAR, 0, 0, tiled=True)

    local_out, reach, silu = pl.pallas_call(
        window_kernel,
        name="window_terms",
        out_shape=(
            shape((4, span, head), f32),
            shape((4, span, head), bf16),
            shape((4, span, head), f32),
        ),
        in_specs=[smem()] + [anywhere()] * 16 + [vmem()] * 6,
        out_specs=tuple(vmem() for _ in range(3)),
        scratch_shapes=buffers((width, width)),
    )(shard_of, *pieces, query_weight, gate_weight, gain, key_rows, fresh, carry, cols, turned)

    total, maps, adds, factors = pl.pallas_call(
        compose_kernel,
        name="compose_near",
        out_shape=(
            shape((rows, head), bf16),
            shape((7, head, head), bf16),
            shape((7, half, head), f32),
            shape((7, 8, head), f32),
        ),
        in_specs=[vmem()],
        out_specs=tuple(vmem() for _ in range(4)),
    )(arrived)

    others = [shift(total, "zh", by) for by in (1, 2, 3)]
    place = jnp.stack([lax.axis_index("zh"), lax.axis_index(NEAR)]).astype(jnp.int32)
    flat = lambda value: value.reshape(4, -1).astype(f32)
    back = pl.pallas_call(
        spread_kernel,
        name="spread_states",
        out_shape=shape((8, half + PACK, head), bf16),
        in_specs=[smem()] * 3 + [vmem()] * 10,
        out_specs=vmem(),
        scratch_shapes=[
            pltpu.VMEM((4, rows, head), bf16),
            pltpu.VMEM((head, head), f32),
            pltpu.VMEM((head, head), f32),
        ],
    )(
        place, new_beta.reshape(4), new_decay.reshape(4), total, *others, maps, adds, factors,
        flat(new_query), flat(new_key), flat(new_value),
    )
    returned = lax.all_to_all(back, NEAR, 0, 0, tiled=True)
    return pl.pallas_call(
        finish_kernel,
        name="finish",
        out_shape=(
            shape((2, span, width), bf16),
            shape((2, 2, 4, head), bf16),
            shape((2, width), f32),
        ),
        in_specs=[vmem()] * 5,
        out_specs=tuple(vmem() for _ in range(3)),
    )(returned, local_out, reach, silu, gain)


def solution(mesh):
    torus = Mesh(mesh.devices.reshape(4, 2, 4, 4, 2), AXES + ("y", "c"))
    sp, tp = AXES, ("y", "c")
    weight = P(None, tp)
    in_specs = (
        P(None, sp, tp),
        weight, weight, weight, weight, weight, weight,
        P(tp), P(tp), P(),
        P(None, tp, None), P(None, tp, None), P(None, tp, None),
        P(None, tp), P(None, tp),
    )
    out_specs = (P(None, sp, tp), P(None, tp, sp, None), P(None, tp))
    return jax.shard_map(
        shards, mesh=torus, in_specs=in_specs, out_specs=out_specs, check_vma=False
    )
```

```python
import jax
import jax.numpy as jnp
from jax import lax
from jax.experimental import pallas as pl
from jax.experimental.pallas import tpu as pltpu
from jax.sharding import Mesh
from jax.sharding import PartitionSpec as P

NEAR = ("zl", "x")
AXES = ("zh", "zl", "x")
PACK = 16
LANES = 128
unit_floor = 1.0
norm_floor = 0.001
bf16 = jnp.bfloat16
f32 = jnp.float32


def dot(left, right, dims=((1,), (0,))):
    return lax.dot_general(
        left.astype(bf16), right.astype(bf16), (dims, ((), ())), preferred_element_type=f32
    )


ROWS = ((1,), (1,))
COLS = ((0,), (0,))


def thirds(value):
    high = value.astype(bf16).astype(f32)
    rest = value - high
    mid = rest.astype(bf16).astype(f32)
    return high, mid, rest - mid


def iota(shape, dim):
    return lax.broadcasted_iota(jnp.int32, shape, dim)


def row_pack(values, width):
    rows = iota((PACK, width), 0)
    packed = jnp.zeros((PACK, width), f32)
    for at, value in enumerate(values):
        packed = jnp.where(rows == at, value, packed)
    return packed


def rms_scale(values, floor, mean):
    total = jnp.sum(values * values, axis=-1, keepdims=True)
    return lax.rsqrt((total / values.shape[-1] if mean else total) + floor)


def shard_index(ahead, swapped):
    core = lax.axis_index("c")
    core = 1 - core if swapped else core
    return lax.rem(lax.axis_index("y") + ahead, 4) * 2 + core


def project_pieces(pieces, slots, weights):
    totals = [None] * len(weights)
    for piece, slot in zip(pieces, slots):
        rows = piece() if callable(piece) else piece[...]
        depth = rows.shape[-1]
        rows = rows.reshape(-1, depth)
        start = pl.multiple_of(shard_index(*slot) * depth, depth)
        for at, weight in enumerate(weights):
            part = weight(rows, start) if callable(weight) else dot(rows, weight[pl.ds(start, depth), :])
            totals[at] = part if totals[at] is None else totals[at] + part
    return totals


def joined(first, second):
    return lambda: jnp.concatenate([first[...], second[...]], axis=0)


def scalar_gates(beta_w, decay_w):
    def project(rows, start):
        depth = rows.shape[-1]
        beta = beta_w[:, pl.ds(start, depth)].astype(f32)
        decay = decay_w[:, pl.ds(start, depth)].astype(f32)
        stacked = row_pack((beta[0:1], beta[1:2], decay[0:1], decay[1:2]), depth)
        stacked = jnp.concatenate([stacked, jnp.zeros((LANES - PACK, depth), f32)], axis=0)
        return dot(rows, stacked, ROWS)

    return project


NEAR_SLOTS = ((0, False), (0, True))
NEXT_SLOTS = ((3, False), (1, False))
LATE_SLOTS = ((3, True), (1, True), (2, False), (2, True))


def early_kernel(own, own_c, key_w, value_w, beta_w, decay_w, key_out, value_out, gate_out):
    weights = (key_w, value_w, scalar_gates(beta_w, decay_w))
    totals = project_pieces((own, own_c), NEAR_SLOTS, weights)
    for ref, total in zip((key_out, value_out, gate_out), totals):
        ref[...] = total


def next_kernel(
    up0, up1, down0, down1, key_w, value_w, beta_w, decay_w, key_in, value_in, gate_in,
    key_out, value_out, gate_out,
):
    weights = (key_w, value_w, scalar_gates(beta_w, decay_w))
    totals = project_pieces((joined(up0, up1), joined(down0, down1)), NEXT_SLOTS, weights)
    before = (key_in, value_in, gate_in)
    for ref, total, old in zip((key_out, value_out, gate_out), totals, before):
        ref[...] = old[...] + total


def lane_pair(ref, first):
    lanes = iota((1, LANES), 1)
    return jnp.where(lanes == first, ref[0], jnp.where(lanes == first + 1, ref[1], 0.0))


def local_kernel(bias_ref, rate_ref, *refs):
    pieces, refs = refs[:8], refs[8:]
    key_w, value_w, beta_w, decay_w, key_in, value_in, gate_in = refs[:7]
    send_ref, key_ref, fresh_ref, carry_ref, cols_ref, rows_ref = refs[7:]
    span = pieces[0].shape[0]
    head = send_ref.shape[-1]
    late = [joined(*pieces[at : at + 2]) for at in range(0, 8, 2)]
    totals = project_pieces(late, LATE_SLOTS, (key_w, value_w, scalar_gates(beta_w, decay_w)))
    key_rows = (key_in[...] + totals[0]).astype(bf16)
    value_rows = (value_in[...] + totals[1]).astype(bf16)
    gates = gate_in[...] + totals[2]
    key_ref[...] = key_rows
    strength = jax.nn.sigmoid(gates + lane_pair(bias_ref, 0))
    decays = -jnp.exp(lane_pair(rate_ref, 2)) * jax.nn.softplus(gates)
    wide = cols_ref.shape[1]
    pairs = []
    lanes = iota((wide, head), 1)
    causal_wide = (iota((wide, wide), 0) >= iota((wide, wide), 1)).astype(bf16)
    for seq in range(2):
        take = slice(seq * span, (seq + 1) * span)
        padded = jnp.concatenate([decays[take], jnp.zeros((wide - span, head), f32)], axis=0)
        cumulative = sum(dot(causal_wide, part) for part in thirds(padded))
        table = jnp.where((lanes == 2) | (lanes == 3), cumulative, 0.0)
        for h in range(2):
            keys = key_rows[take, h * head : (h + 1) * head].astype(f32)
            unit = jnp.concatenate(
                [rms_scale(keys, unit_floor, False), jnp.zeros((wide - span, 1), f32)], axis=0
            )
            beta = jnp.concatenate(
                [strength[take, h : h + 1], jnp.zeros((wide - span, 1), f32)], axis=0
            )
            table = jnp.where(lanes == h, beta, table)
            table = jnp.where(lanes == 4 + h, unit, table)
        cols_ref[seq] = table
        rows_ref[seq] = table.T
    t = iota((span, span), 0)
    s = iota((span, span), 1)
    lower, inverse = [], []
    for pair in range(4):
        seq, h = divmod(pair, 2)
        keys = key_rows[seq * span : (seq + 1) * span, h * head : (h + 1) * head]
        col = lambda at: cols_ref[seq, :span, at + h : at + h + 1]
        row = lambda at: rows_ref[seq, at + h : at + h + 1, :span]
        spread = jnp.where(t >= s, col(2) - row(2), 0.0)
        alike = dot(keys, keys, ROWS) * (col(0) * col(4)) * row(4) * jnp.exp(spread)
        lower.append(jnp.where(t > s, alike, 0.0))
        inverse.append(jnp.where(t // 2 == s // 2, lower[pair], 0.0))
    size = 2
    while size < span:
        mask = (t // (2 * size) == s // (2 * size)) & (t // size != s // size)
        steps = []
        for pair in range(4):
            block = jnp.where(mask, lower[pair], 0.0)
            steps.append(block - dot(block, inverse[pair]))
        for pair in range(4):
            inverse[pair] = inverse[pair] + steps[pair] - dot(inverse[pair], steps[pair])
        size *= 2
    for pair in range(4):
        seq, h = divmod(pair, 2)
        take = slice(seq * span, (seq + 1) * span)
        keys = key_rows[take, h * head : (h + 1) * head]
        values = value_rows[take, h * head : (h + 1) * head]
        col = lambda at: cols_ref[seq, :span, at + h : at + h + 1]
        row = lambda at: rows_ref[seq, at + h : at + h + 1, :span]
        fresh = col(0) * values.astype(f32) - dot(inverse[pair] * row(0), values)
        carry = (col(0) * col(4) * jnp.exp(col(2))) * keys.astype(f32) - dot(
            inverse[pair] * (row(0) * row(4) * jnp.exp(row(2))), keys
        )
        last = cols_ref[seq, span - 1 : span, 2 + h : 3 + h]
        late = col(4) * jnp.exp(last - col(2))
        reach = dot(carry * late, keys, COLS)
        gain = dot(fresh * late, keys, COLS)
        fresh_ref[pair] = fresh.astype(bf16)
        carry_ref[pair] = carry.astype(bf16)
        factor = row_pack(thirds(jnp.broadcast_to(jnp.exp(last), (1, head))), head)
        half = head // 2
        for side in range(2):
            to = 2 * pair + side
            send_ref[to, :head, :] = reach.astype(bf16)
            send_ref[to, head : head + half, :] = gain[side * half : (side + 1) * half].astype(bf16)
            send_ref[to, head + half :, :] = factor.astype(bf16)


def window_kernel(*refs):
    own, own_c, up0, up1, down0, down1 = refs[:6]
    late, refs = refs[6:14], refs[14:]
    query_w, gate_w, gain_ref, key_ref, fresh_ref, carry_ref, cols_ref, rows_ref = refs[:8]
    out_ref, reach_ref, silu_ref = refs[8:]
    span = up0.shape[0]
    head = fresh_ref.shape[-1]
    pieces = [own, own_c, joined(up0, up1), joined(down0, down1)]
    pieces += [joined(*late[at : at + 2]) for at in range(0, 8, 2)]
    slots = NEAR_SLOTS + NEXT_SLOTS + LATE_SLOTS
    query_total, gate_total = project_pieces(pieces, slots, (query_w, gate_w))
    query_rows = query_total.astype(bf16)
    gate_rows = gate_total.astype(bf16).astype(f32)
    t = iota((span, span), 0)
    s = iota((span, span), 1)
    for pair in range(4):
        seq, h = divmod(pair, 2)
        take = slice(seq * span, (seq + 1) * span)
        part = slice(h * head, (h + 1) * head)
        col = lambda at: cols_ref[seq, :span, at + h : at + h + 1]
        row = lambda at: rows_ref[seq, at + h : at + h + 1, :span]
        queries = query_rows[take, part]
        unit = rms_scale(queries.astype(f32), unit_floor, False)
        spread = jnp.where(t >= s, col(2) - row(2), 0.0)
        scores = dot(queries, key_ref[take, part], ROWS) * unit * row(4) * jnp.exp(spread)
        scores = jnp.where(t >= s, scores, 0.0).astype(bf16)
        out_ref[pair] = dot(scores, fresh_ref[pair])
        reach = (unit * jnp.exp(col(2))) * queries.astype(f32) - dot(scores, carry_ref[pair])
        reach_ref[pair] = reach.astype(bf16)
        gate = gate_rows[take, part]
        silu_ref[pair] = gain_ref[...] * gate * jax.nn.sigmoid(gate)


def unpack_factor(block):
    block = block.astype(f32)
    return block[0:1] + block[1:2] + block[2:3]


def compose_kernel(in_ref, total_ref, maps_ref, adds_ref, factors_ref):
    count, rows, head = in_ref.shape
    body = rows - PACK

    def load(at):
        return in_ref[at, :body, :].astype(f32), unpack_factor(in_ref[at, body:, :])

    def join(first, second):
        both, factor = first
        later, later_factor = second
        tail = jnp.concatenate([factor * later[:head], later[head:]], axis=0)
        return later_factor * both - dot(both, later[:head]) + tail, factor * later_factor

    member = [load(at) for at in range(count)]
    upto = [None] * (count + 1)
    upto[1] = member[0]
    c23, c45, c67 = (join(member[at], member[at + 1]) for at in (2, 4, 6))
    upto[2] = join(member[0], member[1])
    c456 = join(c45, member[6])
    c4567 = join(c45, c67)
    upto[4] = join(upto[2], c23)
    upto[8] = join(upto[4], c4567)
    both, factor = upto[8]
    total_ref[:body, :] = both.astype(bf16)
    total_ref[body:, :] = row_pack(thirds(factor), head).astype(bf16)
    upto[3] = join(upto[2], member[2])
    upto[5] = join(upto[4], member[4])
    upto[6] = join(upto[4], c45)
    upto[7] = join(upto[4], c456)
    for at in range(1, count):
        both, factor = upto[at]
        maps_ref[at - 1] = both[:head].astype(bf16)
        adds_ref[at - 1] = both[head:]
        factors_ref[at - 1] = jnp.broadcast_to(factor, (8, head))


def spread_kernel(
    beta_ref, decay_ref, own, back1, back2, back3, maps_ref, adds_ref, factors_ref,
    query_ref, key_ref, value_ref, send_ref, groups_ref, wide_ref, turned_ref,
):
    rows, head = own.shape
    half = head // 2
    far = lax.axis_index("zh")
    near = lax.axis_index("zl") * 4 + lax.axis_index("x")
    pair = near // 2
    side = near % 2
    seq, h = pair // 2, pair % 2

    def chosen(ref):
        total = jnp.zeros((1, head), f32)
        for at in range(4):
            row = ref[at // 2, at % 2 : at % 2 + 1, :].astype(f32)
            total = jnp.where(pair == at, row, total)
        return total

    for slot, ref in enumerate((own, back1, back2, back3)):
        groups_ref[slot] = ref[...]
    state = jnp.zeros((half, head), f32)
    begin = state
    for group in range(4):
        begin = jnp.where(far == group, state, begin)
        block = groups_ref[lax.rem(far - group + 4, 4)]
        added = block[head : head + half].astype(f32)
        if group:
            state = unpack_factor(block[head + half :]) * state - dot(state, block[:head]) + added
        else:
            state = added
    final = state.astype(bf16).astype(f32)
    wide_ref[...] = jnp.zeros((head, head), f32)
    wide_ref[pl.ds(pl.multiple_of(side * half, half), half), :] = final
    padded = wide_ref[...]
    turned_ref[...] = padded.T
    mine = turned_ref[pl.ds(pl.multiple_of(far * 32, 32), 32), :]
    query = chosen(query_ref)
    key = chosen(key_ref)
    query = query * rms_scale(query, unit_floor, False)
    key = key * rms_scale(key, unit_floor, False)
    hits = dot(row_pack(thirds(query) + thirds(key), head), padded, ROWS)
    recall = hits[0:1] + hits[1:2] + hits[2:3]
    retrieve = hits[3:4] + hits[4:5] + hits[5:6]
    intersect = jnp.sum(key * query, axis=-1, keepdims=True)
    fresh = chosen(value_ref) - decay_ref[seq, h] * retrieve
    read = decay_ref[seq, h] * recall + (beta_ref[seq, h] * intersect) * fresh
    read = jnp.where(iota((1, head), 1) // half == side, read, 0.0)
    zero = jnp.zeros((1, head), f32)
    extra = row_pack((zero, zero, zero, zero) + thirds(read), head)
    pick_row = iota((PACK, 32), 0)
    pick_col = iota((PACK, 32), 1)
    for member in range(8):
        if member:
            at = member - 1
            entry = factors_ref[at, 0:1, :] * begin - dot(begin, maps_ref[at]) + adds_ref[at]
        else:
            entry = begin
        send_ref[member, :half, :] = entry.astype(bf16)
        pick = ((pick_row < 4) & (pick_col == 4 * member + pick_row)).astype(bf16)
        send_ref[member, half:, :] = (dot(pick, mine) + extra).astype(bf16)


def finish_kernel(in_ref, out_ref, reach_ref, silu_ref, gain_ref, mixed_ref, cache_ref, read_ref):
    head = in_ref.shape[-1]
    half = head // 2
    for pair in range(4):
        seq, h = divmod(pair, 2)
        incoming = jnp.concatenate([in_ref[2 * pair, :half, :], in_ref[2 * pair + 1, :half, :]], 0)
        whole = out_ref[pair] + dot(reach_ref[pair], incoming, ROWS)
        mixed = whole * rms_scale(whole, norm_floor, True) * silu_ref[pair]
        mixed_ref[seq, :, h * head : (h + 1) * head] = mixed.astype(bf16)
        extra = in_ref[2 * pair, half:, :].astype(f32) + in_ref[2 * pair + 1, half:, :].astype(f32)
        cache_ref[seq, h] = extra[:4].astype(bf16)
        read = extra[4:5] + extra[5:6] + extra[6:7]
        read = read * rms_scale(read, norm_floor, True) * gain_ref[...]
        read_ref[seq : seq + 1, h * head : (h + 1) * head] = read


def vmem():
    return pl.BlockSpec(memory_space=pltpu.VMEM)


def smem():
    return pl.BlockSpec(memory_space=pltpu.SMEM)


def kernel(body, name, outputs, smem_count, args, scratch=(), limit=16):
    placed = [
        arg if at < smem_count else pltpu.with_memory_space_constraint(arg, pltpu.VMEM)
        for at, arg in enumerate(args)
    ]
    specs = [smem() if at < smem_count else vmem() for at in range(len(args))]
    return pl.pallas_call(
        body,
        name=name,
        out_shape=tuple(outputs),
        in_specs=specs,
        out_specs=tuple(vmem() for _ in outputs),
        scratch_shapes=list(scratch),
        compiler_params=pltpu.CompilerParams(vmem_limit_bytes=limit * 1024 * 1024),
    )(*placed)


def shift(value, axis, by):
    length = lax.axis_size(axis)
    return lax.ppermute(value, axis, [(at, (at + by) % length) for at in range(length)])


def shards(
    tokens, query_weight, key_weight, value_weight, gate_weight, beta_weight, decay_weight,
    beta_bias, rate_log, out_gain, new_query, new_key, new_value, new_beta, new_decay,
):
    _, span, depth = tokens.shape
    head = out_gain.shape[0]
    half = head // 2
    wide = 256
    width = query_weight.shape[1]
    rows = head + half + PACK
    first, second = tokens[0], tokens[1]
    swap = lambda value: shift(value, "c", 1)
    tokens_c = swap(tokens)
    up0 = shift(first, "y", 1)
    down1 = shift(second, "y", -1)
    up1 = shift(second, "y", 1)
    down0 = shift(first, "y", -1)
    far0 = shift(up0, "y", 1)
    far1 = shift(down1, "y", -1)
    swapped = [swap(value) for value in (up0, up1, down0, down1)]
    late = [*swapped, far0, far1, swap(far0), swap(far1)]
    gates = (beta_weight.T, decay_weight.T)
    gain = out_gain[None]
    on = pltpu.VMEM
    sums = [on((2 * span, width), f32), on((2 * span, width), f32), on((2 * span, head), f32)]
    weights = (key_weight, value_weight, *gates)
    early = kernel(early_kernel, "early", sums, 0, (tokens, tokens_c, *weights))
    middle = kernel(next_kernel, "middle", sums, 0, (up0, up1, down0, down1, *weights, *early))
    send, key_rows, fresh, carry, cols, turned = kernel(
        local_kernel,
        "local_terms",
        (
            on((8, rows, head), bf16),
            on((2 * span, width), bf16),
            on((4, span, head), bf16),
            on((4, span, head), bf16),
            on((2, wide, head), f32),
            on((2, head, wide), f32),
        ),
        2,
        (beta_bias, rate_log, *late, *weights, *middle),
    )
    arrived = lax.all_to_all(send, NEAR, 0, 0, tiled=True)
    local_out, reach, silu = kernel(
        window_kernel,
        "window_terms",
        (on((4, span, head), f32), on((4, span, head), bf16), on((4, span, head), f32)),
        0,
        (
            tokens, tokens_c, up0, up1, down0, down1, *late,
            query_weight, gate_weight, gain, key_rows, fresh, carry, cols, turned,
        ),
    )
    arrived, local_out = lax.optimization_barrier((arrived, local_out))
    total, maps, adds, factors = kernel(
        compose_kernel,
        "compose_near",
        (
            on((rows, head), bf16),
            on((7, head, head), bf16),
            on((7, half, head), f32),
            on((7, 8, head), f32),
        ),
        0,
        (arrived,),
    )
    others = [shift(total, "zh", by) for by in (1, 2, 3)]
    (back,) = kernel(
        spread_kernel,
        "spread_states",
        (on((8, half + PACK, head), bf16),),
        2,
        (
            new_beta, new_decay, total, *others, maps, adds, factors,
            new_query, new_key, new_value,
        ),
        (on((4, rows, head), bf16), on((head, head), f32), on((head, head), f32)),
    )
    returned = lax.all_to_all(back, NEAR, 0, 0, tiled=True)
    return kernel(
        finish_kernel,
        "finish",
        (
            jax.ShapeDtypeStruct((2, span, width), bf16),
            jax.ShapeDtypeStruct((2, 2, 4, head), bf16),
            jax.ShapeDtypeStruct((2, width), f32),
        ),
        0,
        (returned, local_out, reach, silu, gain),
    )


def solution(mesh):
    torus = Mesh(mesh.devices.reshape(4, 2, 4, 4, 2), AXES + ("y", "c"))
    sp, tp = AXES, ("y", "c")
    weight = P(None, tp)
    in_specs = (
        P(None, sp, tp),
        weight, weight, weight, weight, weight, weight,
        P(tp), P(tp), P(),
        P(None, tp, None), P(None, tp, None), P(None, tp, None),
        P(None, tp), P(None, tp),
    )
    out_specs = (P(None, sp, tp), P(None, tp, sp, None), P(None, tp))
    return jax.shard_map(
        shards, mesh=torus, in_specs=in_specs, out_specs=out_specs, check_vma=False
    )
```

```python
import jax
import jax.numpy as jnp
from jax import lax
from jax.experimental import pallas as pl
from jax.experimental.pallas import tpu as pltpu
from jax.sharding import Mesh
from jax.sharding import PartitionSpec as P

NEAR = ("zl", "x")
AXES = ("zh", "zl", "x")
PACK = 16
LANES = 128
unit_floor = 1.0
norm_floor = 0.001
bf16 = jnp.bfloat16
f32 = jnp.float32


def dot(left, right, dims=((1,), (0,))):
    return lax.dot_general(
        left.astype(bf16), right.astype(bf16), (dims, ((), ())), preferred_element_type=f32
    )


ROWS = ((1,), (1,))
COLS = ((0,), (0,))


def thirds(value):
    high = value.astype(bf16).astype(f32)
    rest = value - high
    mid = rest.astype(bf16).astype(f32)
    return high, mid, rest - mid


def iota(shape, dim):
    return lax.broadcasted_iota(jnp.int32, shape, dim)


def row_pack(values, width):
    rows = iota((PACK, width), 0)
    packed = jnp.zeros((PACK, width), f32)
    for at, value in enumerate(values):
        packed = jnp.where(rows == at, value, packed)
    return packed


def rms_scale(values, floor, mean):
    total = jnp.sum(values * values, axis=-1, keepdims=True)
    return lax.rsqrt((total / values.shape[-1] if mean else total) + floor)


def shard_index(ahead, swapped):
    core = lax.axis_index("c")
    core = 1 - core if swapped else core
    return lax.rem(lax.axis_index("y") + ahead, 4) * 2 + core


def first_row(slot, depth):
    return pl.multiple_of(shard_index(*slot) * depth, depth)


def joined(first, second):
    return jnp.concatenate([first[...], second[...]], axis=0)


def scalar_part(rows, stacked, slot):
    depth = rows.shape[-1]
    weight = stacked[:, pl.ds(first_row(slot, depth), depth)]
    weight = jnp.concatenate([weight, jnp.zeros((LANES - PACK, depth), bf16)], axis=0)
    return dot(rows, weight, ROWS)


SLOTS = (
    (0, False), (0, True), (3, False), (1, False), (3, True), (1, True), (2, False), (2, True),
)


def early_kernel(
    own, own_c, beta_w, decay_w, key_w, value_w, sum_ref, gate_ref, rest_ref, stacked_ref,
    token_buffer, weight_buffer, sems,
):
    depth = own.shape[-1]
    width = key_w.shape[-1]
    first = [pltpu.make_async_copy(own, token_buffer, sems.at[0])]
    later = []
    for at, slot in enumerate(SLOTS):
        start = first_row(slot, depth)
        for side, weight in enumerate((key_w, value_w)):
            lanes = pl.ds(side * width, width)
            source = weight.at[pl.ds(start, depth), :]
            if at < 2:
                to = weight_buffer.at[pl.ds(at * depth, depth), lanes]
                first.append(pltpu.make_async_copy(source, to, sems.at[0]))
            else:
                to = rest_ref.at[pl.ds((at - 2) * depth, depth), lanes]
                later.append(pltpu.make_async_copy(source, to, sems.at[1]))
    for copy in first + later:
        copy.start()
    rows = [ref[at : at + 1, :].astype(f32) for ref in (beta_w, decay_w) for at in range(2)]
    stacked_ref[...] = row_pack(rows, stacked_ref.shape[-1]).astype(bf16)
    for copy in first:
        copy.wait()
    total = gates = 0.0
    for at, piece in enumerate((token_buffer, own_c)):
        rows = piece[...].reshape(-1, depth)
        total = total + dot(rows, weight_buffer[at * depth : (at + 1) * depth, :])
        gates = gates + scalar_part(rows, stacked_ref, SLOTS[at])
    sum_ref[...] = total
    gate_ref[...] = gates
    for copy in later:
        copy.wait()


def add_pieces(pieces, from_slot, rest, stacked, total, gates):
    for at in range(len(pieces) // 2):
        rows = joined(*pieces[2 * at : 2 * at + 2])
        depth = rows.shape[-1]
        slot = from_slot + at
        total = total + dot(rows, rest[(slot - 2) * depth : (slot - 1) * depth, :])
        gates = gates + scalar_part(rows, stacked, SLOTS[slot])
    return total, gates


def middle_kernel(*refs):
    pieces, (sum_in, gate_in, rest, stacked, sum_ref, gate_ref) = refs[:8], refs[8:]
    total, gates = add_pieces(pieces, 2, rest, stacked, sum_in[...], gate_in[...])
    sum_ref[...] = total
    gate_ref[...] = gates


def lane_pair(ref, first):
    lanes = iota((1, LANES), 1)
    return jnp.where(lanes == first, ref[0], jnp.where(lanes == first + 1, ref[1], 0.0))


def local_kernel(bias_ref, rate_ref, *refs):
    pieces, (sum_in, gate_in, rest, stacked) = refs[:4], refs[4:8]
    outputs, buffers, sems = refs[8:14], refs[14:20], refs[20]
    send_ref, key_ref, fresh_ref, carry_ref, cols_ref, rows_ref = buffers
    copies = []

    def give(at, part=None):
        source, to = buffers[at], outputs[at]
        if part is not None:
            source, to = source.at[part], to.at[part]
        copies.append(pltpu.make_async_copy(source, to, sems.at[at]))
        copies[-1].start()

    span = pieces[0].shape[0]
    head = send_ref.shape[-1]
    total, gates = add_pieces(pieces, 6, rest, stacked, sum_in[...], gate_in[...])
    width = total.shape[-1] // 2
    key_rows = total[:, :width].astype(bf16)
    value_rows = total[:, width:].astype(bf16)
    key_ref[...] = key_rows
    give(1)
    strength = jax.nn.sigmoid(gates + lane_pair(bias_ref, 0))
    decays = -jnp.exp(lane_pair(rate_ref, 2)) * jax.nn.softplus(gates)
    wide = cols_ref.shape[1]
    pairs = []
    lanes = iota((wide, head), 1)
    causal_wide = (iota((wide, wide), 0) >= iota((wide, wide), 1)).astype(bf16)
    for seq in range(2):
        take = slice(seq * span, (seq + 1) * span)
        padded = jnp.concatenate([decays[take], jnp.zeros((wide - span, head), f32)], axis=0)
        cumulative = sum(dot(causal_wide, part) for part in thirds(padded))
        table = jnp.where((lanes == 2) | (lanes == 3), cumulative, 0.0)
        for h in range(2):
            keys = key_rows[take, h * head : (h + 1) * head].astype(f32)
            unit = jnp.concatenate(
                [rms_scale(keys, unit_floor, False), jnp.zeros((wide - span, 1), f32)], axis=0
            )
            beta = jnp.concatenate(
                [strength[take, h : h + 1], jnp.zeros((wide - span, 1), f32)], axis=0
            )
            table = jnp.where(lanes == h, beta, table)
            table = jnp.where(lanes == 4 + h, unit, table)
        cols_ref[seq] = table
        rows_ref[seq] = table.T
    give(4)
    give(5)
    t = iota((span, span), 0)
    s = iota((span, span), 1)
    lower, inverse = [], []
    for pair in range(4):
        seq, h = divmod(pair, 2)
        keys = key_rows[seq * span : (seq + 1) * span, h * head : (h + 1) * head]
        col = lambda at: cols_ref[seq, :span, at + h : at + h + 1]
        row = lambda at: rows_ref[seq, at + h : at + h + 1, :span]
        spread = jnp.where(t >= s, col(2) - row(2), 0.0)
        alike = dot(keys, keys, ROWS) * (col(0) * col(4)) * row(4) * jnp.exp(spread)
        lower.append(jnp.where(t > s, alike, 0.0))
        inverse.append(jnp.where(t // 2 == s // 2, lower[pair], 0.0))
    size = 2
    while size < span:
        mask = (t // (2 * size) == s // (2 * size)) & (t // size != s // size)
        steps = []
        for pair in range(4):
            block = jnp.where(mask, lower[pair], 0.0)
            steps.append(block - dot(block, inverse[pair]))
        for pair in range(4):
            inverse[pair] = inverse[pair] + steps[pair] - dot(inverse[pair], steps[pair])
        size *= 2
    for pair in range(4):
        seq, h = divmod(pair, 2)
        take = slice(seq * span, (seq + 1) * span)
        keys = key_rows[take, h * head : (h + 1) * head]
        values = value_rows[take, h * head : (h + 1) * head]
        col = lambda at: cols_ref[seq, :span, at + h : at + h + 1]
        row = lambda at: rows_ref[seq, at + h : at + h + 1, :span]
        fresh = col(0) * values.astype(f32) - dot(inverse[pair] * row(0), values)
        carry = (col(0) * col(4) * jnp.exp(col(2))) * keys.astype(f32) - dot(
            inverse[pair] * (row(0) * row(4) * jnp.exp(row(2))), keys
        )
        last = cols_ref[seq, span - 1 : span, 2 + h : 3 + h]
        late = col(4) * jnp.exp(last - col(2))
        reach = dot(carry * late, keys, COLS)
        gain = dot(fresh * late, keys, COLS)
        fresh_ref[pair] = fresh.astype(bf16)
        carry_ref[pair] = carry.astype(bf16)
        factor = row_pack(thirds(jnp.broadcast_to(jnp.exp(last), (1, head))), head)
        half = head // 2
        for side in range(2):
            to = 2 * pair + side
            send_ref[to, :head, :] = reach.astype(bf16)
            send_ref[to, head : head + half, :] = gain[side * half : (side + 1) * half].astype(bf16)
            send_ref[to, head + half :, :] = factor.astype(bf16)
        give(0, pl.ds(2 * pair, 2))
    give(2)
    give(3)
    for copy in copies:
        copy.wait()


def window_kernel(*refs):
    pieces, refs = refs[:14], refs[14:]
    query_w, gate_w, gain_ref, key_ref, fresh_ref, carry_ref, cols_ref, rows_ref = refs[:8]
    out_ref, reach_ref, silu_ref, token_buffer, query_buffer, gate_buffer, sems = refs[8:]
    span, depth = token_buffer.shape[2:]
    head = fresh_ref.shape[-1]
    weights = ((query_w, query_buffer), (gate_w, gate_buffer))
    copies = []
    for at, slot in enumerate(SLOTS):
        if at < 2:
            parts = [(pieces[at], token_buffer.at[at])]
        else:
            parts = [(pieces[2 * at - 2 + seq], token_buffer.at[at, seq]) for seq in range(2)]
        for weight, buffer in weights:
            parts.append((weight.at[pl.ds(first_row(slot, depth), depth), :], buffer.at[at]))
        copies.append([pltpu.make_async_copy(a, b, sems.at[at]) for a, b in parts])
        for copy in copies[at]:
            copy.start()
    query_total = gate_total = 0.0
    for at in range(8):
        for copy in copies[at]:
            copy.wait()
        rows = token_buffer[at].reshape(-1, depth)
        query_total = query_total + dot(rows, query_buffer[at])
        gate_total = gate_total + dot(rows, gate_buffer[at])
    query_rows = query_total.astype(bf16)
    gate_rows = gate_total.astype(bf16).astype(f32)
    t = iota((span, span), 0)
    s = iota((span, span), 1)
    for pair in range(4):
        seq, h = divmod(pair, 2)
        take = slice(seq * span, (seq + 1) * span)
        part = slice(h * head, (h + 1) * head)
        col = lambda at: cols_ref[seq, :span, at + h : at + h + 1]
        row = lambda at: rows_ref[seq, at + h : at + h + 1, :span]
        queries = query_rows[take, part]
        unit = rms_scale(queries.astype(f32), unit_floor, False)
        spread = jnp.where(t >= s, col(2) - row(2), 0.0)
        scores = dot(queries, key_ref[take, part], ROWS) * unit * row(4) * jnp.exp(spread)
        scores = jnp.where(t >= s, scores, 0.0).astype(bf16)
        out_ref[pair] = dot(scores, fresh_ref[pair])
        reach = (unit * jnp.exp(col(2))) * queries.astype(f32) - dot(scores, carry_ref[pair])
        reach_ref[pair] = reach.astype(bf16)
        gate = gate_rows[take, part]
        silu_ref[pair] = gain_ref[...] * gate * jax.nn.sigmoid(gate)


def unpack_factor(block):
    block = block.astype(f32)
    return block[0:1] + block[1:2] + block[2:3]


def compose_kernel(in_ref, total_ref, maps_ref, adds_ref, factors_ref):
    count, rows, head = in_ref.shape
    body = rows - PACK

    def load(at):
        return in_ref[at, :body, :].astype(f32), unpack_factor(in_ref[at, body:, :])

    def join(first, second):
        both, factor = first
        later, later_factor = second
        tail = jnp.concatenate([factor * later[:head], later[head:]], axis=0)
        return later_factor * both - dot(both, later[:head]) + tail, factor * later_factor

    member = [load(at) for at in range(count)]
    upto = [None] * (count + 1)
    upto[1] = member[0]
    c23, c45, c67 = (join(member[at], member[at + 1]) for at in (2, 4, 6))
    upto[2] = join(member[0], member[1])
    c456 = join(c45, member[6])
    c4567 = join(c45, c67)
    upto[4] = join(upto[2], c23)
    upto[8] = join(upto[4], c4567)
    both, factor = upto[8]
    total_ref[:body, :] = both.astype(bf16)
    total_ref[body:, :] = row_pack(thirds(factor), head).astype(bf16)
    upto[3] = join(upto[2], member[2])
    upto[5] = join(upto[4], member[4])
    upto[6] = join(upto[4], c45)
    upto[7] = join(upto[4], c456)
    for at in range(1, count):
        both, factor = upto[at]
        maps_ref[at - 1] = both[:head].astype(bf16)
        adds_ref[at - 1] = both[head:]
        factors_ref[at - 1] = jnp.broadcast_to(factor, (8, head))


def spread_kernel(
    beta_ref, decay_ref, own, back1, back2, back3, maps_ref, adds_ref, factors_ref,
    query_ref, key_ref, value_ref, out_in, reach_in, silu_in,
    send_ref, out_ref, reach_ref, silu_ref, groups_ref, wide_ref, turned_ref, sems,
):
    moved = ((out_in, out_ref), (reach_in, reach_ref), (silu_in, silu_ref))
    copies = [pltpu.make_async_copy(a, b, sems.at[at]) for at, (a, b) in enumerate(moved)]
    for copy in copies:
        copy.start()
    rows, head = own.shape
    half = head // 2
    far = lax.axis_index("zh")
    near = lax.axis_index("zl") * 4 + lax.axis_index("x")
    pair = near // 2
    side = near % 2
    seq, h = pair // 2, pair % 2

    def chosen(ref):
        total = jnp.zeros((1, head), f32)
        for at in range(4):
            row = ref[at // 2, at % 2 : at % 2 + 1, :].astype(f32)
            total = jnp.where(pair == at, row, total)
        return total

    for slot, ref in enumerate((own, back1, back2, back3)):
        groups_ref[slot] = ref[...]
    state = jnp.zeros((half, head), f32)
    begin = state
    for group in range(4):
        begin = jnp.where(far == group, state, begin)
        block = groups_ref[lax.rem(far - group + 4, 4)]
        added = block[head : head + half].astype(f32)
        if group:
            state = unpack_factor(block[head + half :]) * state - dot(state, block[:head]) + added
        else:
            state = added
    final = state.astype(bf16).astype(f32)
    wide_ref[...] = jnp.zeros((head, head), f32)
    wide_ref[pl.ds(pl.multiple_of(side * half, half), half), :] = final
    padded = wide_ref[...]
    turned_ref[...] = padded.T
    mine = turned_ref[pl.ds(pl.multiple_of(far * 32, 32), 32), :]
    query = chosen(query_ref)
    key = chosen(key_ref)
    query = query * rms_scale(query, unit_floor, False)
    key = key * rms_scale(key, unit_floor, False)
    hits = dot(row_pack(thirds(query) + thirds(key), head), padded, ROWS)
    recall = hits[0:1] + hits[1:2] + hits[2:3]
    retrieve = hits[3:4] + hits[4:5] + hits[5:6]
    intersect = jnp.sum(key * query, axis=-1, keepdims=True)
    fresh = chosen(value_ref) - decay_ref[seq, h] * retrieve
    read = decay_ref[seq, h] * recall + (beta_ref[seq, h] * intersect) * fresh
    read = jnp.where(iota((1, head), 1) // half == side, read, 0.0)
    zero = jnp.zeros((1, head), f32)
    extra = row_pack((zero, zero, zero, zero) + thirds(read), head)
    pick_row = iota((PACK, 32), 0)
    pick_col = iota((PACK, 32), 1)
    for member in range(8):
        if member:
            at = member - 1
            entry = factors_ref[at, 0:1, :] * begin - dot(begin, maps_ref[at]) + adds_ref[at]
        else:
            entry = begin
        send_ref[member, :half, :] = entry.astype(bf16)
        pick = ((pick_row < 4) & (pick_col == 4 * member + pick_row)).astype(bf16)
        send_ref[member, half:, :] = (dot(pick, mine) + extra).astype(bf16)
    for copy in copies:
        copy.wait()


def finish_kernel(in_ref, out_ref, reach_ref, silu_ref, gain_ref, mixed_ref, cache_ref, read_ref):
    head = in_ref.shape[-1]
    half = head // 2
    for pair in range(4):
        seq, h = divmod(pair, 2)
        incoming = jnp.concatenate([in_ref[2 * pair, :half, :], in_ref[2 * pair + 1, :half, :]], 0)
        whole = out_ref[pair] + dot(reach_ref[pair], incoming, ROWS)
        mixed = whole * rms_scale(whole, norm_floor, True) * silu_ref[pair]
        mixed_ref[seq, :, h * head : (h + 1) * head] = mixed.astype(bf16)
        extra = in_ref[2 * pair, half:, :].astype(f32) + in_ref[2 * pair + 1, half:, :].astype(f32)
        cache_ref[seq, h] = extra[:4].astype(bf16)
        read = extra[4:5] + extra[5:6] + extra[6:7]
        read = read * rms_scale(read, norm_floor, True) * gain_ref[...]
        read_ref[seq : seq + 1, h * head : (h + 1) * head] = read


def vmem():
    return pl.BlockSpec(memory_space=pltpu.VMEM)


def smem():
    return pl.BlockSpec(memory_space=pltpu.SMEM)


def kernel(body, name, outputs, kinds, args, scratch=(), limit=16):
    given = {"s": smem, "v": vmem, "p": vmem, "h": lambda: pl.BlockSpec(memory_space=pl.ANY)}
    placed = [
        arg
        if kind == "s"
        else pltpu.with_memory_space_constraint(arg, pltpu.VMEM if kind == "p" else pltpu.HBM)
        for kind, arg in zip(kinds, args, strict=True)
    ]
    plain = lambda out: pltpu.HBM(out.shape, out.dtype)
    return pl.pallas_call(
        body,
        name=name,
        out_shape=tuple(out if kind == "p" else plain(out) for kind, out in outputs),
        in_specs=[given[kind]() for kind in kinds],
        out_specs=tuple(given[kind]() for kind, _ in outputs),
        scratch_shapes=list(scratch),
        compiler_params=pltpu.CompilerParams(vmem_limit_bytes=limit * 1024 * 1024),
    )(*placed)


def shift(value, axis, by):
    length = lax.axis_size(axis)
    return lax.ppermute(value, axis, [(at, (at + by) % length) for at in range(length)])


def shards(
    tokens, query_weight, key_weight, value_weight, gate_weight, beta_weight, decay_weight,
    beta_bias, rate_log, out_gain, new_query, new_key, new_value, new_beta, new_decay,
):
    _, span, depth = tokens.shape
    head = out_gain.shape[0]
    half = head // 2
    wide = 256
    width = query_weight.shape[1]
    rows = head + half + PACK
    on, dma = pltpu.VMEM, pltpu.SemaphoreType.DMA
    depth = tokens.shape[2]
    swap = lambda value: shift(value, "c", 1)
    tokens_c = swap(tokens)
    first, second = tokens[0], tokens[1]
    up0 = shift(first, "y", 1)
    down1 = shift(second, "y", -1)
    up1 = shift(second, "y", 1)
    down0 = shift(first, "y", -1)
    sums = [("p", on((2 * span, 2 * width), f32)), ("p", on((2 * span, head), f32))]
    early = kernel(
        early_kernel,
        "early",
        sums + [("p", on((6 * depth, 2 * width), bf16)), ("p", on((PACK, 8 * depth), bf16))],
        "hpvvhh",
        (tokens, tokens_c, beta_weight.T, decay_weight.T, key_weight, value_weight),
        (on((2, span, depth), bf16), on((2 * depth, 2 * width), bf16), dma((2,))),
    )
    up0, down1, *early = lax.optimization_barrier((up0, down1, *early))
    rest = early[2:]
    far0 = shift(up0, "y", 1)
    far1 = shift(down1, "y", -1)
    near = (up0, up1, down0, down1)
    swapped = [swap(value) for value in near]
    middle = kernel(
        middle_kernel, "middle", sums, "p" * 12, (*near, *swapped, *early[:2], *rest)
    )
    far0, far1, *middle = lax.optimization_barrier((far0, far1, *middle))
    last = [far0, far1, swap(far0), swap(far1)]
    local_shapes = [
        on((8, rows, head), bf16),
        on((2 * span, width), bf16),
        on((4, span, head), bf16),
        on((4, span, head), bf16),
        on((2, wide, head), f32),
        on((2, head, wide), f32),
    ]
    send, *shared = kernel(
        local_kernel,
        "local_terms",
        [("h", out) for out in local_shapes],
        "ss" + "p" * 8,
        (beta_bias, rate_log, *last, *middle, *rest),
        (*local_shapes, dma((6,))),
    )
    arrived = lax.all_to_all(send, NEAR, 0, 0, tiled=True)
    gain = out_gain[None]
    finals = [on((4, span, head), f32), on((4, span, head), bf16), on((4, span, head), f32)]
    local_out, reach, silu = kernel(
        window_kernel,
        "window_terms",
        [("v", out) for out in finals],
        "h" * 16 + "v" * 6,
        (tokens, tokens_c, *near, *swapped, *last, query_weight, gate_weight, gain, *shared),
        (
            on((8, 2, span, depth), bf16),
            on((8, depth, width), bf16),
            on((8, depth, width), bf16),
            dma((8,)),
        ),
        24,
    )
    arrived, local_out = lax.optimization_barrier((arrived, local_out))
    total, maps, adds, factors = kernel(
        compose_kernel,
        "compose_near",
        [
            ("p", on((rows, head), bf16)),
            ("p", on((7, head, head), bf16)),
            ("p", on((7, half, head), f32)),
            ("p", on((7, 8, head), f32)),
        ],
        "p",
        (arrived,),
    )
    others = [shift(total, "zh", by) for by in (1, 2, 3)]
    back, *finals_in = kernel(
        spread_kernel,
        "spread_states",
        [("p", on((8, half + PACK, head), bf16)), *(("p", out) for out in finals)],
        "ss" + "p" * 10 + "hhh",
        (
            new_beta, new_decay, total, *others, maps, adds, factors,
            new_query, new_key, new_value, local_out, reach, silu,
        ),
        (
            on((4, rows, head), bf16), on((head, head), f32), on((head, head), f32), dma((3,)),
        ),
    )
    returned = lax.all_to_all(back, NEAR, 0, 0, tiled=True)
    return kernel(
        finish_kernel,
        "finish",
        [
            ("v", on((2, span, width), bf16)),
            ("v", on((2, 2, 4, head), bf16)),
            ("v", on((2, width), f32)),
        ],
        "ppppp",
        (returned, *finals_in, gain),
    )


def solution(mesh):
    torus = Mesh(mesh.devices.reshape(4, 2, 4, 4, 2), AXES + ("y", "c"))
    sp, tp = AXES, ("y", "c")
    weight = P(None, tp)
    in_specs = (
        P(None, sp, tp),
        weight, weight, weight, weight, weight, weight,
        P(tp), P(tp), P(),
        P(None, tp, None), P(None, tp, None), P(None, tp, None),
        P(None, tp), P(None, tp),
    )
    out_specs = (P(None, sp, tp), P(None, tp, sp, None), P(None, tp))
    return jax.shard_map(
        shards, mesh=torus, in_specs=in_specs, out_specs=out_specs, check_vma=False
    )
```

```python
import functools

import jax
import jax.numpy as jnp
from jax import lax
from jax.experimental import pallas as pl
from jax.experimental.pallas import tpu as pltpu
from jax.sharding import Mesh
from jax.sharding import PartitionSpec as P


NEAR = ("zl", "x")
AXES = ("zh", "zl", "x")
PACK = 16
LANES = 128
unit_floor = 1.0
norm_floor = 0.001
bf16 = jnp.bfloat16
f32 = jnp.float32


def dot(left, right, dims=((1,), (0,))):
    return lax.dot_general(
        left.astype(bf16), right.astype(bf16), (dims, ((), ())), preferred_element_type=f32
    )


ROWS = ((1,), (1,))
COLS = ((0,), (0,))


def thirds(value):
    high = value.astype(bf16).astype(f32)
    rest = value - high
    mid = rest.astype(bf16).astype(f32)
    return high, mid, rest - mid


def iota(shape, dim):
    return lax.broadcasted_iota(jnp.int32, shape, dim)


def row_pack(values, width):
    rows = iota((PACK, width), 0)
    packed = jnp.zeros((PACK, width), f32)
    for at, value in enumerate(values):
        packed = jnp.where(rows == at, value, packed)
    return packed


def rms_scale(values, floor, mean):
    total = jnp.sum(values * values, axis=-1, keepdims=True)
    return lax.rsqrt((total / values.shape[-1] if mean else total) + floor)


def shard_index(ahead, swapped):
    core = lax.axis_index("c")
    core = 1 - core if swapped else core
    return lax.rem(lax.axis_index("y") + ahead, 4) * 2 + core


def first_row(slot, depth):
    return pl.multiple_of(shard_index(*slot) * depth, depth)


def joined(first, second):
    return jnp.concatenate([first[...], second[...]], axis=0)


def scalar_part(rows, stacked, slot):
    depth = rows.shape[-1]
    weight = stacked[:, pl.ds(first_row(slot, depth), depth)]
    weight = jnp.concatenate([weight, jnp.zeros((LANES - PACK, depth), bf16)], axis=0)
    return dot(rows, weight, ROWS)


SLOTS = (
    (0, False), (0, True), (3, False), (1, False), (3, True), (1, True), (2, False), (2, True),
)


def early_kernel(
    own, own_c, beta_w, decay_w, key_w, value_w, sum_ref, gate_ref, rest_ref, stacked_ref,
    token_buffer, weight_buffer, scalar_buffer, sems,
):
    depth = own.shape[-1]
    width = key_w.shape[-1]
    first = [pltpu.make_async_copy(own, token_buffer, sems.at[0])]
    for at, weight in enumerate((beta_w, decay_w)):
        first.append(pltpu.make_async_copy(weight, scalar_buffer.at[at], sems.at[0]))
    later = []
    for at, slot in enumerate(SLOTS):
        start = first_row(slot, depth)
        for side, weight in enumerate((key_w, value_w)):
            lanes = pl.ds(side * width, width)
            source = weight.at[pl.ds(start, depth), :]
            if at < 2:
                to = weight_buffer.at[pl.ds(at * depth, depth), lanes]
                first.append(pltpu.make_async_copy(source, to, sems.at[0]))
            else:
                to = rest_ref.at[pl.ds((at - 2) * depth, depth), lanes]
                later.append(pltpu.make_async_copy(source, to, sems.at[1]))
    for copy in first + later:
        copy.start()
    for copy in first:
        copy.wait()
    rows = [scalar_buffer[at, h : h + 1, :].astype(f32) for at in range(2) for h in range(2)]
    stacked_ref[...] = row_pack(rows, stacked_ref.shape[-1]).astype(bf16)
    total = gates = 0.0
    for at, piece in enumerate((token_buffer, own_c)):
        rows = piece[...].reshape(-1, depth)
        total = total + dot(rows, weight_buffer[at * depth : (at + 1) * depth, :])
        gates = gates + scalar_part(rows, stacked_ref, SLOTS[at])
    sum_ref[...] = total
    gate_ref[...] = gates
    for copy in later:
        copy.wait()


def add_pieces(pieces, from_slot, rest, stacked, total, gates):
    for at in range(len(pieces) // 2):
        rows = joined(*pieces[2 * at : 2 * at + 2])
        depth = rows.shape[-1]
        slot = from_slot + at
        total = total + dot(rows, rest[(slot - 2) * depth : (slot - 1) * depth, :])
        gates = gates + scalar_part(rows, stacked, SLOTS[slot])
    return total, gates


def middle_kernel(first_slot, *refs):
    pieces, (sum_in, gate_in, rest, stacked, sum_ref, gate_ref) = refs[:-6], refs[-6:]
    total, gates = add_pieces(pieces, first_slot, rest, stacked, sum_in[...], gate_in[...])
    sum_ref[...] = total
    gate_ref[...] = gates


def lane_pair(ref, first):
    lanes = iota((1, LANES), 1)
    return jnp.where(lanes == first, ref[0], jnp.where(lanes == first + 1, ref[1], 0.0))


def local_kernel(bias_ref, rate_ref, *refs):
    pieces, (sum_in, gate_in, rest, stacked) = refs[:2], refs[2:6]
    outputs, buffers, sems = refs[6:12], refs[12:18], refs[18]
    send_ref, key_ref, fresh_ref, carry_ref, cols_ref, rows_ref = buffers
    copies = []

    def give(at, part=None):
        source, to = buffers[at], outputs[at]
        if part is not None:
            source, to = source.at[part], to.at[part]
        copies.append(pltpu.make_async_copy(source, to, sems.at[at]))
        copies[-1].start()

    span = pieces[0].shape[0]
    head = send_ref.shape[-1]
    total, gates = add_pieces(pieces, 7, rest, stacked, sum_in[...], gate_in[...])
    width = total.shape[-1] // 2
    key_rows = total[:, :width].astype(bf16)
    value_rows = total[:, width:].astype(bf16)
    key_ref[...] = key_rows
    give(1)
    strength = jax.nn.sigmoid(gates + lane_pair(bias_ref, 0))
    decays = -jnp.exp(lane_pair(rate_ref, 2)) * jax.nn.softplus(gates)
    wide = cols_ref.shape[1]
    lanes = iota((wide, head), 1)
    causal_wide = (iota((wide, wide), 0) >= iota((wide, wide), 1)).astype(bf16)
    for seq in range(2):
        take = slice(seq * span, (seq + 1) * span)
        padded = jnp.concatenate([decays[take], jnp.zeros((wide - span, head), f32)], axis=0)
        cumulative = sum(dot(causal_wide, part) for part in thirds(padded))
        table = jnp.where((lanes == 2) | (lanes == 3), cumulative, 0.0)
        for h in range(2):
            keys = key_rows[take, h * head : (h + 1) * head].astype(f32)
            unit = jnp.concatenate(
                [rms_scale(keys, unit_floor, False), jnp.zeros((wide - span, 1), f32)], axis=0
            )
            beta = jnp.concatenate(
                [strength[take, h : h + 1], jnp.zeros((wide - span, 1), f32)], axis=0
            )
            table = jnp.where(lanes == h, beta, table)
            table = jnp.where(lanes == 4 + h, unit, table)
        cols_ref[seq] = table
        rows_ref[seq] = table.T
    give(4)
    give(5)
    t = iota((span, span), 0)
    s = iota((span, span), 1)
    apart = t ^ s
    lower, inverse = [], []
    for pair in range(4):
        seq, h = divmod(pair, 2)
        keys = key_rows[seq * span : (seq + 1) * span, h * head : (h + 1) * head]
        col = lambda at: cols_ref[seq, :span, at + h : at + h + 1]
        row = lambda at: rows_ref[seq, at + h : at + h + 1, :span]
        spread = jnp.where(t >= s, col(2) - row(2), 0.0)
        alike = dot(keys, keys, ROWS) * (col(0) * col(4)) * row(4) * jnp.exp(spread)
        lower.append(jnp.where(t > s, alike, 0.0))
        inverse.append(jnp.where(apart < 2, lower[pair], 0.0))
    size = 2
    while size < span:
        mask = (apart >= size) & (apart < 2 * size)
        steps = []
        for pair in range(4):
            block = jnp.where(mask, lower[pair], 0.0)
            steps.append(block - dot(block, inverse[pair]))
        for pair in range(4):
            inverse[pair] = inverse[pair] + steps[pair] - dot(inverse[pair], steps[pair])
        size *= 2
    for pair in range(4):
        seq, h = divmod(pair, 2)
        take = slice(seq * span, (seq + 1) * span)
        keys = key_rows[take, h * head : (h + 1) * head]
        values = value_rows[take, h * head : (h + 1) * head]
        col = lambda at: cols_ref[seq, :span, at + h : at + h + 1]
        row = lambda at: rows_ref[seq, at + h : at + h + 1, :span]
        fresh = col(0) * values.astype(f32) - dot(inverse[pair] * row(0), values)
        carry = (col(0) * col(4) * jnp.exp(col(2))) * keys.astype(f32) - dot(
            inverse[pair] * (row(0) * row(4) * jnp.exp(row(2))), keys
        )
        last = cols_ref[seq, span - 1 : span, 2 + h : 3 + h]
        late = col(4) * jnp.exp(last - col(2))
        reach = dot(carry * late, keys, COLS)
        gain = dot(fresh * late, keys, COLS)
        fresh_ref[pair] = fresh.astype(bf16)
        carry_ref[pair] = carry.astype(bf16)
        factor = row_pack(thirds(jnp.broadcast_to(jnp.exp(last), (1, head))), head)
        half = head // 2
        for side in range(2):
            to = 2 * pair + side
            send_ref[to, :head, :] = reach.astype(bf16)
            send_ref[to, head : head + half, :] = gain[side * half : (side + 1) * half].astype(bf16)
            send_ref[to, head + half :, :] = factor.astype(bf16)
        give(0, pl.ds(2 * pair, 2))
    give(2)
    give(3)
    for copy in copies:
        copy.wait()


def window_kernel(*refs):
    pieces, refs = refs[:14], refs[14:]
    query_w, gate_w, gain_ref, key_ref, fresh_ref, carry_ref, cols_ref, rows_ref = refs[:8]
    out_ref, reach_ref, silu_ref, token_buffer, query_buffer, gate_buffer, sems = refs[8:]
    span, depth = token_buffer.shape[2:]
    head = fresh_ref.shape[-1]
    weights = ((query_w, query_buffer), (gate_w, gate_buffer))
    copies = []
    for at, slot in enumerate(SLOTS):
        if at < 2:
            parts = [(pieces[at], token_buffer.at[at])]
        else:
            parts = [(pieces[2 * at - 2 + seq], token_buffer.at[at, seq]) for seq in range(2)]
        for weight, buffer in weights:
            parts.append((weight.at[pl.ds(first_row(slot, depth), depth), :], buffer.at[at]))
        copies.append([pltpu.make_async_copy(a, b, sems.at[at]) for a, b in parts])
        for copy in copies[at]:
            copy.start()
    query_total = gate_total = 0.0
    for at in range(8):
        for copy in copies[at]:
            copy.wait()
        rows = token_buffer[at].reshape(-1, depth)
        query_total = query_total + dot(rows, query_buffer[at])
        gate_total = gate_total + dot(rows, gate_buffer[at])
    query_rows = query_total.astype(bf16)
    gate_rows = gate_total.astype(bf16).astype(f32)
    t = iota((span, span), 0)
    s = iota((span, span), 1)
    for pair in range(4):
        seq, h = divmod(pair, 2)
        take = slice(seq * span, (seq + 1) * span)
        part = slice(h * head, (h + 1) * head)
        col = lambda at: cols_ref[seq, :span, at + h : at + h + 1]
        row = lambda at: rows_ref[seq, at + h : at + h + 1, :span]
        queries = query_rows[take, part]
        unit = rms_scale(queries.astype(f32), unit_floor, False)
        spread = jnp.where(t >= s, col(2) - row(2), 0.0)
        scores = dot(queries, key_ref[take, part], ROWS) * unit * row(4) * jnp.exp(spread)
        scores = jnp.where(t >= s, scores, 0.0).astype(bf16)
        out_ref[pair] = dot(scores, fresh_ref[pair])
        reach = (unit * jnp.exp(col(2))) * queries.astype(f32) - dot(scores, carry_ref[pair])
        reach_ref[pair] = reach.astype(bf16)
        gate = gate_rows[take, part]
        silu_ref[pair] = gain_ref[...] * gate * jax.nn.sigmoid(gate)


def unpack_factor(block):
    block = block.astype(f32)
    return block[0:1] + block[1:2] + block[2:3]


def compose_kernel(in_ref, total_ref, maps_ref, adds_ref, factors_ref):
    count, rows, head = in_ref.shape
    body = rows - PACK

    def load(at):
        return in_ref[at, :body, :].astype(f32), unpack_factor(in_ref[at, body:, :])

    def join(first, second):
        both, factor = first
        later, later_factor = second
        tail = jnp.concatenate([factor * later[:head], later[head:]], axis=0)
        return later_factor * both - dot(both, later[:head]) + tail, factor * later_factor

    member = [load(at) for at in range(count)]
    upto = [None] * (count + 1)
    upto[1] = member[0]
    c23, c45, c67 = (join(member[at], member[at + 1]) for at in (2, 4, 6))
    upto[2] = join(member[0], member[1])
    c456 = join(c45, member[6])
    c4567 = join(c45, c67)
    upto[4] = join(upto[2], c23)
    upto[8] = join(upto[4], c4567)
    both, factor = upto[8]
    total_ref[:body, :] = both.astype(bf16)
    total_ref[body:, :] = row_pack(thirds(factor), head).astype(bf16)
    upto[3] = join(upto[2], member[2])
    upto[5] = join(upto[4], member[4])
    upto[6] = join(upto[4], c45)
    upto[7] = join(upto[4], c456)
    for at in range(1, count):
        both, factor = upto[at]
        maps_ref[at - 1] = both[:head].astype(bf16)
        adds_ref[at - 1] = both[head:]
        factors_ref[at - 1] = jnp.broadcast_to(factor, (8, head))


def spread_kernel(
    beta_ref, decay_ref, own, back1, back2, back3, maps_ref, adds_ref, factors_ref,
    query_ref, key_ref, value_ref, send_ref, groups_ref, wide_ref, turned_ref,
):
    _, head = own.shape
    half = head // 2
    far = lax.axis_index("zh")
    near = lax.axis_index("zl") * 4 + lax.axis_index("x")
    pair = near // 2
    side = near % 2
    seq, h = pair // 2, pair % 2

    def chosen(ref):
        total = jnp.zeros((1, head), f32)
        for at in range(4):
            row = ref[at // 2, at % 2 : at % 2 + 1, :].astype(f32)
            total = jnp.where(pair == at, row, total)
        return total

    for slot, ref in enumerate((own, back1, back2, back3)):
        groups_ref[slot] = ref[...]
    state = jnp.zeros((half, head), f32)
    begin = state
    for group in range(4):
        begin = jnp.where(far == group, state, begin)
        block = groups_ref[lax.rem(far - group + 4, 4)]
        added = block[head : head + half].astype(f32)
        if group:
            state = unpack_factor(block[head + half :]) * state - dot(state, block[:head]) + added
        else:
            state = added
    final = state.astype(bf16).astype(f32)
    wide_ref[...] = jnp.zeros((head, head), f32)
    wide_ref[pl.ds(pl.multiple_of(side * half, half), half), :] = final
    padded = wide_ref[...]
    turned_ref[...] = padded.T
    mine = turned_ref[pl.ds(pl.multiple_of(far * 32, 32), 32), :]
    query = chosen(query_ref)
    key = chosen(key_ref)
    query = query * rms_scale(query, unit_floor, False)
    key = key * rms_scale(key, unit_floor, False)
    hits = dot(row_pack(thirds(query) + thirds(key), head), padded, ROWS)
    recall = hits[0:1] + hits[1:2] + hits[2:3]
    retrieve = hits[3:4] + hits[4:5] + hits[5:6]
    intersect = jnp.sum(key * query, axis=-1, keepdims=True)
    fresh = chosen(value_ref) - decay_ref[seq, h] * retrieve
    read = decay_ref[seq, h] * recall + (beta_ref[seq, h] * intersect) * fresh
    read = jnp.where(iota((1, head), 1) // half == side, read, 0.0)
    zero = jnp.zeros((1, head), f32)
    extra = row_pack((zero, zero, zero, zero) + thirds(read), head)
    pick_row = iota((PACK, 32), 0)
    pick_col = iota((PACK, 32), 1)
    for member in range(8):
        if member:
            at = member - 1
            entry = factors_ref[at, 0:1, :] * begin - dot(begin, maps_ref[at]) + adds_ref[at]
        else:
            entry = begin
        send_ref[member, :half, :] = entry.astype(bf16)
        pick = ((pick_row < 4) & (pick_col == 4 * member + pick_row)).astype(bf16)
        send_ref[member, half:, :] = (dot(pick, mine) + extra).astype(bf16)


def load_kernel(_, *refs):
    count = len(refs) // 2
    sources, outputs, sems = refs[:count], refs[count : 2 * count], refs[2 * count]
    copies = [
        pltpu.make_async_copy(a, b, sems.at[at]) for at, (a, b) in enumerate(zip(sources, outputs))
    ]
    for copy in copies:
        copy.start()
    for copy in copies:
        copy.wait()


def finish_kernel(in_ref, out_ref, reach_ref, silu_ref, gain_ref, mixed_ref, cache_ref, read_ref):
    head = in_ref.shape[-1]
    half = head // 2
    for pair in range(4):
        seq, h = divmod(pair, 2)
        incoming = jnp.concatenate([in_ref[2 * pair, :half, :], in_ref[2 * pair + 1, :half, :]], 0)
        whole = out_ref[pair] + dot(reach_ref[pair], incoming, ROWS)
        mixed = whole * rms_scale(whole, norm_floor, True) * silu_ref[pair]
        mixed_ref[seq, :, h * head : (h + 1) * head] = mixed.astype(bf16)
        extra = in_ref[2 * pair, half:, :].astype(f32) + in_ref[2 * pair + 1, half:, :].astype(f32)
        cache_ref[seq, h] = extra[:4].astype(bf16)
        read = extra[4:5] + extra[5:6] + extra[6:7]
        read = read * rms_scale(read, norm_floor, True) * gain_ref[...]
        read_ref[seq : seq + 1, h * head : (h + 1) * head] = read


def vmem():
    return pl.BlockSpec(memory_space=pltpu.VMEM)


def smem():
    return pl.BlockSpec(memory_space=pltpu.SMEM)


def kernel(body, outputs, kinds, args, scratch=(), limit=16):
    given = {"s": smem, "v": vmem, "p": vmem, "h": lambda: pl.BlockSpec(memory_space=pl.ANY)}
    placed = [
        arg
        if kind == "s"
        else pltpu.with_memory_space_constraint(arg, pltpu.VMEM if kind == "p" else pltpu.HBM)
        for kind, arg in zip(kinds, args, strict=True)
    ]
    plain = lambda out: pltpu.HBM(out.shape, out.dtype)
    return pl.pallas_call(
        body,
        out_shape=tuple(out if kind == "p" else plain(out) for kind, out in outputs),
        in_specs=[given[kind]() for kind in kinds],
        out_specs=tuple(given[kind]() for kind, _ in outputs),
        scratch_shapes=list(scratch),
        compiler_params=pltpu.CompilerParams(vmem_limit_bytes=limit * 1024 * 1024),
    )(*placed)


def shift(value, axis, by):
    length = lax.axis_size(axis)
    return lax.ppermute(value, axis, [(at, (at + by) % length) for at in range(length)])


def shards(
    tokens, query_weight, key_weight, value_weight, gate_weight, beta_weight, decay_weight,
    beta_bias, rate_log, out_gain, new_query, new_key, new_value, new_beta, new_decay,
):
    _, span, depth = tokens.shape
    head = out_gain.shape[0]
    half = head // 2
    wide = 256
    width = query_weight.shape[1]
    rows = head + half + PACK
    on, dma = pltpu.VMEM, pltpu.SemaphoreType.DMA
    depth = tokens.shape[2]
    swap = lambda value: shift(value, "c", 1)
    tokens_c = swap(tokens)
    first, second = tokens[0], tokens[1]
    up0 = shift(first, "y", 1)
    down1 = shift(second, "y", -1)
    tokens_c, first, second = lax.optimization_barrier((tokens_c, first, second))
    up1 = shift(second, "y", 1)
    down0 = shift(first, "y", -1)
    early_c, up0, down1 = lax.optimization_barrier((tokens_c, up0, down1))
    sums = [("p", on((2 * span, 2 * width), f32)), ("p", on((2 * span, head), f32))]
    early = kernel(
        early_kernel,
        sums + [("p", on((6 * depth, 2 * width), bf16)), ("p", on((PACK, 8 * depth), bf16))],
        "hphhhh",
        (tokens, early_c, beta_weight.T, decay_weight.T, key_weight, value_weight),
        (
            on((2, span, depth), bf16),
            on((2 * depth, 2 * width), bf16),
            on((2, 2, 8 * depth), bf16),
            dma((2,)),
        ),
    )
    early = list(early)
    rest = early[2:]
    far0 = shift(up0, "y", 1)
    far1 = shift(down1, "y", -1)
    up1, down0, *early[:2] = lax.optimization_barrier((up1, down0, *early[:2]))
    near = (up0, up1, down0, down1)
    swapped = []
    for value in near:
        swapped.append(swap(value))
    middle = kernel(
        functools.partial(middle_kernel, 2), sums, "p" * 12, (*near, *swapped, *early[:2], *rest)
    )
    far0, far1, *middle = lax.optimization_barrier((far0, far1, *middle))
    last = [far0, far1, swap(far0), swap(far1)]
    middle = kernel(
        functools.partial(middle_kernel, 6), sums, "p" * 6, (far0, far1, *middle, *rest)
    )
    far_c0, far_c1, *middle = lax.optimization_barrier((*last[2:], *middle))
    last[2:] = [far_c0, far_c1]
    local_shapes = [
        on((8, rows, head), bf16),
        on((2 * span, width), bf16),
        on((4, span, head), bf16),
        on((4, span, head), bf16),
        on((2, wide, head), f32),
        on((2, head, wide), f32),
    ]
    send, *shared = kernel(
        local_kernel,
        [("h", out) for out in local_shapes],
        "ss" + "p" * 6,
        (beta_bias, rate_log, *last[2:], *middle, *rest),
        (*local_shapes, dma((6,))),
    )
    arrived = lax.all_to_all(send, NEAR, 0, 0, tiled=True)
    gain = out_gain[None]
    finals = [on((4, span, head), f32), on((4, span, head), bf16), on((4, span, head), f32)]
    local_out, reach, silu = kernel(
        window_kernel,
        [("v", out) for out in finals],
        "h" * 16 + "v" * 6,
        (tokens, tokens_c, *near, *swapped, *last, query_weight, gate_weight, gain, *shared),
        (
            on((8, 2, span, depth), bf16),
            on((8, depth, width), bf16),
            on((8, depth, width), bf16),
            dma((8,)),
        ),
        24,
    )
    arrived, local_out = lax.optimization_barrier((arrived, local_out))
    total, maps, adds, factors = kernel(
        compose_kernel,
        [
            ("p", on((rows, head), bf16)),
            ("p", on((7, head, head), bf16)),
            ("p", on((7, half, head), f32)),
            ("p", on((7, 8, head), f32)),
        ],
        "p",
        (arrived,),
    )
    others = [shift(total, "zh", by) for by in (1, 2, 3)]
    finals_in = kernel(
        load_kernel,
        [("p", out) for out in finals],
        "phhh",
        (total, local_out, reach, silu),
        (dma((3,)),),
    )
    *others, loaded = lax.optimization_barrier((*others, finals_in[0]))
    finals_in = (loaded, *finals_in[1:])
    (back,) = kernel(
        spread_kernel,
        [("p", on((8, half + PACK, head), bf16))],
        "ss" + "p" * 10,
        (
            new_beta, new_decay, total, *others, maps, adds, factors,
            new_query, new_key, new_value,
        ),
        (on((4, rows, head), bf16), on((head, head), f32), on((head, head), f32)),
    )
    returned = lax.all_to_all(back, NEAR, 0, 0, tiled=True)
    return kernel(
        finish_kernel,
        [
            ("v", on((2, span, width), bf16)),
            ("v", on((2, 2, 4, head), bf16)),
            ("v", on((2, width), f32)),
        ],
        "ppppp",
        (returned, *finals_in, gain),
    )


def solution(mesh):
    torus = Mesh(mesh.devices.reshape(4, 2, 4, 4, 2), AXES + ("y", "c"))
    sp, tp = AXES, ("y", "c")
    weight = P(None, tp)
    in_specs = (
        P(None, sp, tp),
        weight, weight, weight, weight, weight, weight,
        P(tp), P(tp), P(),
        P(None, tp, None), P(None, tp, None), P(None, tp, None),
        P(None, tp), P(None, tp),
    )
    out_specs = (P(None, sp, tp), P(None, tp, sp, None), P(None, tp))

    return jax.shard_map(
        shards, mesh=torus, in_specs=in_specs, out_specs=out_specs, check_vma=False
    )
```

```python
import functools

import jax
import jax.numpy as jnp
from jax import lax
from jax.experimental import pallas as pl
from jax.experimental.pallas import tpu as pltpu
from jax.sharding import Mesh
from jax.sharding import PartitionSpec as P


NEAR = ("zl", "x")
AXES = ("zh", "zl", "x")
PACK = 16
LANES = 128
unit_floor = 1.0
norm_floor = 0.001
bf16 = jnp.bfloat16
f32 = jnp.float32


def dot(left, right, dims=((1,), (0,))):
    return lax.dot_general(
        left.astype(bf16), right.astype(bf16), (dims, ((), ())), preferred_element_type=f32
    )


ROWS = ((1,), (1,))
COLS = ((0,), (0,))


def thirds(value):
    high = value.astype(bf16).astype(f32)
    rest = value - high
    mid = rest.astype(bf16).astype(f32)
    return high, mid, rest - mid


def iota(shape, dim):
    return lax.broadcasted_iota(jnp.int32, shape, dim)


def row_pack(values, width):
    rows = iota((PACK, width), 0)
    packed = jnp.zeros((PACK, width), f32)
    for at, value in enumerate(values):
        packed = jnp.where(rows == at, value, packed)
    return packed


def rms_scale(values, floor, mean):
    total = jnp.sum(values * values, axis=-1, keepdims=True)
    return lax.rsqrt((total / values.shape[-1] if mean else total) + floor)


def shard_index(ahead, swapped):
    core = lax.axis_index("c")
    core = 1 - core if swapped else core
    return lax.rem(lax.axis_index("y") + ahead, 4) * 2 + core


def first_row(slot, depth):
    return pl.multiple_of(shard_index(*slot) * depth, depth)


def joined(first, second):
    return jnp.concatenate([first[...], second[...]], axis=0)


def scalar_part(rows, stacked, slot):
    depth = rows.shape[-1]
    weight = stacked[:, pl.ds(first_row(slot, depth), depth)]
    weight = jnp.concatenate([weight, jnp.zeros((LANES - PACK, depth), bf16)], axis=0)
    return dot(rows, weight, ROWS)


SLOTS = (
    (0, False), (0, True), (3, False), (1, False), (3, True), (1, True), (2, False), (2, True),
)


def early_kernel(
    own, own_c, beta_w, decay_w, key_w, value_w, sum_ref, gate_ref, rest_ref, stacked_ref,
    token_buffer, weight_buffer, scalar_buffer, sems,
):
    depth = own.shape[-1]
    width = key_w.shape[-1]
    first = [pltpu.make_async_copy(own, token_buffer, sems.at[0])]
    for at, weight in enumerate((beta_w, decay_w)):
        first.append(pltpu.make_async_copy(weight, scalar_buffer.at[at], sems.at[0]))
    later = []
    for at, slot in enumerate(SLOTS):
        start = first_row(slot, depth)
        for side, weight in enumerate((key_w, value_w)):
            lanes = pl.ds(side * width, width)
            source = weight.at[pl.ds(start, depth), :]
            if at < 2:
                to = weight_buffer.at[pl.ds(at * depth, depth), lanes]
                first.append(pltpu.make_async_copy(source, to, sems.at[0]))
            else:
                to = rest_ref.at[pl.ds((at - 2) * depth, depth), lanes]
                later.append(pltpu.make_async_copy(source, to, sems.at[1]))
    for copy in first + later:
        copy.start()
    for copy in first:
        copy.wait()
    rows = [scalar_buffer[at, h : h + 1, :].astype(f32) for at in range(2) for h in range(2)]
    stacked_ref[...] = row_pack(rows, stacked_ref.shape[-1]).astype(bf16)
    total = gates = 0.0
    for at, piece in enumerate((token_buffer, own_c)):
        rows = piece[...].reshape(-1, depth)
        total = total + dot(rows, weight_buffer[at * depth : (at + 1) * depth, :])
        gates = gates + scalar_part(rows, stacked_ref, SLOTS[at])
    sum_ref[...] = total
    gate_ref[...] = gates
    for copy in later:
        copy.wait()


def add_pieces(pieces, from_slot, rest, stacked, total, gates):
    for at in range(len(pieces) // 2):
        rows = joined(*pieces[2 * at : 2 * at + 2])
        depth = rows.shape[-1]
        slot = from_slot + at
        total = total + dot(rows, rest[(slot - 2) * depth : (slot - 1) * depth, :])
        gates = gates + scalar_part(rows, stacked, SLOTS[slot])
    return total, gates


def middle_kernel(first_slot, *refs):
    pieces, (sum_in, gate_in, rest, stacked, sum_ref, gate_ref) = refs[:-6], refs[-6:]
    total, gates = add_pieces(pieces, first_slot, rest, stacked, sum_in[...], gate_in[...])
    sum_ref[...] = total
    gate_ref[...] = gates


def lane_pair(ref, first):
    lanes = iota((1, LANES), 1)
    return jnp.where(lanes == first, ref[0], jnp.where(lanes == first + 1, ref[1], 0.0))


def local_kernel(bias_ref, rate_ref, *refs):
    pieces, (sum_in, gate_in, rest, stacked) = refs[:2], refs[2:6]
    outputs, buffers, sems = refs[6:12], refs[12:18], refs[18]
    send_ref, key_ref, fresh_ref, carry_ref, cols_ref, rows_ref = buffers
    copies = []

    def give(at, part=None):
        source, to = buffers[at], outputs[at]
        if part is not None:
            source, to = source.at[part], to.at[part]
        copies.append(pltpu.make_async_copy(source, to, sems.at[at]))
        copies[-1].start()

    span = pieces[0].shape[0]
    head = send_ref.shape[-1]
    total, gates = add_pieces(pieces, 7, rest, stacked, sum_in[...], gate_in[...])
    width = total.shape[-1] // 2
    key_rows = total[:, :width].astype(bf16)
    value_rows = total[:, width:].astype(bf16)
    key_ref[...] = key_rows
    give(1)
    strength = jax.nn.sigmoid(gates + lane_pair(bias_ref, 0))
    decays = -jnp.exp(lane_pair(rate_ref, 2)) * jax.nn.softplus(gates)
    wide = cols_ref.shape[1]
    lanes = iota((wide, head), 1)
    causal_wide = (iota((wide, wide), 0) >= iota((wide, wide), 1)).astype(bf16)
    for seq in range(2):
        take = slice(seq * span, (seq + 1) * span)
        padded = jnp.concatenate([decays[take], jnp.zeros((wide - span, head), f32)], axis=0)
        cumulative = sum(dot(causal_wide, part) for part in thirds(padded))
        table = jnp.where((lanes == 2) | (lanes == 3), cumulative, 0.0)
        for h in range(2):
            keys = key_rows[take, h * head : (h + 1) * head].astype(f32)
            unit = jnp.concatenate(
                [rms_scale(keys, unit_floor, False), jnp.zeros((wide - span, 1), f32)], axis=0
            )
            beta = jnp.concatenate(
                [strength[take, h : h + 1], jnp.zeros((wide - span, 1), f32)], axis=0
            )
            table = jnp.where(lanes == h, beta, table)
            table = jnp.where(lanes == 4 + h, unit, table)
        cols_ref[seq] = table
        rows_ref[seq] = table.T
    give(4)
    give(5)
    t = iota((span, span), 0)
    s = iota((span, span), 1)
    apart = t ^ s
    lower, inverse = [], []
    for pair in range(4):
        seq, h = divmod(pair, 2)
        keys = key_rows[seq * span : (seq + 1) * span, h * head : (h + 1) * head]
        col = lambda at: cols_ref[seq, :span, at + h : at + h + 1]
        row = lambda at: rows_ref[seq, at + h : at + h + 1, :span]
        spread = jnp.where(t >= s, col(2) - row(2), 0.0)
        alike = dot(keys, keys, ROWS) * (col(0) * col(4)) * row(4) * jnp.exp(spread)
        lower.append(jnp.where(t > s, alike, 0.0))
        inverse.append(jnp.where(apart < 2, lower[pair], 0.0))
    size = 2
    while size < span:
        mask = (apart >= size) & (apart < 2 * size)
        steps = []
        for pair in range(4):
            block = jnp.where(mask, lower[pair], 0.0)
            steps.append(block - dot(block, inverse[pair]))
        for pair in range(4):
            inverse[pair] = inverse[pair] + steps[pair] - dot(inverse[pair], steps[pair])
        size *= 2
    for pair in range(4):
        seq, h = divmod(pair, 2)
        take = slice(seq * span, (seq + 1) * span)
        keys = key_rows[take, h * head : (h + 1) * head]
        values = value_rows[take, h * head : (h + 1) * head]
        col = lambda at: cols_ref[seq, :span, at + h : at + h + 1]
        row = lambda at: rows_ref[seq, at + h : at + h + 1, :span]
        fresh = col(0) * values.astype(f32) - dot(inverse[pair] * row(0), values)
        carry = (col(0) * col(4) * jnp.exp(col(2))) * keys.astype(f32) - dot(
            inverse[pair] * (row(0) * row(4) * jnp.exp(row(2))), keys
        )
        last = cols_ref[seq, span - 1 : span, 2 + h : 3 + h]
        late = col(4) * jnp.exp(last - col(2))
        reach = dot(carry * late, keys, COLS)
        gain = dot(fresh * late, keys, COLS)
        fresh_ref[pair] = fresh.astype(bf16)
        carry_ref[pair] = carry.astype(bf16)
        factor = row_pack(thirds(jnp.broadcast_to(jnp.exp(last), (1, head))), head)
        half = head // 2
        for side in range(2):
            to = 2 * pair + side
            send_ref[to, :head, :] = reach.astype(bf16)
            send_ref[to, head : head + half, :] = gain[side * half : (side + 1) * half].astype(bf16)
            send_ref[to, head + half :, :] = factor.astype(bf16)
        give(0, pl.ds(2 * pair, 2))
    give(2)
    give(3)
    for copy in copies:
        copy.wait()


def window_kernel(*refs):
    pieces, refs = refs[:14], refs[14:]
    query_w, gate_w, gain_ref, key_ref, fresh_ref, carry_ref, cols_ref, rows_ref = refs[:8]
    out_ref, reach_ref, silu_ref, token_buffer, query_buffer, gate_buffer, sems = refs[8:]
    span, depth = token_buffer.shape[2:]
    head = fresh_ref.shape[-1]
    weights = ((query_w, query_buffer), (gate_w, gate_buffer))
    copies = []
    for at, slot in enumerate(SLOTS):
        if at < 2:
            parts = [(pieces[at], token_buffer.at[at])]
        else:
            parts = [(pieces[2 * at - 2 + seq], token_buffer.at[at, seq]) for seq in range(2)]
        for weight, buffer in weights:
            parts.append((weight.at[pl.ds(first_row(slot, depth), depth), :], buffer.at[at]))
        copies.append([pltpu.make_async_copy(a, b, sems.at[at]) for a, b in parts])
        for copy in copies[at]:
            copy.start()
    query_total = gate_total = 0.0
    for at in range(8):
        for copy in copies[at]:
            copy.wait()
        rows = token_buffer[at].reshape(-1, depth)
        query_total = query_total + dot(rows, query_buffer[at])
        gate_total = gate_total + dot(rows, gate_buffer[at])
    query_rows = query_total.astype(bf16)
    gate_rows = gate_total.astype(bf16).astype(f32)
    t = iota((span, span), 0)
    s = iota((span, span), 1)
    for pair in range(4):
        seq, h = divmod(pair, 2)
        take = slice(seq * span, (seq + 1) * span)
        part = slice(h * head, (h + 1) * head)
        col = lambda at: cols_ref[seq, :span, at + h : at + h + 1]
        row = lambda at: rows_ref[seq, at + h : at + h + 1, :span]
        queries = query_rows[take, part]
        unit = rms_scale(queries.astype(f32), unit_floor, False)
        spread = jnp.where(t >= s, col(2) - row(2), 0.0)
        scores = dot(queries, key_ref[take, part], ROWS) * unit * row(4) * jnp.exp(spread)
        scores = jnp.where(t >= s, scores, 0.0).astype(bf16)
        out_ref[pair] = dot(scores, fresh_ref[pair])
        reach = (unit * jnp.exp(col(2))) * queries.astype(f32) - dot(scores, carry_ref[pair])
        reach_ref[pair] = reach.astype(bf16)
        gate = gate_rows[take, part]
        silu_ref[pair] = gain_ref[...] * gate * jax.nn.sigmoid(gate)


def unpack_factor(block):
    block = block.astype(f32)
    return block[0:1] + block[1:2] + block[2:3]


def compose_kernel(in_ref, total_ref, maps_ref, adds_ref, factors_ref):
    count, rows, head = in_ref.shape
    body = rows - PACK

    def load(at):
        return in_ref[at, :body, :].astype(f32), unpack_factor(in_ref[at, body:, :])

    def join(first, second):
        both, factor = first
        later, later_factor = second
        tail = jnp.concatenate([factor * later[:head], later[head:]], axis=0)
        return later_factor * both - dot(both, later[:head]) + tail, factor * later_factor

    member = [load(at) for at in range(count)]
    upto = [None] * (count + 1)
    upto[1] = member[0]
    c23, c45, c67 = (join(member[at], member[at + 1]) for at in (2, 4, 6))
    upto[2] = join(member[0], member[1])
    c456 = join(c45, member[6])
    c4567 = join(c45, c67)
    upto[4] = join(upto[2], c23)
    upto[8] = join(upto[4], c4567)
    both, factor = upto[8]
    total_ref[:body, :] = both.astype(bf16)
    total_ref[body:, :] = row_pack(thirds(factor), head).astype(bf16)
    upto[3] = join(upto[2], member[2])
    upto[5] = join(upto[4], member[4])
    upto[6] = join(upto[4], c45)
    upto[7] = join(upto[4], c456)
    for at in range(1, count):
        both, factor = upto[at]
        maps_ref[at - 1] = both[:head].astype(bf16)
        adds_ref[at - 1] = both[head:]
        factors_ref[at - 1] = jnp.broadcast_to(factor, (8, head))


def spread_kernel(
    beta_ref, decay_ref, own, back1, back2, back3, maps_ref, adds_ref, factors_ref,
    query_ref, key_ref, value_ref, send_ref, groups_ref, wide_ref, turned_ref,
):
    _, head = own.shape
    half = head // 2
    far = lax.axis_index("zh")
    near = lax.axis_index("zl") * 4 + lax.axis_index("x")
    pair = near // 2
    side = near % 2
    seq, h = pair // 2, pair % 2

    def chosen(ref):
        total = jnp.zeros((1, head), f32)
        for at in range(4):
            row = ref[at // 2, at % 2 : at % 2 + 1, :].astype(f32)
            total = jnp.where(pair == at, row, total)
        return total

    for slot, ref in enumerate((own, back1, back2, back3)):
        groups_ref[slot] = ref[...]
    state = jnp.zeros((half, head), f32)
    begin = state
    for group in range(4):
        begin = jnp.where(far == group, state, begin)
        block = groups_ref[lax.rem(far - group + 4, 4)]
        added = block[head : head + half].astype(f32)
        if group:
            state = unpack_factor(block[head + half :]) * state - dot(state, block[:head]) + added
        else:
            state = added
    final = state.astype(bf16).astype(f32)
    wide_ref[...] = jnp.zeros((head, head), f32)
    wide_ref[pl.ds(pl.multiple_of(side * half, half), half), :] = final
    padded = wide_ref[...]
    turned_ref[...] = padded.T
    mine = turned_ref[pl.ds(pl.multiple_of(far * 32, 32), 32), :]
    query = chosen(query_ref)
    key = chosen(key_ref)
    query = query * rms_scale(query, unit_floor, False)
    key = key * rms_scale(key, unit_floor, False)
    hits = dot(row_pack(thirds(query) + thirds(key), head), padded, ROWS)
    recall = hits[0:1] + hits[1:2] + hits[2:3]
    retrieve = hits[3:4] + hits[4:5] + hits[5:6]
    intersect = jnp.sum(key * query, axis=-1, keepdims=True)
    fresh = chosen(value_ref) - decay_ref[seq, h] * retrieve
    read = decay_ref[seq, h] * recall + (beta_ref[seq, h] * intersect) * fresh
    read = jnp.where(iota((1, head), 1) // half == side, read, 0.0)
    zero = jnp.zeros((1, head), f32)
    extra = row_pack((zero, zero, zero, zero) + thirds(read), head)
    pick_row = iota((PACK, 32), 0)
    pick_col = iota((PACK, 32), 1)
    for member in range(8):
        if member:
            at = member - 1
            entry = factors_ref[at, 0:1, :] * begin - dot(begin, maps_ref[at]) + adds_ref[at]
        else:
            entry = begin
        send_ref[member, :half, :] = entry.astype(bf16)
        pick = ((pick_row < 4) & (pick_col == 4 * member + pick_row)).astype(bf16)
        send_ref[member, half:, :] = (dot(pick, mine) + extra).astype(bf16)


def load_kernel(_, *refs):
    count = len(refs) // 2
    sources, outputs, sems = refs[:count], refs[count : 2 * count], refs[2 * count]
    copies = [
        pltpu.make_async_copy(a, b, sems.at[at]) for at, (a, b) in enumerate(zip(sources, outputs))
    ]
    for copy in copies:
        copy.start()
    for copy in copies:
        copy.wait()


def finish_kernel(in_ref, out_ref, reach_ref, silu_ref, gain_ref, mixed_ref, cache_ref, read_ref):
    head = in_ref.shape[-1]
    half = head // 2
    for pair in range(4):
        seq, h = divmod(pair, 2)
        incoming = jnp.concatenate([in_ref[2 * pair, :half, :], in_ref[2 * pair + 1, :half, :]], 0)
        whole = out_ref[pair] + dot(reach_ref[pair], incoming, ROWS)
        mixed = whole * rms_scale(whole, norm_floor, True) * silu_ref[pair]
        mixed_ref[seq, :, h * head : (h + 1) * head] = mixed.astype(bf16)
        extra = in_ref[2 * pair, half:, :].astype(f32) + in_ref[2 * pair + 1, half:, :].astype(f32)
        cache_ref[seq, h] = extra[:4].astype(bf16)
        read = extra[4:5] + extra[5:6] + extra[6:7]
        read = read * rms_scale(read, norm_floor, True) * gain_ref[...]
        read_ref[seq : seq + 1, h * head : (h + 1) * head] = read


def vmem():
    return pl.BlockSpec(memory_space=pltpu.VMEM)


def smem():
    return pl.BlockSpec(memory_space=pltpu.SMEM)


def kernel(body, outputs, kinds, args, scratch=(), limit=16):
    given = {"s": smem, "v": vmem, "p": vmem, "h": lambda: pl.BlockSpec(memory_space=pl.ANY)}
    placed = [
        arg
        if kind == "s"
        else pltpu.with_memory_space_constraint(arg, pltpu.VMEM if kind == "p" else pltpu.HBM)
        for kind, arg in zip(kinds, args, strict=True)
    ]
    plain = lambda out: pltpu.HBM(out.shape, out.dtype)
    return pl.pallas_call(
        body,
        out_shape=tuple(out if kind == "p" else plain(out) for kind, out in outputs),
        in_specs=[given[kind]() for kind in kinds],
        out_specs=tuple(given[kind]() for kind, _ in outputs),
        scratch_shapes=list(scratch),
        compiler_params=pltpu.CompilerParams(vmem_limit_bytes=limit * 1024 * 1024),
    )(*placed)


def shift(value, axis, by):
    length = lax.axis_size(axis)
    return lax.ppermute(value, axis, [(at, (at + by) % length) for at in range(length)])


def shards(
    tokens, query_weight, key_weight, value_weight, gate_weight, beta_weight, decay_weight,
    beta_bias, rate_log, out_gain, new_query, new_key, new_value, new_beta, new_decay,
):
    _, span, depth = tokens.shape
    head = out_gain.shape[0]
    half = head // 2
    wide = 256
    width = query_weight.shape[1]
    rows = head + half + PACK
    on, dma = pltpu.VMEM, pltpu.SemaphoreType.DMA
    depth = tokens.shape[2]
    swap = lambda value: shift(value, "c", 1)
    tokens_c = swap(tokens)
    first, second = tokens[0], tokens[1]
    up0 = shift(first, "y", 1)
    down1 = shift(second, "y", -1)
    sums = [("p", on((2 * span, 2 * width), f32)), ("p", on((2 * span, head), f32))]
    early = kernel(
        early_kernel,
        sums + [("p", on((6 * depth, 2 * width), bf16)), ("p", on((PACK, 8 * depth), bf16))],
        "hphhhh",
        (tokens, tokens_c, beta_weight.T, decay_weight.T, key_weight, value_weight),
        (
            on((2, span, depth), bf16),
            on((2 * depth, 2 * width), bf16),
            on((2, 2, 8 * depth), bf16),
            dma((2,)),
        ),
    )
    early = list(early)
    first, second, *early[:2] = lax.optimization_barrier((first, second, *early[:2]))
    up1 = shift(second, "y", 1)
    down0 = shift(first, "y", -1)
    rest = early[2:]
    far0 = shift(up0, "y", 1)
    far1 = shift(down1, "y", -1)
    near = (up0, up1, down0, down1)
    swapped = []
    for value in near:
        swapped.append(swap(value))
    middle = kernel(
        functools.partial(middle_kernel, 2), sums, "p" * 12, (*near, *swapped, *early[:2], *rest)
    )
    far0, far1, *middle = lax.optimization_barrier((far0, far1, *middle))
    last = [far0, far1, swap(far0), swap(far1)]
    middle = kernel(
        functools.partial(middle_kernel, 6), sums, "p" * 6, (far0, far1, *middle, *rest)
    )
    far_c0, far_c1, *middle = lax.optimization_barrier((*last[2:], *middle))
    last[2:] = [far_c0, far_c1]
    local_shapes = [
        on((8, rows, head), bf16),
        on((2 * span, width), bf16),
        on((4, span, head), bf16),
        on((4, span, head), bf16),
        on((2, wide, head), f32),
        on((2, head, wide), f32),
    ]
    send, *shared = kernel(
        local_kernel,
        [("h", out) for out in local_shapes],
        "ss" + "p" * 6,
        (beta_bias, rate_log, *last[2:], *middle, *rest),
        (*local_shapes, dma((6,))),
    )
    arrived = lax.all_to_all(send, NEAR, 0, 0, tiled=True)
    gain = out_gain[None]
    finals = [on((4, span, head), f32), on((4, span, head), bf16), on((4, span, head), f32)]
    local_out, reach, silu = kernel(
        window_kernel,
        [("v", out) for out in finals],
        "h" * 16 + "v" * 6,
        (tokens, tokens_c, *near, *swapped, *last, query_weight, gate_weight, gain, *shared),
        (
            on((8, 2, span, depth), bf16),
            on((8, depth, width), bf16),
            on((8, depth, width), bf16),
            dma((8,)),
        ),
        24,
    )
    arrived, local_out = lax.optimization_barrier((arrived, local_out))
    total, maps, adds, factors = kernel(
        compose_kernel,
        [
            ("p", on((rows, head), bf16)),
            ("p", on((7, head, head), bf16)),
            ("p", on((7, half, head), f32)),
            ("p", on((7, 8, head), f32)),
        ],
        "p",
        (arrived,),
    )
    others = [shift(total, "zh", by) for by in (1, 2, 3)]
    finals_in = kernel(
        load_kernel,
        [("p", out) for out in finals],
        "phhh",
        (total, local_out, reach, silu),
        (dma((3,)),),
    )
    *others, loaded = lax.optimization_barrier((*others, finals_in[0]))
    finals_in = (loaded, *finals_in[1:])
    (back,) = kernel(
        spread_kernel,
        [("p", on((8, half + PACK, head), bf16))],
        "ss" + "p" * 10,
        (
            new_beta, new_decay, total, *others, maps, adds, factors,
            new_query, new_key, new_value,
        ),
        (on((4, rows, head), bf16), on((head, head), f32), on((head, head), f32)),
    )
    returned = lax.all_to_all(back, NEAR, 0, 0, tiled=True)
    return kernel(
        finish_kernel,
        [
            ("v", on((2, span, width), bf16)),
            ("v", on((2, 2, 4, head), bf16)),
            ("v", on((2, width), f32)),
        ],
        "ppppp",
        (returned, *finals_in, gain),
    )


def solution(mesh):
    torus = Mesh(mesh.devices.reshape(4, 2, 4, 4, 2), AXES + ("y", "c"))
    sp, tp = AXES, ("y", "c")
    weight = P(None, tp)
    in_specs = (
        P(None, sp, tp),
        weight, weight, weight, weight, weight, weight,
        P(tp), P(tp), P(),
        P(None, tp, None), P(None, tp, None), P(None, tp, None),
        P(None, tp), P(None, tp),
    )
    out_specs = (P(None, sp, tp), P(None, tp, sp, None), P(None, tp))

    return jax.shard_map(
        shards, mesh=torus, in_specs=in_specs, out_specs=out_specs, check_vma=False
    )
```

```python
import functools

import jax
import jax.numpy as jnp
from jax import lax
from jax.experimental import pallas as pl
from jax.experimental.pallas import tpu as pltpu
from jax.sharding import Mesh
from jax.sharding import PartitionSpec as P


NEAR = ("zl", "x")
AXES = ("zh", "zl", "x")
PACK = 16
LANES = 128
unit_floor = 1.0
norm_floor = 0.001
bf16 = jnp.bfloat16
f32 = jnp.float32


def dot(left, right, dims=((1,), (0,))):
    return lax.dot_general(
        left.astype(bf16), right.astype(bf16), (dims, ((), ())), preferred_element_type=f32
    )


ROWS = ((1,), (1,))
COLS = ((0,), (0,))


def thirds(value):
    high = value.astype(bf16).astype(f32)
    rest = value - high
    mid = rest.astype(bf16).astype(f32)
    return high, mid, rest - mid


def iota(shape, dim):
    return lax.broadcasted_iota(jnp.int32, shape, dim)


def row_pack(values, width):
    rows = iota((PACK, width), 0)
    packed = jnp.zeros((PACK, width), f32)
    for at, value in enumerate(values):
        packed = jnp.where(rows == at, value, packed)
    return packed


def rms_scale(values, floor, mean):
    total = jnp.sum(values * values, axis=-1, keepdims=True)
    return lax.rsqrt((total / values.shape[-1] if mean else total) + floor)


def shard_index(ahead, swapped):
    core = lax.axis_index("c")
    core = 1 - core if swapped else core
    return lax.rem(lax.axis_index("y") + ahead, 4) * 2 + core


def first_row(slot, depth):
    return pl.multiple_of(shard_index(*slot) * depth, depth)


def joined(first, second):
    return jnp.concatenate([first[...], second[...]], axis=0)


def scalar_part(rows, stacked, slot):
    depth = rows.shape[-1]
    weight = stacked[:, pl.ds(first_row(slot, depth), depth)]
    weight = jnp.concatenate([weight, jnp.zeros((LANES - PACK, depth), bf16)], axis=0)
    return dot(rows, weight, ROWS)


SLOTS = (
    (0, False), (0, True), (3, False), (1, False), (3, True), (1, True), (2, False), (2, True),
)


def early_kernel(
    own, own_c, beta_w, decay_w, key_w, value_w, sum_ref, gate_ref, rest_ref, stacked_ref,
    token_buffer, weight_buffer, scalar_buffer, sems,
):
    depth = own.shape[-1]
    width = key_w.shape[-1]
    first = [pltpu.make_async_copy(own, token_buffer, sems.at[0])]
    for at, weight in enumerate((beta_w, decay_w)):
        first.append(pltpu.make_async_copy(weight, scalar_buffer.at[at], sems.at[0]))
    later = []
    for at, slot in enumerate(SLOTS):
        start = first_row(slot, depth)
        for side, weight in enumerate((key_w, value_w)):
            lanes = pl.ds(side * width, width)
            source = weight.at[pl.ds(start, depth), :]
            if at < 2:
                to = weight_buffer.at[pl.ds(at * depth, depth), lanes]
                first.append(pltpu.make_async_copy(source, to, sems.at[0]))
            else:
                to = rest_ref.at[pl.ds((at - 2) * depth, depth), lanes]
                later.append(pltpu.make_async_copy(source, to, sems.at[1]))
    for copy in first + later:
        copy.start()
    for copy in first:
        copy.wait()
    rows = [scalar_buffer[at, h : h + 1, :].astype(f32) for at in range(2) for h in range(2)]
    stacked_ref[...] = row_pack(rows, stacked_ref.shape[-1]).astype(bf16)
    total = gates = 0.0
    for at, piece in enumerate((token_buffer, own_c)):
        rows = piece[...].reshape(-1, depth)
        total = total + dot(rows, weight_buffer[at * depth : (at + 1) * depth, :])
        gates = gates + scalar_part(rows, stacked_ref, SLOTS[at])
    sum_ref[...] = total
    gate_ref[...] = gates
    for copy in later:
        copy.wait()


def add_pieces(pieces, from_slot, rest, stacked, total, gates):
    for at in range(len(pieces) // 2):
        rows = joined(*pieces[2 * at : 2 * at + 2])
        depth = rows.shape[-1]
        slot = from_slot + at
        total = total + dot(rows, rest[(slot - 2) * depth : (slot - 1) * depth, :])
        gates = gates + scalar_part(rows, stacked, SLOTS[slot])
    return total, gates


def middle_kernel(first_slot, *refs):
    pieces, (sum_in, gate_in, rest, stacked, sum_ref, gate_ref) = refs[:-6], refs[-6:]
    total, gates = add_pieces(pieces, first_slot, rest, stacked, sum_in[...], gate_in[...])
    sum_ref[...] = total
    gate_ref[...] = gates


def lane_pair(ref, first):
    lanes = iota((1, LANES), 1)
    pair = ref[...]
    return jnp.where(
        lanes == first, pair[:, 0:1], jnp.where(lanes == first + 1, pair[:, 1:2], 0.0)
    )


def local_kernel(bias_ref, rate_ref, *refs):
    pieces, (sum_in, gate_in, rest, stacked) = refs[:2], refs[2:6]
    outputs, buffers, sems = refs[6:12], refs[12:18], refs[18]
    send_ref, key_ref, fresh_ref, carry_ref, cols_ref, rows_ref = buffers
    copies = []

    def give(at, part=None):
        source, to = buffers[at], outputs[at]
        if part is not None:
            source, to = source.at[part], to.at[part]
        copies.append(pltpu.make_async_copy(source, to, sems.at[at]))
        copies[-1].start()

    span = pieces[0].shape[0]
    head = send_ref.shape[-1]
    total, gates = add_pieces(pieces, 7, rest, stacked, sum_in[...], gate_in[...])
    width = total.shape[-1] // 2
    key_rows = total[:, :width].astype(bf16)
    value_rows = total[:, width:].astype(bf16)
    key_ref[...] = key_rows
    give(1)
    strength = jax.nn.sigmoid(gates + lane_pair(bias_ref, 0))
    decays = -jnp.exp(lane_pair(rate_ref, 2)) * jax.nn.softplus(gates)
    wide = cols_ref.shape[1]
    lanes = iota((wide, head), 1)
    causal_wide = (iota((wide, wide), 0) >= iota((wide, wide), 1)).astype(bf16)
    for seq in range(2):
        take = slice(seq * span, (seq + 1) * span)
        padded = jnp.concatenate([decays[take], jnp.zeros((wide - span, head), f32)], axis=0)
        cumulative = sum(dot(causal_wide, part) for part in thirds(padded))
        table = jnp.where((lanes == 2) | (lanes == 3), cumulative, 0.0)
        for h in range(2):
            keys = key_rows[take, h * head : (h + 1) * head].astype(f32)
            unit = jnp.concatenate(
                [rms_scale(keys, unit_floor, False), jnp.zeros((wide - span, 1), f32)], axis=0
            )
            beta = jnp.concatenate(
                [strength[take, h : h + 1], jnp.zeros((wide - span, 1), f32)], axis=0
            )
            table = jnp.where(lanes == h, beta, table)
            table = jnp.where(lanes == 4 + h, unit, table)
        cols_ref[seq] = table
        rows_ref[seq] = table.T
    give(4)
    give(5)
    half = head // 2
    t = iota((head, head), 0)
    s = iota((head, head), 1)
    apart = t ^ s
    upper, lower = slice(0, head), slice(head, span)
    blocks = []
    for pair in range(4):
        seq, h = divmod(pair, 2)
        keys = key_rows[seq * span : (seq + 1) * span, h * head : (h + 1) * head]

        def alike(of, with_, mask):
            col = lambda at: cols_ref[seq, of, at + h : at + h + 1]
            row = lambda at: rows_ref[seq, at + h : at + h + 1, with_]
            spread = col(2) - row(2)
            if mask is not None:
                spread = jnp.where(mask, spread, 0.0)
            product = dot(keys[of], keys[with_], ROWS)
            product = product * (col(0) * col(4)) * row(4) * jnp.exp(spread)
            return product if mask is None else jnp.where(mask, product, 0.0)

        def started(block):
            size = block.shape[0]
            near, same = apart[:size, :size] < 2, (t == s)[:size, :size]
            return jnp.where(same, 1.0, jnp.where(near, -block, 0.0)).astype(bf16)

        first = alike(upper, upper, t > s)
        second = alike(lower, lower, (t > s)[:half, :half])
        across = alike(lower, upper, None)
        blocks.append(
            [first.astype(bf16), second.astype(bf16), across.astype(bf16)]
            + [started(first), started(second)]
        )
    size = 2
    while size < half:
        mask = jnp.where((apart >= size) & (apart < 2 * size), 1.0, 0.0).astype(bf16)
        steps = []
        for first, second, _, x_first, x_second in blocks:
            step = dot(first * mask, x_first).astype(bf16)
            steps.append((step, dot(second * mask[:half, :half], x_second).astype(bf16)))
        for block, (step_first, step_second) in zip(blocks, steps):
            block[3] = block[3] - dot(block[3], step_first).astype(bf16)
            block[4] = block[4] - dot(block[4], step_second).astype(bf16)
        size *= 2
    left = jnp.where(iota((half, head), 1) < half, 1.0, 0.0).astype(bf16)
    blank = jnp.zeros((half, head), bf16)
    steps = [dot(block[0][half:] * left, block[3]).astype(bf16) for block in blocks]
    for block, step in zip(blocks, steps):
        change = dot(block[3][half:], jnp.concatenate([blank, step], axis=0)).astype(bf16)
        block[3] = jnp.concatenate([block[3][:half], block[3][half:] - change], axis=0)
    steps = [dot(block[2], block[3]).astype(bf16) for block in blocks]
    for pair in range(4):
        seq, h = divmod(pair, 2)
        take = slice(seq * span, (seq + 1) * span)
        keys = key_rows[take, h * head : (h + 1) * head]
        values = value_rows[take, h * head : (h + 1) * head]
        col = lambda at: cols_ref[seq, :span, at + h : at + h + 1]
        row = lambda at: rows_ref[seq, at + h : at + h + 1, :span]
        off_first = jnp.where(t == s, 0.0, blocks[pair][3].astype(f32))
        off_second = jnp.where((t == s)[:half, :half], 0.0, blocks[pair][4].astype(f32))
        off_across = -dot(blocks[pair][4], steps[pair])

        def applied(weight, right):
            top = dot(off_first * weight[:, upper], right[upper])
            low = dot(off_across * weight[:, upper], right[upper])
            low = low + dot(off_second * weight[:, lower], right[lower])
            return jnp.concatenate([top, low], axis=0)

        fresh = col(0) * values.astype(f32) + applied(row(0), values)
        carry = (col(0) * col(4) * jnp.exp(col(2))) * keys.astype(f32) + applied(
            row(0) * row(4) * jnp.exp(row(2)), keys
        )
        last = cols_ref[seq, span - 1 : span, 2 + h : 3 + h]
        late = col(4) * jnp.exp(last - col(2))
        reach = dot(carry * late, keys, COLS)
        gain = dot(fresh * late, keys, COLS)
        fresh_ref[pair] = fresh.astype(bf16)
        carry_ref[pair] = carry.astype(bf16)
        factor = row_pack(thirds(jnp.broadcast_to(jnp.exp(last), (1, head))), head)
        for side in range(2):
            to = 2 * pair + side
            send_ref[to, :head, :] = reach.astype(bf16)
            send_ref[to, head : head + half, :] = gain[side * half : (side + 1) * half].astype(bf16)
            send_ref[to, head + half :, :] = factor.astype(bf16)
        give(0, pl.ds(2 * pair, 2))
    give(2)
    give(3)
    for copy in copies:
        copy.wait()


def window_kernel(*refs):
    pieces, refs = refs[:14], refs[14:]
    query_w, gate_w, gain_ref, key_ref, fresh_ref, carry_ref, cols_ref, rows_ref = refs[:8]
    out_ref, reach_ref, silu_ref, token_buffer, query_buffer, gate_buffer, sems = refs[8:]
    span, depth = token_buffer.shape[2:]
    head = fresh_ref.shape[-1]
    weights = ((query_w, query_buffer), (gate_w, gate_buffer))
    copies = []
    for at, slot in enumerate(SLOTS):
        if at < 2:
            parts = [(pieces[at], token_buffer.at[at])]
        else:
            parts = [(pieces[2 * at - 2 + seq], token_buffer.at[at, seq]) for seq in range(2)]
        for weight, buffer in weights:
            parts.append((weight.at[pl.ds(first_row(slot, depth), depth), :], buffer.at[at]))
        copies.append([pltpu.make_async_copy(a, b, sems.at[at]) for a, b in parts])
        for copy in copies[at]:
            copy.start()
    query_total = gate_total = 0.0
    for at in range(8):
        for copy in copies[at]:
            copy.wait()
        rows = token_buffer[at].reshape(-1, depth)
        query_total = query_total + dot(rows, query_buffer[at])
        gate_total = gate_total + dot(rows, gate_buffer[at])
    query_rows = query_total.astype(bf16)
    gate_rows = gate_total.astype(bf16).astype(f32)
    t = iota((span, span), 0)
    s = iota((span, span), 1)
    for pair in range(4):
        seq, h = divmod(pair, 2)
        take = slice(seq * span, (seq + 1) * span)
        part = slice(h * head, (h + 1) * head)
        col = lambda at: cols_ref[seq, :span, at + h : at + h + 1]
        row = lambda at: rows_ref[seq, at + h : at + h + 1, :span]
        queries = query_rows[take, part]
        unit = rms_scale(queries.astype(f32), unit_floor, False)
        spread = jnp.where(t >= s, col(2) - row(2), 0.0)
        scores = dot(queries, key_ref[take, part], ROWS) * unit * row(4) * jnp.exp(spread)
        scores = jnp.where(t >= s, scores, 0.0).astype(bf16)
        out_ref[pair] = dot(scores, fresh_ref[pair])
        reach = (unit * jnp.exp(col(2))) * queries.astype(f32) - dot(scores, carry_ref[pair])
        reach_ref[pair] = reach.astype(bf16)
        gate = gate_rows[take, part]
        silu_ref[pair] = gain_ref[...] * gate * jax.nn.sigmoid(gate)


def unpack_factor(block):
    block = block.astype(f32)
    return block[0:1] + block[1:2] + block[2:3]


def compose_kernel(in_ref, total_ref, maps_ref, adds_ref, factors_ref):
    count, rows, head = in_ref.shape
    body = rows - PACK

    def load(at):
        return in_ref[at, :body, :].astype(f32), unpack_factor(in_ref[at, body:, :])

    def join(first, second):
        both, factor = first
        later, later_factor = second
        tail = jnp.concatenate([factor * later[:head], later[head:]], axis=0)
        return later_factor * both - dot(both, later[:head]) + tail, factor * later_factor

    member = [load(at) for at in range(count)]
    upto = [None] * (count + 1)
    upto[1] = member[0]
    c23, c45, c67 = (join(member[at], member[at + 1]) for at in (2, 4, 6))
    upto[2] = join(member[0], member[1])
    c456 = join(c45, member[6])
    c4567 = join(c45, c67)
    upto[4] = join(upto[2], c23)
    upto[8] = join(upto[4], c4567)
    both, factor = upto[8]
    total_ref[:body, :] = both.astype(bf16)
    total_ref[body:, :] = row_pack(thirds(factor), head).astype(bf16)
    upto[3] = join(upto[2], member[2])
    upto[5] = join(upto[4], member[4])
    upto[6] = join(upto[4], c45)
    upto[7] = join(upto[4], c456)
    for at in range(1, count):
        both, factor = upto[at]
        maps_ref[at - 1] = both[:head].astype(bf16)
        adds_ref[at - 1] = both[head:]
        factors_ref[at - 1] = jnp.broadcast_to(factor, (8, head))


def spread_kernel(
    beta_ref, decay_ref, own, back1, back2, back3, maps_ref, adds_ref, factors_ref,
    query_ref, key_ref, value_ref, send_ref, groups_ref, wide_ref, turned_ref,
):
    _, head = own.shape
    half = head // 2
    far = lax.axis_index("zh")
    near = lax.axis_index("zl") * 4 + lax.axis_index("x")
    pair = near // 2
    side = near % 2

    def scalar(ref):
        total = jnp.zeros((1, 1), f32)
        for at in range(4):
            entry = ref[at // 2 : at // 2 + 1, at % 2 : at % 2 + 1]
            total = jnp.where(pair == at, entry, total)
        return total

    def chosen(ref):
        total = jnp.zeros((1, head), f32)
        for at in range(4):
            row = ref[at // 2, at % 2 : at % 2 + 1, :].astype(f32)
            total = jnp.where(pair == at, row, total)
        return total

    for slot, ref in enumerate((own, back1, back2, back3)):
        groups_ref[slot] = ref[...]
    state = jnp.zeros((half, head), f32)
    begin = state
    for group in range(4):
        begin = jnp.where(far == group, state, begin)
        block = groups_ref[lax.bitwise_xor(far, group)]
        added = block[head : head + half].astype(f32)
        if group:
            state = unpack_factor(block[head + half :]) * state - dot(state, block[:head]) + added
        else:
            state = added
    final = state.astype(bf16).astype(f32)
    wide_ref[...] = jnp.zeros((head, head), f32)
    wide_ref[pl.ds(pl.multiple_of(side * half, half), half), :] = final
    padded = wide_ref[...]
    turned_ref[...] = padded.T
    mine = turned_ref[pl.ds(pl.multiple_of(far * 32, 32), 32), :]
    query = chosen(query_ref)
    key = chosen(key_ref)
    query = query * rms_scale(query, unit_floor, False)
    key = key * rms_scale(key, unit_floor, False)
    hits = dot(row_pack(thirds(query) + thirds(key), head), padded, ROWS)
    recall = hits[0:1] + hits[1:2] + hits[2:3]
    retrieve = hits[3:4] + hits[4:5] + hits[5:6]
    decay = scalar(decay_ref)
    intersect = jnp.sum(key * query, axis=-1, keepdims=True)
    fresh = chosen(value_ref) - decay * retrieve
    read = decay * recall + (scalar(beta_ref) * intersect) * fresh
    read = jnp.where(iota((1, head), 1) // half == side, read, 0.0)
    zero = jnp.zeros((1, head), f32)
    extra = row_pack((zero, zero, zero, zero) + thirds(read), head)
    pick_row = iota((PACK, 32), 0)
    pick_col = iota((PACK, 32), 1)
    for member in range(8):
        if member:
            at = member - 1
            entry = factors_ref[at, 0:1, :] * begin - dot(begin, maps_ref[at]) + adds_ref[at]
        else:
            entry = begin
        send_ref[member, :half, :] = entry.astype(bf16)
        pick = ((pick_row < 4) & (pick_col == 4 * member + pick_row)).astype(bf16)
        send_ref[member, half:, :] = (dot(pick, mine) + extra).astype(bf16)


def load_kernel(_, *refs):
    count = len(refs) // 2
    sources, outputs, sems = refs[:count], refs[count : 2 * count], refs[2 * count]
    copies = [
        pltpu.make_async_copy(a, b, sems.at[at]) for at, (a, b) in enumerate(zip(sources, outputs))
    ]
    for copy in copies:
        copy.start()
    for copy in copies:
        copy.wait()


def finish_kernel(in_ref, out_ref, reach_ref, silu_ref, gain_ref, mixed_ref, cache_ref, read_ref):
    head = in_ref.shape[-1]
    half = head // 2
    for pair in range(4):
        seq, h = divmod(pair, 2)
        incoming = jnp.concatenate([in_ref[2 * pair, :half, :], in_ref[2 * pair + 1, :half, :]], 0)
        whole = out_ref[pair] + dot(reach_ref[pair], incoming, ROWS)
        mixed = whole * rms_scale(whole, norm_floor, True) * silu_ref[pair]
        mixed_ref[seq, :, h * head : (h + 1) * head] = mixed.astype(bf16)
        extra = in_ref[2 * pair, half:, :].astype(f32) + in_ref[2 * pair + 1, half:, :].astype(f32)
        cache_ref[seq, h] = extra[:4].astype(bf16)
        read = extra[4:5] + extra[5:6] + extra[6:7]
        read = read * rms_scale(read, norm_floor, True) * gain_ref[...]
        read_ref[seq : seq + 1, h * head : (h + 1) * head] = read


def vmem():
    return pl.BlockSpec(memory_space=pltpu.VMEM)


def smem():
    return pl.BlockSpec(memory_space=pltpu.SMEM)


def kernel(body, outputs, kinds, args, scratch=(), limit=16):
    given = {"s": smem, "v": vmem, "p": vmem, "h": lambda: pl.BlockSpec(memory_space=pl.ANY)}
    placed = [
        arg
        if kind == "s"
        else pltpu.with_memory_space_constraint(arg, pltpu.VMEM if kind == "p" else pltpu.HBM)
        for kind, arg in zip(kinds, args, strict=True)
    ]
    plain = lambda out: pltpu.HBM(out.shape, out.dtype)
    return pl.pallas_call(
        body,
        out_shape=tuple(out if kind == "p" else plain(out) for kind, out in outputs),
        in_specs=[given[kind]() for kind in kinds],
        out_specs=tuple(given[kind]() for kind, _ in outputs),
        scratch_shapes=list(scratch),
        compiler_params=pltpu.CompilerParams(vmem_limit_bytes=limit * 1024 * 1024),
    )(*placed)


def shift(value, axis, by):
    length = lax.axis_size(axis)
    return lax.ppermute(value, axis, [(at, (at + by) % length) for at in range(length)])


def shards(
    tokens, query_weight, key_weight, value_weight, gate_weight, beta_weight, decay_weight,
    beta_bias, rate_log, out_gain, new_query, new_key, new_value, new_beta, new_decay,
):
    _, span, depth = tokens.shape
    head = out_gain.shape[0]
    half = head // 2
    wide = 256
    width = query_weight.shape[1]
    rows = head + half + PACK
    on, dma = pltpu.VMEM, pltpu.SemaphoreType.DMA
    depth = tokens.shape[2]
    swap = lambda value: shift(value, "c", 1)
    tokens_c = swap(tokens)
    first, second = tokens[0], tokens[1]
    up0 = shift(first, "y", 1)
    down1 = shift(second, "y", -1)
    sums = [("p", on((2 * span, 2 * width), f32)), ("p", on((2 * span, head), f32))]
    early = kernel(
        early_kernel,
        sums + [("p", on((6 * depth, 2 * width), bf16)), ("p", on((PACK, 8 * depth), bf16))],
        "hphhhh",
        (tokens, tokens_c, beta_weight.T, decay_weight.T, key_weight, value_weight),
        (
            on((2, span, depth), bf16),
            on((2 * depth, 2 * width), bf16),
            on((2, 2, 8 * depth), bf16),
            dma((2,)),
        ),
    )
    early = list(early)
    first, second, *early[:2] = lax.optimization_barrier((first, second, *early[:2]))
    up1 = shift(second, "y", 1)
    down0 = shift(first, "y", -1)
    rest = early[2:]
    far0 = shift(up0, "y", 1)
    far1 = shift(down1, "y", -1)
    near = (up0, up1, down0, down1)
    swapped = []
    for value in near:
        swapped.append(swap(value))
    middle = kernel(
        functools.partial(middle_kernel, 2), sums, "p" * 12, (*near, *swapped, *early[:2], *rest)
    )
    far0, far1, *middle = lax.optimization_barrier((far0, far1, *middle))
    last = [far0, far1, swap(far0), swap(far1)]
    middle = kernel(
        functools.partial(middle_kernel, 6), sums, "p" * 6, (far0, far1, *middle, *rest)
    )
    far_c0, far_c1, *middle = lax.optimization_barrier((*last[2:], *middle))
    last[2:] = [far_c0, far_c1]
    local_shapes = [
        on((8, rows, head), bf16),
        on((2 * span, width), bf16),
        on((4, span, head), bf16),
        on((4, span, head), bf16),
        on((2, wide, head), f32),
        on((2, head, wide), f32),
    ]
    send, *shared = kernel(
        local_kernel,
        [("h", out) for out in local_shapes],
        "p" * 8,
        (beta_bias[None], rate_log[None], *last[2:], *middle, *rest),
        (*local_shapes, dma((6,))),
    )
    arrived = lax.all_to_all(send, NEAR, 0, 0, tiled=True)
    gain = out_gain[None]
    finals = [on((4, span, head), f32), on((4, span, head), bf16), on((4, span, head), f32)]
    local_out, reach, silu = kernel(
        window_kernel,
        [("v", out) for out in finals],
        "h" * 16 + "v" * 6,
        (tokens, tokens_c, *near, *swapped, *last, query_weight, gate_weight, gain, *shared),
        (
            on((8, 2, span, depth), bf16),
            on((8, depth, width), bf16),
            on((8, depth, width), bf16),
            dma((8,)),
        ),
        24,
    )
    arrived, local_out = lax.optimization_barrier((arrived, local_out))
    total, maps, adds, factors = kernel(
        compose_kernel,
        [
            ("p", on((rows, head), bf16)),
            ("p", on((7, head, head), bf16)),
            ("p", on((7, half, head), f32)),
            ("p", on((7, 8, head), f32)),
        ],
        "p",
        (arrived,),
    )
    others = [
        lax.ppermute(total, "zh", [(at, at ^ by) for at in range(4)]) for by in (1, 2, 3)
    ]
    finals_in = kernel(
        load_kernel,
        [("p", out) for out in finals],
        "phhh",
        (total, local_out, reach, silu),
        (dma((3,)),),
    )
    *others, loaded = lax.optimization_barrier((*others, finals_in[0]))
    finals_in = (loaded, *finals_in[1:])
    (back,) = kernel(
        spread_kernel,
        [("p", on((8, half + PACK, head), bf16))],
        "p" * 12,
        (
            new_beta, new_decay, total, *others, maps, adds, factors,
            new_query, new_key, new_value,
        ),
        (on((4, rows, head), bf16), on((head, head), f32), on((head, head), f32)),
    )
    returned = lax.all_to_all(back, NEAR, 0, 0, tiled=True)
    return kernel(
        finish_kernel,
        [
            ("v", on((2, span, width), bf16)),
            ("v", on((2, 2, 4, head), bf16)),
            ("v", on((2, width), f32)),
        ],
        "ppppp",
        (returned, *finals_in, gain),
    )


def solution(mesh):
    torus = Mesh(mesh.devices.reshape(4, 2, 4, 4, 2), AXES + ("y", "c"))
    sp, tp = AXES, ("y", "c")
    weight = P(None, tp)
    in_specs = (
        P(None, sp, tp),
        weight, weight, weight, weight, weight, weight,
        P(tp), P(tp), P(),
        P(None, tp, None), P(None, tp, None), P(None, tp, None),
        P(None, tp), P(None, tp),
    )
    out_specs = (P(None, sp, tp), P(None, tp, sp, None), P(None, tp))

    return jax.shard_map(
        shards, mesh=torus, in_specs=in_specs, out_specs=out_specs, check_vma=False
    )
```

```python
import functools

import jax
import jax.numpy as jnp
from jax import lax
from jax.experimental import pallas as pl
from jax.experimental.pallas import tpu as pltpu
from jax.sharding import Mesh
from jax.sharding import PartitionSpec as P


NEAR = ("zl", "x")
AXES = ("zh", "zl", "x")
PACK = 16
LANES = 128
unit_floor = 1.0
norm_floor = 0.001
bf16 = jnp.bfloat16
f32 = jnp.float32


def dot(left, right, dims=((1,), (0,))):
    return lax.dot_general(
        left.astype(bf16), right.astype(bf16), (dims, ((), ())), preferred_element_type=f32
    )


ROWS = ((1,), (1,))
COLS = ((0,), (0,))


def thirds(value):
    high = value.astype(bf16).astype(f32)
    rest = value - high
    mid = rest.astype(bf16).astype(f32)
    return high, mid, rest - mid


def iota(shape, dim):
    return lax.broadcasted_iota(jnp.int32, shape, dim)


def row_pack(values, width):
    rows = iota((PACK, width), 0)
    packed = jnp.zeros((PACK, width), f32)
    for at, value in enumerate(values):
        packed = jnp.where(rows == at, value, packed)
    return packed


def rms_scale(values, floor, mean):
    total = jnp.sum(values * values, axis=-1, keepdims=True)
    return lax.rsqrt((total / values.shape[-1] if mean else total) + floor)


def shard_index(ahead, swapped):
    core = lax.axis_index("c")
    core = 1 - core if swapped else core
    return lax.rem(lax.axis_index("y") + ahead, 4) * 2 + core


def first_row(slot, depth):
    return pl.multiple_of(shard_index(*slot) * depth, depth)


def joined(first, second):
    return jnp.concatenate([first[...], second[...]], axis=0)


def scalar_part(rows, stacked, slot):
    depth = rows.shape[-1]
    weight = stacked[:, pl.ds(first_row(slot, depth), depth)]
    weight = jnp.concatenate([weight, jnp.zeros((LANES - PACK, depth), bf16)], axis=0)
    return dot(rows, weight, ROWS)


SLOTS = (
    (0, False), (0, True), (3, False), (1, False), (3, True), (1, True), (2, False), (2, True),
)


def early_kernel(
    own, own_c, beta_w, decay_w, key_w, value_w, sum_ref, gate_ref, rest_ref, stacked_ref,
    token_buffer, weight_buffer, scalar_buffer, sems,
):
    depth = own.shape[-1]
    width = key_w.shape[-1]
    first = [pltpu.make_async_copy(own, token_buffer, sems.at[0])]
    for at, weight in enumerate((beta_w, decay_w)):
        first.append(pltpu.make_async_copy(weight, scalar_buffer.at[at], sems.at[0]))
    later = []
    for at, slot in enumerate(SLOTS):
        start = first_row(slot, depth)
        for side, weight in enumerate((key_w, value_w)):
            lanes = pl.ds(side * width, width)
            source = weight.at[pl.ds(start, depth), :]
            if at < 2:
                to = weight_buffer.at[pl.ds(at * depth, depth), lanes]
                first.append(pltpu.make_async_copy(source, to, sems.at[0]))
            else:
                to = rest_ref.at[pl.ds((at - 2) * depth, depth), lanes]
                later.append(pltpu.make_async_copy(source, to, sems.at[1]))
    for copy in first + later:
        copy.start()
    for copy in first:
        copy.wait()
    rows = [scalar_buffer[at, h : h + 1, :].astype(f32) for at in range(2) for h in range(2)]
    stacked_ref[...] = row_pack(rows, stacked_ref.shape[-1]).astype(bf16)
    total = gates = 0.0
    for at, piece in enumerate((token_buffer, own_c)):
        rows = piece[...].reshape(-1, depth)
        total = total + dot(rows, weight_buffer[at * depth : (at + 1) * depth, :])
        gates = gates + scalar_part(rows, stacked_ref, SLOTS[at])
    sum_ref[...] = total
    gate_ref[...] = gates
    for copy in later:
        copy.wait()


def add_pieces(pieces, from_slot, rest, stacked, total, gates):
    for at in range(len(pieces) // 2):
        rows = joined(*pieces[2 * at : 2 * at + 2])
        depth = rows.shape[-1]
        slot = from_slot + at
        total = total + dot(rows, rest[(slot - 2) * depth : (slot - 1) * depth, :])
        gates = gates + scalar_part(rows, stacked, SLOTS[slot])
    return total, gates


def middle_kernel(first_slot, *refs):
    pieces, (sum_in, gate_in, rest, stacked, sum_ref, gate_ref) = refs[:-6], refs[-6:]
    total, gates = add_pieces(pieces, first_slot, rest, stacked, sum_in[...], gate_in[...])
    sum_ref[...] = total
    gate_ref[...] = gates


def lane_pair(ref, first):
    lanes = iota((1, LANES), 1)
    pair = ref[...]
    return jnp.where(
        lanes == first, pair[:, 0:1], jnp.where(lanes == first + 1, pair[:, 1:2], 0.0)
    )


def local_kernel(bias_ref, rate_ref, *refs):
    pieces, (sum_in, gate_in, rest, stacked) = refs[:2], refs[2:6]
    outputs, buffers, sems = refs[6:12], refs[12:18], refs[18]
    send_ref, key_ref, fresh_ref, carry_ref, cols_ref, rows_ref = buffers
    copies = []

    def give(at, part=None):
        source, to = buffers[at], outputs[at]
        if part is not None:
            source, to = source.at[part], to.at[part]
        copies.append(pltpu.make_async_copy(source, to, sems.at[at]))
        copies[-1].start()

    span = pieces[0].shape[0]
    head = send_ref.shape[-1]
    total, gates = add_pieces(pieces, 7, rest, stacked, sum_in[...], gate_in[...])
    width = total.shape[-1] // 2
    key_rows = total[:, :width].astype(bf16)
    value_rows = total[:, width:].astype(bf16)
    key_ref[...] = key_rows
    give(1)
    strength = jax.nn.sigmoid(gates + lane_pair(bias_ref, 0))
    decays = -jnp.exp(lane_pair(rate_ref, 2)) * jax.nn.softplus(gates)
    wide = cols_ref.shape[1]
    lanes = iota((wide, head), 1)
    causal_wide = (iota((wide, wide), 0) >= iota((wide, wide), 1)).astype(bf16)
    for seq in range(2):
        take = slice(seq * span, (seq + 1) * span)
        padded = jnp.concatenate([decays[take], jnp.zeros((wide - span, head), f32)], axis=0)
        cumulative = sum(dot(causal_wide, part) for part in thirds(padded))
        table = jnp.where((lanes == 2) | (lanes == 3), cumulative, 0.0)
        for h in range(2):
            keys = key_rows[take, h * head : (h + 1) * head].astype(f32)
            unit = jnp.concatenate(
                [rms_scale(keys, unit_floor, False), jnp.zeros((wide - span, 1), f32)], axis=0
            )
            beta = jnp.concatenate(
                [strength[take, h : h + 1], jnp.zeros((wide - span, 1), f32)], axis=0
            )
            table = jnp.where(lanes == h, beta, table)
            table = jnp.where(lanes == 4 + h, unit, table)
        cols_ref[seq] = table
        rows_ref[seq] = table.T
    give(4)
    give(5)
    half = head // 2
    t = iota((head, head), 0)
    s = iota((head, head), 1)
    apart = t ^ s
    upper, lower = slice(0, head), slice(head, span)
    blocks = []
    for pair in range(4):
        seq, h = divmod(pair, 2)
        keys = key_rows[seq * span : (seq + 1) * span, h * head : (h + 1) * head]

        def alike(of, with_, mask):
            col = lambda at: cols_ref[seq, of, at + h : at + h + 1]
            row = lambda at: rows_ref[seq, at + h : at + h + 1, with_]
            spread = col(2) - row(2)
            if mask is not None:
                spread = jnp.where(mask, spread, 0.0)
            product = dot(keys[of], keys[with_], ROWS)
            product = product * (col(0) * col(4)) * row(4) * jnp.exp(spread)
            return product if mask is None else jnp.where(mask, product, 0.0)

        def started(block):
            size = block.shape[0]
            near, same = apart[:size, :size] < 2, (t == s)[:size, :size]
            return jnp.where(same, 1.0, jnp.where(near, -block, 0.0)).astype(bf16)

        first = alike(upper, upper, t > s)
        second = alike(lower, lower, (t > s)[:half, :half])
        across = alike(lower, upper, None)
        blocks.append(
            [first.astype(bf16), second.astype(bf16), across.astype(bf16)]
            + [started(first), started(second)]
        )
    size = 2
    while size < half:
        mask = jnp.where((apart >= size) & (apart < 2 * size), 1.0, 0.0).astype(bf16)
        steps = []
        for first, second, _, x_first, x_second in blocks:
            step = dot(first * mask, x_first).astype(bf16)
            steps.append((step, dot(second * mask[:half, :half], x_second).astype(bf16)))
        for block, (step_first, step_second) in zip(blocks, steps):
            block[3] = block[3] - dot(block[3], step_first).astype(bf16)
            block[4] = block[4] - dot(block[4], step_second).astype(bf16)
        size *= 2
    left = jnp.where(iota((half, head), 1) < half, 1.0, 0.0).astype(bf16)
    blank = jnp.zeros((half, head), bf16)
    steps = [dot(block[0][half:] * left, block[3]).astype(bf16) for block in blocks]
    for block, step in zip(blocks, steps):
        change = dot(block[3][half:], jnp.concatenate([blank, step], axis=0)).astype(bf16)
        block[3] = jnp.concatenate([block[3][:half], block[3][half:] - change], axis=0)
    steps = [dot(block[2], block[3]).astype(bf16) for block in blocks]
    for pair in range(4):
        seq, h = divmod(pair, 2)
        take = slice(seq * span, (seq + 1) * span)
        keys = key_rows[take, h * head : (h + 1) * head]
        values = value_rows[take, h * head : (h + 1) * head]
        col = lambda at: cols_ref[seq, :span, at + h : at + h + 1]
        row = lambda at: rows_ref[seq, at + h : at + h + 1, :span]
        off_first = jnp.where(t == s, 0.0, blocks[pair][3].astype(f32))
        off_second = jnp.where((t == s)[:half, :half], 0.0, blocks[pair][4].astype(f32))
        off_across = -dot(blocks[pair][4], steps[pair])

        def applied(weight, right):
            top = dot(off_first * weight[:, upper], right[upper])
            low = dot(off_across * weight[:, upper], right[upper])
            low = low + dot(off_second * weight[:, lower], right[lower])
            return jnp.concatenate([top, low], axis=0)

        fresh = col(0) * values.astype(f32) + applied(row(0), values)
        carry = (col(0) * col(4) * jnp.exp(col(2))) * keys.astype(f32) + applied(
            row(0) * row(4) * jnp.exp(row(2)), keys
        )
        last = cols_ref[seq, span - 1 : span, 2 + h : 3 + h]
        late = col(4) * jnp.exp(last - col(2))
        reach = dot(carry * late, keys, COLS)
        gain = dot(fresh * late, keys, COLS)
        fresh_ref[pair] = fresh.astype(bf16)
        carry_ref[pair] = carry.astype(bf16)
        factor = row_pack(thirds(jnp.broadcast_to(jnp.exp(last), (1, head))), head)
        for side in range(2):
            to = 2 * pair + side
            send_ref[to, :head, :] = reach.astype(bf16)
            send_ref[to, head : head + half, :] = gain[side * half : (side + 1) * half].astype(bf16)
            send_ref[to, head + half :, :] = factor.astype(bf16)
        give(0, pl.ds(2 * pair, 2))
    give(2)
    give(3)
    for copy in copies:
        copy.wait()


def window_kernel(*refs):
    pieces, refs = refs[:14], refs[14:]
    query_w, gate_w, gain_ref, shared, refs = refs[0], refs[1], refs[2], refs[3:8], refs[8:]
    outputs, refs = refs[:3], refs[3:]
    token_buffer, query_buffer, gate_buffer, sems, more_sems = refs[:5]
    shared_buffers, output_buffers = refs[5:10], refs[10:]
    key_ref, fresh_ref, carry_ref, cols_ref, rows_ref = shared_buffers
    out_ref, reach_ref, silu_ref = output_buffers
    span, depth = token_buffer.shape[2:]
    head = fresh_ref.shape[-1]
    weights = ((query_w, query_buffer), (gate_w, gate_buffer))
    copies = []
    for at, slot in enumerate(SLOTS):
        if at < 2:
            parts = [(pieces[at], token_buffer.at[at])]
        else:
            parts = [(pieces[2 * at - 2 + seq], token_buffer.at[at, seq]) for seq in range(2)]
        for weight, buffer in weights:
            parts.append((weight.at[pl.ds(first_row(slot, depth), depth), :], buffer.at[at]))
        copies.append([pltpu.make_async_copy(a, b, sems.at[at]) for a, b in parts])
        for copy in copies[at]:
            copy.start()
    given = [
        pltpu.make_async_copy(a, b, more_sems.at[at])
        for at, (a, b) in enumerate(zip(shared, shared_buffers))
    ]
    for copy in given:
        copy.start()
    query_total = gate_total = 0.0
    for at in range(8):
        for copy in copies[at]:
            copy.wait()
        rows = token_buffer[at].reshape(-1, depth)
        query_total = query_total + dot(rows, query_buffer[at])
        gate_total = gate_total + dot(rows, gate_buffer[at])
    for copy in given:
        copy.wait()
    query_rows = query_total.astype(bf16)
    gate_rows = gate_total.astype(bf16).astype(f32)
    t = iota((span, span), 0)
    s = iota((span, span), 1)
    taken = []
    for pair in range(4):
        seq, h = divmod(pair, 2)
        take = slice(seq * span, (seq + 1) * span)
        part = slice(h * head, (h + 1) * head)
        col = lambda at: cols_ref[seq, :span, at + h : at + h + 1]
        row = lambda at: rows_ref[seq, at + h : at + h + 1, :span]
        queries = query_rows[take, part]
        unit = rms_scale(queries.astype(f32), unit_floor, False)
        spread = jnp.where(t >= s, col(2) - row(2), 0.0)
        scores = dot(queries, key_ref[take, part], ROWS) * unit * row(4) * jnp.exp(spread)
        scores = jnp.where(t >= s, scores, 0.0).astype(bf16)
        out_ref[pair] = dot(scores, fresh_ref[pair])
        reach = (unit * jnp.exp(col(2))) * queries.astype(f32) - dot(scores, carry_ref[pair])
        reach_ref[pair] = reach.astype(bf16)
        gate = gate_rows[take, part]
        silu_ref[pair] = gain_ref[...] * gate * jax.nn.sigmoid(gate)
        for at, (a, b) in enumerate(zip(output_buffers, outputs)):
            taken.append(pltpu.make_async_copy(a.at[pair], b.at[pair], more_sems.at[5 + at]))
            taken[-1].start()
    for copy in taken:
        copy.wait()


def unpack_factor(block):
    block = block.astype(f32)
    return block[0:1] + block[1:2] + block[2:3]


def compose_kernel(in_ref, total_ref, maps_ref, adds_ref, factors_ref):
    count, rows, head = in_ref.shape
    body = rows - PACK

    def load(at):
        return in_ref[at, :body, :].astype(f32), unpack_factor(in_ref[at, body:, :])

    def join(first, second):
        both, factor = first
        later, later_factor = second
        tail = jnp.concatenate([factor * later[:head], later[head:]], axis=0)
        return later_factor * both - dot(both, later[:head]) + tail, factor * later_factor

    member = [load(at) for at in range(count)]
    upto = [None] * (count + 1)
    upto[1] = member[0]
    c23, c45, c67 = (join(member[at], member[at + 1]) for at in (2, 4, 6))
    upto[2] = join(member[0], member[1])
    c456 = join(c45, member[6])
    c4567 = join(c45, c67)
    upto[4] = join(upto[2], c23)
    upto[8] = join(upto[4], c4567)
    both, factor = upto[8]
    total_ref[:body, :] = both.astype(bf16)
    total_ref[body:, :] = row_pack(thirds(factor), head).astype(bf16)
    upto[3] = join(upto[2], member[2])
    upto[5] = join(upto[4], member[4])
    upto[6] = join(upto[4], c45)
    upto[7] = join(upto[4], c456)
    for at in range(1, count):
        both, factor = upto[at]
        maps_ref[at - 1] = both[:head].astype(bf16)
        adds_ref[at - 1] = both[head:]
        factors_ref[at - 1] = jnp.broadcast_to(factor, (8, head))


def spread_kernel(
    beta_ref, decay_ref, own, back1, back2, back3, maps_ref, adds_ref, factors_ref,
    query_ref, key_ref, value_ref, send_ref, groups_ref, wide_ref, turned_ref,
):
    _, head = own.shape
    half = head // 2
    far = lax.axis_index("zh")
    near = lax.axis_index("zl") * 4 + lax.axis_index("x")
    pair = near // 2
    side = near % 2

    def scalar(ref):
        total = jnp.zeros((1, 1), f32)
        for at in range(4):
            entry = ref[at // 2 : at // 2 + 1, at % 2 : at % 2 + 1]
            total = jnp.where(pair == at, entry, total)
        return total

    def chosen(ref):
        total = jnp.zeros((1, head), f32)
        for at in range(4):
            row = ref[at // 2, at % 2 : at % 2 + 1, :].astype(f32)
            total = jnp.where(pair == at, row, total)
        return total

    for slot, ref in enumerate((own, back1, back2, back3)):
        groups_ref[slot] = ref[...]
    state = jnp.zeros((half, head), f32)
    begin = state
    for group in range(4):
        begin = jnp.where(far == group, state, begin)
        block = groups_ref[lax.bitwise_xor(far, group)]
        added = block[head : head + half].astype(f32)
        if group:
            state = unpack_factor(block[head + half :]) * state - dot(state, block[:head]) + added
        else:
            state = added
    final = state.astype(bf16).astype(f32)
    wide_ref[...] = jnp.zeros((head, head), f32)
    wide_ref[pl.ds(pl.multiple_of(side * half, half), half), :] = final
    padded = wide_ref[...]
    turned_ref[...] = padded.T
    mine = turned_ref[pl.ds(pl.multiple_of(far * 32, 32), 32), :]
    query = chosen(query_ref)
    key = chosen(key_ref)
    query = query * rms_scale(query, unit_floor, False)
    key = key * rms_scale(key, unit_floor, False)
    hits = dot(row_pack(thirds(query) + thirds(key), head), padded, ROWS)
    recall = hits[0:1] + hits[1:2] + hits[2:3]
    retrieve = hits[3:4] + hits[4:5] + hits[5:6]
    decay = scalar(decay_ref)
    intersect = jnp.sum(key * query, axis=-1, keepdims=True)
    fresh = chosen(value_ref) - decay * retrieve
    read = decay * recall + (scalar(beta_ref) * intersect) * fresh
    read = jnp.where(iota((1, head), 1) // half == side, read, 0.0)
    zero = jnp.zeros((1, head), f32)
    extra = row_pack((zero, zero, zero, zero) + thirds(read), head)
    pick_row = iota((PACK, 32), 0)
    pick_col = iota((PACK, 32), 1)
    for member in range(8):
        if member:
            at = member - 1
            entry = factors_ref[at, 0:1, :] * begin - dot(begin, maps_ref[at]) + adds_ref[at]
        else:
            entry = begin
        send_ref[member, :half, :] = entry.astype(bf16)
        pick = ((pick_row < 4) & (pick_col == 4 * member + pick_row)).astype(bf16)
        send_ref[member, half:, :] = (dot(pick, mine) + extra).astype(bf16)


def load_kernel(_, *refs):
    count = len(refs) // 2
    sources, outputs, sems = refs[:count], refs[count : 2 * count], refs[2 * count]
    copies = [
        pltpu.make_async_copy(a, b, sems.at[at]) for at, (a, b) in enumerate(zip(sources, outputs))
    ]
    for copy in copies:
        copy.start()
    for copy in copies:
        copy.wait()


def finish_kernel(in_ref, out_ref, reach_ref, silu_ref, gain_ref, mixed_ref, cache_ref, read_ref):
    head = in_ref.shape[-1]
    half = head // 2
    for pair in range(4):
        seq, h = divmod(pair, 2)
        incoming = jnp.concatenate([in_ref[2 * pair, :half, :], in_ref[2 * pair + 1, :half, :]], 0)
        whole = out_ref[pair] + dot(reach_ref[pair], incoming, ROWS)
        mixed = whole * rms_scale(whole, norm_floor, True) * silu_ref[pair]
        mixed_ref[seq, :, h * head : (h + 1) * head] = mixed.astype(bf16)
        extra = in_ref[2 * pair, half:, :].astype(f32) + in_ref[2 * pair + 1, half:, :].astype(f32)
        cache_ref[seq, h] = extra[:4].astype(bf16)
        read = extra[4:5] + extra[5:6] + extra[6:7]
        read = read * rms_scale(read, norm_floor, True) * gain_ref[...]
        read_ref[seq : seq + 1, h * head : (h + 1) * head] = read


def vmem():
    return pl.BlockSpec(memory_space=pltpu.VMEM)


def smem():
    return pl.BlockSpec(memory_space=pltpu.SMEM)


def kernel(body, outputs, kinds, args, scratch=(), limit=16):
    given = {"s": smem, "v": vmem, "p": vmem, "h": lambda: pl.BlockSpec(memory_space=pl.ANY)}
    placed = [
        arg
        if kind == "s"
        else pltpu.with_memory_space_constraint(arg, pltpu.VMEM if kind == "p" else pltpu.HBM)
        for kind, arg in zip(kinds, args, strict=True)
    ]
    plain = lambda out: pltpu.HBM(out.shape, out.dtype)
    return pl.pallas_call(
        body,
        out_shape=tuple(out if kind == "p" else plain(out) for kind, out in outputs),
        in_specs=[given[kind]() for kind in kinds],
        out_specs=tuple(given[kind]() for kind, _ in outputs),
        scratch_shapes=list(scratch),
        compiler_params=pltpu.CompilerParams(vmem_limit_bytes=limit * 1024 * 1024),
    )(*placed)


def shift(value, axis, by):
    length = lax.axis_size(axis)
    return lax.ppermute(value, axis, [(at, (at + by) % length) for at in range(length)])


def shards(
    tokens, query_weight, key_weight, value_weight, gate_weight, beta_weight, decay_weight,
    beta_bias, rate_log, out_gain, new_query, new_key, new_value, new_beta, new_decay,
):
    _, span, depth = tokens.shape
    head = out_gain.shape[0]
    half = head // 2
    wide = 256
    width = query_weight.shape[1]
    rows = head + half + PACK
    on, dma = pltpu.VMEM, pltpu.SemaphoreType.DMA
    depth = tokens.shape[2]
    swap = lambda value: shift(value, "c", 1)
    tokens_c = swap(tokens)
    first, second = tokens[0], tokens[1]
    up0 = shift(first, "y", 1)
    down1 = shift(second, "y", -1)
    sums = [("p", on((2 * span, 2 * width), f32)), ("p", on((2 * span, head), f32))]
    early = kernel(
        early_kernel,
        sums + [("p", on((6 * depth, 2 * width), bf16)), ("p", on((PACK, 8 * depth), bf16))],
        "hphhhh",
        (tokens, tokens_c, beta_weight.T, decay_weight.T, key_weight, value_weight),
        (
            on((2, span, depth), bf16),
            on((2 * depth, 2 * width), bf16),
            on((2, 2, 8 * depth), bf16),
            dma((2,)),
        ),
    )
    early = list(early)
    first, second, *early[:2] = lax.optimization_barrier((first, second, *early[:2]))
    up1 = shift(second, "y", 1)
    down0 = shift(first, "y", -1)
    rest = early[2:]
    far0 = shift(up0, "y", 1)
    far1 = shift(down1, "y", -1)
    near = (up0, up1, down0, down1)
    swapped = []
    for value in near:
        swapped.append(swap(value))
    middle = kernel(functools.partial(middle_kernel, 2), sums, "p" * 8, (*near, *early[:2], *rest))
    far0, far1, *middle = lax.optimization_barrier((far0, far1, *middle))
    last = [far0, far1]
    for at in range(2):
        last.append(swap(last[at]))
    middle = kernel(
        functools.partial(middle_kernel, 4), sums, "p" * 10, (*swapped, far0, far1, *middle, *rest)
    )
    far_c0, far_c1, *middle = lax.optimization_barrier((*last[2:], *middle))
    last[2:] = [far_c0, far_c1]
    local_shapes = [
        on((8, rows, head), bf16),
        on((2 * span, width), bf16),
        on((4, span, head), bf16),
        on((4, span, head), bf16),
        on((2, wide, head), f32),
        on((2, head, wide), f32),
    ]
    send, *shared = kernel(
        local_kernel,
        [("h", out) for out in local_shapes],
        "p" * 8,
        (beta_bias[None], rate_log[None], *last[2:], *middle, *rest),
        (*local_shapes, dma((6,))),
    )
    arrived = lax.all_to_all(send, NEAR, 0, 0, tiled=True)
    gain = out_gain[None]
    finals = [on((4, span, head), f32), on((4, span, head), bf16), on((4, span, head), f32)]
    local_out, reach, silu = kernel(
        window_kernel,
        [("h", out) for out in finals],
        "h" * 16 + "v" + "h" * 5,
        (tokens, tokens_c, *near, *swapped, *last, query_weight, gate_weight, gain, *shared),
        (
            on((8, 2, span, depth), bf16),
            on((8, depth, width), bf16),
            on((8, depth, width), bf16),
            dma((8,)),
            dma((8,)),
            *local_shapes[1:],
            *finals,
        ),
        24,
    )
    arrived, local_out = lax.optimization_barrier((arrived, local_out))
    total, maps, adds, factors = kernel(
        compose_kernel,
        [
            ("p", on((rows, head), bf16)),
            ("p", on((7, head, head), bf16)),
            ("p", on((7, half, head), f32)),
            ("p", on((7, 8, head), f32)),
        ],
        "p",
        (arrived,),
    )
    others = [
        lax.ppermute(total, "zh", [(at, at ^ by) for at in range(4)]) for by in (1, 2, 3)
    ]
    finals_in = kernel(
        load_kernel,
        [("p", out) for out in finals],
        "phhh",
        (total, local_out, reach, silu),
        (dma((3,)),),
    )
    *others, loaded = lax.optimization_barrier((*others, finals_in[0]))
    finals_in = (loaded, *finals_in[1:])
    (back,) = kernel(
        spread_kernel,
        [("p", on((8, half + PACK, head), bf16))],
        "p" * 12,
        (
            new_beta, new_decay, total, *others, maps, adds, factors,
            new_query, new_key, new_value,
        ),
        (on((4, rows, head), bf16), on((head, head), f32), on((head, head), f32)),
    )
    returned = lax.all_to_all(back, NEAR, 0, 0, tiled=True)
    return kernel(
        finish_kernel,
        [
            ("v", on((2, span, width), bf16)),
            ("v", on((2, 2, 4, head), bf16)),
            ("v", on((2, width), f32)),
        ],
        "ppppp",
        (returned, *finals_in, gain),
    )


def solution(mesh):
    torus = Mesh(mesh.devices.reshape(4, 2, 4, 4, 2), AXES + ("y", "c"))
    sp, tp = AXES, ("y", "c")
    weight = P(None, tp)
    in_specs = (
        P(None, sp, tp),
        weight, weight, weight, weight, weight, weight,
        P(tp), P(tp), P(),
        P(None, tp, None), P(None, tp, None), P(None, tp, None),
        P(None, tp), P(None, tp),
    )
    out_specs = (P(None, sp, tp), P(None, tp, sp, None), P(None, tp))

    return jax.shard_map(
        shards, mesh=torus, in_specs=in_specs, out_specs=out_specs, check_vma=False
    )
```

```python
import functools

import jax
import jax.numpy as jnp
from jax import lax
from jax.experimental import pallas as pl
from jax.experimental.pallas import tpu as pltpu
from jax.sharding import Mesh
from jax.sharding import PartitionSpec as P


NEAR = ("zl", "x")
AXES = ("zh", "zl", "x")
PACK = 16
LANES = 128
unit_floor = 1.0
norm_floor = 0.001
bf16 = jnp.bfloat16
f32 = jnp.float32


def dot(left, right, dims=((1,), (0,))):
    return lax.dot_general(
        left.astype(bf16), right.astype(bf16), (dims, ((), ())), preferred_element_type=f32
    )


ROWS = ((1,), (1,))
COLS = ((0,), (0,))


def thirds(value):
    high = value.astype(bf16).astype(f32)
    rest = value - high
    mid = rest.astype(bf16).astype(f32)
    return high, mid, rest - mid


def iota(shape, dim):
    return lax.broadcasted_iota(jnp.int32, shape, dim)


def row_pack(values, width):
    rows = iota((PACK, width), 0)
    packed = jnp.zeros((PACK, width), f32)
    for at, value in enumerate(values):
        packed = jnp.where(rows == at, value, packed)
    return packed


def rms_scale(values, floor, mean):
    total = jnp.sum(values * values, axis=-1, keepdims=True)
    return lax.rsqrt((total / values.shape[-1] if mean else total) + floor)


def shard_index(ahead, swapped):
    core = lax.axis_index("c")
    core = 1 - core if swapped else core
    return lax.rem(lax.axis_index("y") + ahead, 4) * 2 + core


def first_row(slot, depth):
    return pl.multiple_of(shard_index(*slot) * depth, depth)


def joined(first, second):
    return jnp.concatenate([first[...], second[...]], axis=0)


def scalar_part(rows, stacked, slot):
    depth = rows.shape[-1]
    weight = stacked[:, pl.ds(first_row(slot, depth), depth)]
    weight = jnp.concatenate([weight, jnp.zeros((LANES - PACK, depth), bf16)], axis=0)
    return dot(rows, weight, ROWS)


SLOTS = (
    (0, False), (0, True), (3, False), (1, False), (3, True), (1, True), (2, False), (2, True),
)


def early_kernel(
    own, own_c, beta_w, decay_w, key_w, value_w, sum_ref, gate_ref, rest_ref, stacked_ref,
    token_buffer, weight_buffer, scalar_buffer, sems,
):
    depth = own.shape[-1]
    width = key_w.shape[-1]
    first = [pltpu.make_async_copy(own, token_buffer, sems.at[0])]
    for at, weight in enumerate((beta_w, decay_w)):
        first.append(pltpu.make_async_copy(weight, scalar_buffer.at[at], sems.at[0]))
    later = []
    for at, slot in enumerate(SLOTS):
        start = first_row(slot, depth)
        for side, weight in enumerate((key_w, value_w)):
            lanes = pl.ds(side * width, width)
            source = weight.at[pl.ds(start, depth), :]
            if at < 2:
                to = weight_buffer.at[pl.ds(at * depth, depth), lanes]
                first.append(pltpu.make_async_copy(source, to, sems.at[0]))
            else:
                to = rest_ref.at[pl.ds((at - 2) * depth, depth), lanes]
                later.append(pltpu.make_async_copy(source, to, sems.at[1]))
    for copy in first + later:
        copy.start()
    for copy in first:
        copy.wait()
    rows = [scalar_buffer[at, h : h + 1, :].astype(f32) for at in range(2) for h in range(2)]
    stacked_ref[...] = row_pack(rows, stacked_ref.shape[-1]).astype(bf16)
    total = gates = 0.0
    for at, piece in enumerate((token_buffer, own_c)):
        rows = piece[...].reshape(-1, depth)
        total = total + dot(rows, weight_buffer[at * depth : (at + 1) * depth, :])
        gates = gates + scalar_part(rows, stacked_ref, SLOTS[at])
    sum_ref[...] = total
    gate_ref[...] = gates
    for copy in later:
        copy.wait()


def add_pieces(pieces, from_slot, rest, stacked, total, gates):
    for at in range(len(pieces) // 2):
        rows = joined(*pieces[2 * at : 2 * at + 2])
        depth = rows.shape[-1]
        slot = from_slot + at
        total = total + dot(rows, rest[(slot - 2) * depth : (slot - 1) * depth, :])
        gates = gates + scalar_part(rows, stacked, SLOTS[slot])
    return total, gates


def middle_kernel(first_slot, *refs):
    pieces, (sum_in, gate_in, rest, stacked, sum_ref, gate_ref) = refs[:-6], refs[-6:]
    total, gates = add_pieces(pieces, first_slot, rest, stacked, sum_in[...], gate_in[...])
    sum_ref[...] = total
    gate_ref[...] = gates


def lane_pair(ref, first):
    lanes = iota((1, LANES), 1)
    pair = ref[...]
    return jnp.where(
        lanes == first, pair[:, 0:1], jnp.where(lanes == first + 1, pair[:, 1:2], 0.0)
    )


def local_kernel(bias_ref, rate_ref, *refs):
    pieces, (sum_in, gate_in, rest, stacked) = refs[:2], refs[2:6]
    outputs, buffers, sems = refs[6:12], refs[12:18], refs[18]
    send_ref, key_ref, fresh_ref, carry_ref, cols_ref, rows_ref = buffers
    copies = []

    def give(at, part=None):
        source, to = buffers[at], outputs[at]
        if part is not None:
            source, to = source.at[part], to.at[part]
        copies.append(pltpu.make_async_copy(source, to, sems.at[at]))
        copies[-1].start()

    span = pieces[0].shape[0]
    head = send_ref.shape[-1]
    total, gates = add_pieces(pieces, 7, rest, stacked, sum_in[...], gate_in[...])
    width = total.shape[-1] // 2
    key_rows = total[:, :width].astype(bf16)
    value_rows = total[:, width:].astype(bf16)
    key_ref[...] = key_rows
    give(1)
    strength = jax.nn.sigmoid(gates + lane_pair(bias_ref, 0))
    decays = -jnp.exp(lane_pair(rate_ref, 2)) * jax.nn.softplus(gates)
    wide = cols_ref.shape[1]
    lanes = iota((wide, head), 1)
    causal_wide = (iota((wide, wide), 0) >= iota((wide, wide), 1)).astype(bf16)
    for seq in range(2):
        take = slice(seq * span, (seq + 1) * span)
        padded = jnp.concatenate([decays[take], jnp.zeros((wide - span, head), f32)], axis=0)
        cumulative = sum(dot(causal_wide, part) for part in thirds(padded))
        table = jnp.where((lanes == 2) | (lanes == 3), cumulative, 0.0)
        for h in range(2):
            keys = key_rows[take, h * head : (h + 1) * head].astype(f32)
            unit = jnp.concatenate(
                [rms_scale(keys, unit_floor, False), jnp.zeros((wide - span, 1), f32)], axis=0
            )
            beta = jnp.concatenate(
                [strength[take, h : h + 1], jnp.zeros((wide - span, 1), f32)], axis=0
            )
            table = jnp.where(lanes == h, beta, table)
            table = jnp.where(lanes == 4 + h, unit, table)
        cols_ref[seq] = table
        rows_ref[seq] = table.T
    give(4)
    give(5)
    half = head // 2
    t = iota((head, head), 0)
    s = iota((head, head), 1)
    apart = t ^ s
    upper, lower = slice(0, head), slice(head, span)
    blocks = []
    for pair in range(4):
        seq, h = divmod(pair, 2)
        keys = key_rows[seq * span : (seq + 1) * span, h * head : (h + 1) * head]

        def alike(of, with_, mask):
            col = lambda at: cols_ref[seq, of, at + h : at + h + 1]
            row = lambda at: rows_ref[seq, at + h : at + h + 1, with_]
            spread = col(2) - row(2)
            if mask is not None:
                spread = jnp.where(mask, spread, 0.0)
            product = dot(keys[of], keys[with_], ROWS)
            product = product * (col(0) * col(4)) * row(4) * jnp.exp(spread)
            return product if mask is None else jnp.where(mask, product, 0.0)

        def started(block):
            size = block.shape[0]
            near, same = apart[:size, :size] < 2, (t == s)[:size, :size]
            return jnp.where(same, 1.0, jnp.where(near, -block, 0.0)).astype(bf16)

        first = alike(upper, upper, t > s)
        second = alike(lower, lower, (t > s)[:half, :half])
        across = alike(lower, upper, None)
        blocks.append(
            [first.astype(bf16), second.astype(bf16), across.astype(bf16)]
            + [started(first), started(second)]
        )
    size = 2
    while size < half:
        mask = jnp.where((apart >= size) & (apart < 2 * size), 1.0, 0.0).astype(bf16)
        steps = []
        for first, second, _, x_first, x_second in blocks:
            step = dot(first * mask, x_first).astype(bf16)
            steps.append((step, dot(second * mask[:half, :half], x_second).astype(bf16)))
        for block, (step_first, step_second) in zip(blocks, steps):
            block[3] = block[3] - dot(block[3], step_first).astype(bf16)
            block[4] = block[4] - dot(block[4], step_second).astype(bf16)
        size *= 2
    left = jnp.where(iota((half, head), 1) < half, 1.0, 0.0).astype(bf16)
    blank = jnp.zeros((half, head), bf16)
    steps = [dot(block[0][half:] * left, block[3]).astype(bf16) for block in blocks]
    for block, step in zip(blocks, steps):
        change = dot(block[3][half:], jnp.concatenate([blank, step], axis=0)).astype(bf16)
        block[3] = jnp.concatenate([block[3][:half], block[3][half:] - change], axis=0)
    steps = [dot(block[2], block[3]).astype(bf16) for block in blocks]
    for pair in range(4):
        seq, h = divmod(pair, 2)
        take = slice(seq * span, (seq + 1) * span)
        keys = key_rows[take, h * head : (h + 1) * head]
        values = value_rows[take, h * head : (h + 1) * head]
        col = lambda at: cols_ref[seq, :span, at + h : at + h + 1]
        row = lambda at: rows_ref[seq, at + h : at + h + 1, :span]
        off_first = jnp.where(t == s, 0.0, blocks[pair][3].astype(f32))
        off_second = jnp.where((t == s)[:half, :half], 0.0, blocks[pair][4].astype(f32))
        off_across = -dot(blocks[pair][4], steps[pair])

        def applied(weight, right):
            top = dot(off_first * weight[:, upper], right[upper])
            low = dot(off_across * weight[:, upper], right[upper])
            low = low + dot(off_second * weight[:, lower], right[lower])
            return jnp.concatenate([top, low], axis=0)

        fresh = col(0) * values.astype(f32) + applied(row(0), values)
        carry = (col(0) * col(4) * jnp.exp(col(2))) * keys.astype(f32) + applied(
            row(0) * row(4) * jnp.exp(row(2)), keys
        )
        last = cols_ref[seq, span - 1 : span, 2 + h : 3 + h]
        late = col(4) * jnp.exp(last - col(2))
        reach = dot(carry * late, keys, COLS)
        gain = dot(fresh * late, keys, COLS)
        fresh_ref[pair] = fresh.astype(bf16)
        carry_ref[pair] = carry.astype(bf16)
        give(2, pair)
        give(3, pair)
        factor = row_pack(thirds(jnp.broadcast_to(jnp.exp(last), (1, head))), head)
        for side in range(2):
            to = 2 * pair + side
            send_ref[to, :head, :] = reach.astype(bf16)
            send_ref[to, head : head + half, :] = gain[side * half : (side + 1) * half].astype(bf16)
            send_ref[to, head + half :, :] = factor.astype(bf16)
        give(0, pl.ds(2 * pair, 2))
    for copy in copies:
        copy.wait()


def window_kernel(*refs):
    pieces, refs = refs[:14], refs[14:]
    query_w, gate_w, gain_ref, shared, refs = refs[0], refs[1], refs[2], refs[3:8], refs[8:]
    outputs, refs = refs[:3], refs[3:]
    token_buffer, query_buffer, gate_buffer, sems, more_sems = refs[:5]
    shared_buffers, output_buffers = refs[5:10], refs[10:]
    key_ref, fresh_ref, carry_ref, cols_ref, rows_ref = shared_buffers
    out_ref, reach_ref, silu_ref = output_buffers
    span, depth = token_buffer.shape[2:]
    head = fresh_ref.shape[-1]
    weights = ((query_w, query_buffer), (gate_w, gate_buffer))
    copies = []
    for at, slot in enumerate(SLOTS):
        if at < 2:
            parts = [(pieces[at], token_buffer.at[at])]
        else:
            parts = [(pieces[2 * at - 2 + seq], token_buffer.at[at, seq]) for seq in range(2)]
        for weight, buffer in weights:
            parts.append((weight.at[pl.ds(first_row(slot, depth), depth), :], buffer.at[at]))
        copies.append([pltpu.make_async_copy(a, b, sems.at[at]) for a, b in parts])
        for copy in copies[at]:
            copy.start()
    given = [
        pltpu.make_async_copy(a, b, more_sems.at[at])
        for at, (a, b) in enumerate(zip(shared, shared_buffers))
    ]
    for copy in given:
        copy.start()
    query_total = gate_total = 0.0
    for at in range(8):
        for copy in copies[at]:
            copy.wait()
        rows = token_buffer[at].reshape(-1, depth)
        query_total = query_total + dot(rows, query_buffer[at])
        gate_total = gate_total + dot(rows, gate_buffer[at])
    for copy in given:
        copy.wait()
    query_rows = query_total.astype(bf16)
    gate_rows = gate_total.astype(bf16).astype(f32)
    t = iota((span, span), 0)
    s = iota((span, span), 1)
    taken = []
    for pair in range(4):
        seq, h = divmod(pair, 2)
        take = slice(seq * span, (seq + 1) * span)
        part = slice(h * head, (h + 1) * head)
        col = lambda at: cols_ref[seq, :span, at + h : at + h + 1]
        row = lambda at: rows_ref[seq, at + h : at + h + 1, :span]
        queries = query_rows[take, part]
        unit = rms_scale(queries.astype(f32), unit_floor, False)
        spread = jnp.where(t >= s, col(2) - row(2), 0.0)
        scores = dot(queries, key_ref[take, part], ROWS) * unit * row(4) * jnp.exp(spread)
        scores = jnp.where(t >= s, scores, 0.0).astype(bf16)
        out_ref[pair] = dot(scores, fresh_ref[pair])
        reach = (unit * jnp.exp(col(2))) * queries.astype(f32) - dot(scores, carry_ref[pair])
        reach_ref[pair] = reach.astype(bf16)
        gate = gate_rows[take, part]
        silu_ref[pair] = gain_ref[...] * gate * jax.nn.sigmoid(gate)
        for at, (a, b) in enumerate(zip(output_buffers, outputs)):
            taken.append(pltpu.make_async_copy(a.at[pair], b.at[pair], more_sems.at[5 + at]))
            taken[-1].start()
    for copy in taken:
        copy.wait()


def unpack_factor(block):
    block = block.astype(f32)
    return block[0:1] + block[1:2] + block[2:3]


def compose_kernel(in_ref, total_ref, maps_ref, adds_ref, factors_ref):
    count, rows, head = in_ref.shape
    body = rows - PACK

    def load(at):
        return in_ref[at, :body, :].astype(f32), unpack_factor(in_ref[at, body:, :])

    def join(first, second):
        both, factor = first
        later, later_factor = second
        tail = jnp.concatenate([factor * later[:head], later[head:]], axis=0)
        return later_factor * both - dot(both, later[:head]) + tail, factor * later_factor

    member = [load(at) for at in range(count)]
    upto = [None] * (count + 1)
    upto[1] = member[0]
    c23, c45, c67 = (join(member[at], member[at + 1]) for at in (2, 4, 6))
    upto[2] = join(member[0], member[1])
    c456 = join(c45, member[6])
    c4567 = join(c45, c67)
    upto[4] = join(upto[2], c23)
    upto[8] = join(upto[4], c4567)
    both, factor = upto[8]
    total_ref[:body, :] = both.astype(bf16)
    total_ref[body:, :] = row_pack(thirds(factor), head).astype(bf16)
    upto[3] = join(upto[2], member[2])
    upto[5] = join(upto[4], member[4])
    upto[6] = join(upto[4], c45)
    upto[7] = join(upto[4], c456)
    for at in range(1, count):
        both, factor = upto[at]
        maps_ref[at - 1] = both[:head].astype(bf16)
        adds_ref[at - 1] = both[head:]
        factors_ref[at - 1] = jnp.broadcast_to(factor, (8, head))


def spread_kernel(
    beta_ref, decay_ref, own, back1, back2, back3, maps_ref, adds_ref, factors_ref,
    query_ref, key_ref, value_ref, send_ref, groups_ref, wide_ref, turned_ref,
):
    _, head = own.shape
    half = head // 2
    far = lax.axis_index("zh")
    near = lax.axis_index("zl") * 4 + lax.axis_index("x")
    pair = near // 2
    side = near % 2

    def scalar(ref):
        total = jnp.zeros((1, 1), f32)
        for at in range(4):
            entry = ref[at // 2 : at // 2 + 1, at % 2 : at % 2 + 1]
            total = jnp.where(pair == at, entry, total)
        return total

    def chosen(ref):
        total = jnp.zeros((1, head), f32)
        for at in range(4):
            row = ref[at // 2, at % 2 : at % 2 + 1, :].astype(f32)
            total = jnp.where(pair == at, row, total)
        return total

    for slot, ref in enumerate((own, back1, back2, back3)):
        groups_ref[slot] = ref[...]
    state = jnp.zeros((half, head), f32)
    begin = state
    for group in range(4):
        begin = jnp.where(far == group, state, begin)
        block = groups_ref[lax.bitwise_xor(far, group)]
        added = block[head : head + half].astype(f32)
        if group:
            state = unpack_factor(block[head + half :]) * state - dot(state, block[:head]) + added
        else:
            state = added
    final = state.astype(bf16).astype(f32)
    wide_ref[...] = jnp.zeros((head, head), f32)
    wide_ref[pl.ds(pl.multiple_of(side * half, half), half), :] = final
    padded = wide_ref[...]
    turned_ref[...] = padded.T
    mine = turned_ref[pl.ds(pl.multiple_of(far * 32, 32), 32), :]
    query = chosen(query_ref)
    key = chosen(key_ref)
    query = query * rms_scale(query, unit_floor, False)
    key = key * rms_scale(key, unit_floor, False)
    hits = dot(row_pack(thirds(query) + thirds(key), head), padded, ROWS)
    recall = hits[0:1] + hits[1:2] + hits[2:3]
    retrieve = hits[3:4] + hits[4:5] + hits[5:6]
    decay = scalar(decay_ref)
    intersect = jnp.sum(key * query, axis=-1, keepdims=True)
    fresh = chosen(value_ref) - decay * retrieve
    read = decay * recall + (scalar(beta_ref) * intersect) * fresh
    read = jnp.where(iota((1, head), 1) // half == side, read, 0.0)
    zero = jnp.zeros((1, head), f32)
    extra = row_pack((zero, zero, zero, zero) + thirds(read), head)
    pick_row = iota((PACK, 32), 0)
    pick_col = iota((PACK, 32), 1)
    for member in range(8):
        if member:
            at = member - 1
            entry = factors_ref[at, 0:1, :] * begin - dot(begin, maps_ref[at]) + adds_ref[at]
        else:
            entry = begin
        send_ref[member, :half, :] = entry.astype(bf16)
        pick = ((pick_row < 4) & (pick_col == 4 * member + pick_row)).astype(bf16)
        send_ref[member, half:, :] = (dot(pick, mine) + extra).astype(bf16)


def load_kernel(_, *refs):
    count = len(refs) // 2
    sources, outputs, sems = refs[:count], refs[count : 2 * count], refs[2 * count]
    copies = [
        pltpu.make_async_copy(a, b, sems.at[at]) for at, (a, b) in enumerate(zip(sources, outputs))
    ]
    for copy in copies:
        copy.start()
    for copy in copies:
        copy.wait()


def finish_kernel(
    in_ref, out_ref, reach_ref, silu_ref, gain_ref, mixed_out, cache_ref, read_ref, mixed_ref, sems
):
    head = in_ref.shape[-1]
    half = head // 2
    copies = []
    for pair in range(4):
        seq, h = divmod(pair, 2)
        incoming = jnp.concatenate([in_ref[2 * pair, :half, :], in_ref[2 * pair + 1, :half, :]], 0)
        whole = out_ref[pair] + dot(reach_ref[pair], incoming, ROWS)
        mixed = whole * rms_scale(whole, norm_floor, True) * silu_ref[pair]
        lanes = pl.ds(h * head, head)
        mixed_ref[seq, :, h * head : (h + 1) * head] = mixed.astype(bf16)
        copies.append(
            pltpu.make_async_copy(
                mixed_ref.at[seq, :, lanes], mixed_out.at[seq, :, lanes], sems.at[pair]
            )
        )
        copies[-1].start()
    for pair in range(4):
        seq, h = divmod(pair, 2)
        extra = in_ref[2 * pair, half:, :].astype(f32) + in_ref[2 * pair + 1, half:, :].astype(f32)
        cache_ref[seq, h] = extra[:4].astype(bf16)
        read = extra[4:5] + extra[5:6] + extra[6:7]
        read = read * rms_scale(read, norm_floor, True) * gain_ref[...]
        read_ref[seq : seq + 1, h * head : (h + 1) * head] = read
    for copy in copies:
        copy.wait()


def vmem():
    return pl.BlockSpec(memory_space=pltpu.VMEM)


def smem():
    return pl.BlockSpec(memory_space=pltpu.SMEM)


def kernel(body, outputs, kinds, args, scratch=(), limit=16):
    given = {"s": smem, "v": vmem, "p": vmem, "h": lambda: pl.BlockSpec(memory_space=pl.ANY)}
    placed = [
        arg
        if kind == "s"
        else pltpu.with_memory_space_constraint(arg, pltpu.VMEM if kind == "p" else pltpu.HBM)
        for kind, arg in zip(kinds, args, strict=True)
    ]
    plain = lambda out: pltpu.HBM(out.shape, out.dtype)
    return pl.pallas_call(
        body,
        out_shape=tuple(out if kind == "p" else plain(out) for kind, out in outputs),
        in_specs=[given[kind]() for kind in kinds],
        out_specs=tuple(given[kind]() for kind, _ in outputs),
        scratch_shapes=list(scratch),
        compiler_params=pltpu.CompilerParams(vmem_limit_bytes=limit * 1024 * 1024),
    )(*placed)


def shift(value, axis, by):
    length = lax.axis_size(axis)
    return lax.ppermute(value, axis, [(at, (at + by) % length) for at in range(length)])


def shards(
    tokens, query_weight, key_weight, value_weight, gate_weight, beta_weight, decay_weight,
    beta_bias, rate_log, out_gain, new_query, new_key, new_value, new_beta, new_decay,
):
    _, span, depth = tokens.shape
    head = out_gain.shape[0]
    half = head // 2
    wide = 256
    width = query_weight.shape[1]
    rows = head + half + PACK
    on, dma = pltpu.VMEM, pltpu.SemaphoreType.DMA
    depth = tokens.shape[2]
    swap = lambda value: shift(value, "c", 1)
    tokens_c = swap(tokens)
    first, second = tokens[0], tokens[1]
    up0 = shift(first, "y", 1)
    down1 = shift(second, "y", -1)
    sums = [("p", on((2 * span, 2 * width), f32)), ("p", on((2 * span, head), f32))]
    early = kernel(
        early_kernel,
        sums + [("p", on((6 * depth, 2 * width), bf16)), ("p", on((PACK, 8 * depth), bf16))],
        "hphhhh",
        (tokens, tokens_c, beta_weight.T, decay_weight.T, key_weight, value_weight),
        (
            on((2, span, depth), bf16),
            on((2 * depth, 2 * width), bf16),
            on((2, 2, 8 * depth), bf16),
            dma((2,)),
        ),
    )
    early = list(early)
    first, second, *early[:2] = lax.optimization_barrier((first, second, *early[:2]))
    up1 = shift(second, "y", 1)
    down0 = shift(first, "y", -1)
    rest = early[2:]
    far0 = shift(up0, "y", 1)
    far1 = shift(down1, "y", -1)
    near = (up0, up1, down0, down1)
    swapped = []
    for value in near:
        swapped.append(swap(value))
    middle = kernel(
        functools.partial(middle_kernel, 2), sums, "p" * 12, (*near, *swapped, *early[:2], *rest)
    )
    far0, far1, *middle = lax.optimization_barrier((far0, far1, *middle))
    last = [far0, far1, swap(far0), swap(far1)]
    middle = kernel(
        functools.partial(middle_kernel, 6), sums, "p" * 6, (far0, far1, *middle, *rest)
    )
    far_c0, far_c1, *middle = lax.optimization_barrier((*last[2:], *middle))
    last[2:] = [far_c0, far_c1]
    local_shapes = [
        on((8, rows, head), bf16),
        on((2 * span, width), bf16),
        on((4, span, head), bf16),
        on((4, span, head), bf16),
        on((2, wide, head), f32),
        on((2, head, wide), f32),
    ]
    send, *shared = kernel(
        local_kernel,
        [("h", out) for out in local_shapes],
        "p" * 8,
        (beta_bias[None], rate_log[None], *last[2:], *middle, *rest),
        (*local_shapes, dma((6,))),
    )
    arrived = lax.all_to_all(send, NEAR, 0, 0, tiled=True)
    gain = out_gain[None]
    finals = [on((4, span, head), f32), on((4, span, head), bf16), on((4, span, head), f32)]
    local_out, reach, silu = kernel(
        window_kernel,
        [("h", out) for out in finals],
        "h" * 16 + "v" + "h" * 5,
        (tokens, tokens_c, *near, *swapped, *last, query_weight, gate_weight, gain, *shared),
        (
            on((8, 2, span, depth), bf16),
            on((8, depth, width), bf16),
            on((8, depth, width), bf16),
            dma((8,)),
            dma((8,)),
            *local_shapes[1:],
            *finals,
        ),
        24,
    )
    arrived, local_out = lax.optimization_barrier((arrived, local_out))
    total, maps, adds, factors = kernel(
        compose_kernel,
        [
            ("p", on((rows, head), bf16)),
            ("p", on((7, head, head), bf16)),
            ("p", on((7, half, head), f32)),
            ("p", on((7, 8, head), f32)),
        ],
        "p",
        (arrived,),
    )
    others = [
        lax.ppermute(total, "zh", [(at, at ^ by) for at in range(4)]) for by in (1, 2, 3)
    ]
    finals_in = kernel(
        load_kernel,
        [("p", out) for out in finals],
        "phhh",
        (total, local_out, reach, silu),
        (dma((3,)),),
    )
    *others, loaded = lax.optimization_barrier((*others, finals_in[0]))
    finals_in = (loaded, *finals_in[1:])
    (back,) = kernel(
        spread_kernel,
        [("p", on((8, half + PACK, head), bf16))],
        "p" * 12,
        (
            new_beta, new_decay, total, *others, maps, adds, factors,
            new_query, new_key, new_value,
        ),
        (on((4, rows, head), bf16), on((head, head), f32), on((head, head), f32)),
    )
    returned = lax.all_to_all(back, NEAR, 0, 0, tiled=True)
    return kernel(
        finish_kernel,
        [
            ("h", on((2, span, width), bf16)),
            ("v", on((2, 2, 4, head), bf16)),
            ("v", on((2, width), f32)),
        ],
        "ppppp",
        (returned, *finals_in, gain),
        (on((2, span, width), bf16), dma((4,))),
    )


def solution(mesh):
    torus = Mesh(mesh.devices.reshape(4, 2, 4, 4, 2), AXES + ("y", "c"))
    sp, tp = AXES, ("y", "c")
    weight = P(None, tp)
    in_specs = (
        P(None, sp, tp),
        weight, weight, weight, weight, weight, weight,
        P(tp), P(tp), P(),
        P(None, tp, None), P(None, tp, None), P(None, tp, None),
        P(None, tp), P(None, tp),
    )
    out_specs = (P(None, sp, tp), P(None, tp, sp, None), P(None, tp))

    return jax.shard_map(
        shards, mesh=torus, in_specs=in_specs, out_specs=out_specs, check_vma=False
    )
```

```python
import functools

import jax
import jax.numpy as jnp
from jax import lax
from jax.experimental import pallas as pl
from jax.experimental.pallas import tpu as pltpu
from jax.sharding import Mesh
from jax.sharding import PartitionSpec as P


NEAR = ("zl", "x")
AXES = ("zh", "zl", "x")
PACK = 16
LANES = 128
unit_floor = 1.0
norm_floor = 0.001
bf16 = jnp.bfloat16
f32 = jnp.float32


def dot(left, right, dims=((1,), (0,))):
    return lax.dot_general(
        left.astype(bf16), right.astype(bf16), (dims, ((), ())), preferred_element_type=f32
    )


ROWS = ((1,), (1,))
COLS = ((0,), (0,))


def thirds(value):
    high = value.astype(bf16).astype(f32)
    rest = value - high
    mid = rest.astype(bf16).astype(f32)
    return high, mid, rest - mid


def iota(shape, dim):
    return lax.broadcasted_iota(jnp.int32, shape, dim)


def row_pack(values, width):
    rows = iota((PACK, width), 0)
    packed = jnp.zeros((PACK, width), f32)
    for at, value in enumerate(values):
        packed = jnp.where(rows == at, value, packed)
    return packed


def rms_scale(values, floor, mean):
    total = jnp.sum(values * values, axis=-1, keepdims=True)
    return lax.rsqrt((total / values.shape[-1] if mean else total) + floor)


def shard_index(ahead, swapped):
    core = lax.axis_index("c")
    core = 1 - core if swapped else core
    return lax.rem(lax.axis_index("y") + ahead, 4) * 2 + core


def first_row(slot, depth):
    return pl.multiple_of(shard_index(*slot) * depth, depth)


def joined(first, second):
    return jnp.concatenate([first[...], second[...]], axis=0)


def scalar_part(rows, stacked, slot):
    depth = rows.shape[-1]
    weight = stacked[:, pl.ds(first_row(slot, depth), depth)]
    weight = jnp.concatenate([weight, jnp.zeros((LANES - PACK, depth), bf16)], axis=0)
    return dot(rows, weight, ROWS)


SLOTS = (
    (0, False), (0, True), (3, False), (1, False), (3, True), (1, True), (2, False), (2, True),
)


def split_kernel(source, first, second, sems):
    copies = [
        pltpu.make_async_copy(source.at[at], to, sems.at[at]) for at, to in enumerate((first, second))
    ]
    for copy in copies:
        copy.start()
    for copy in copies:
        copy.wait()


def early_kernel(
    own_first, own_second, own_c, beta_w, decay_w, key_w, value_w, sum_ref, gate_ref, rest_ref, stacked_ref,
    weight_buffer, scalar_buffer, sems,
):
    depth = own_c.shape[-1]
    width = key_w.shape[-1]
    first = []
    for at, weight in enumerate((beta_w, decay_w)):
        first.append(pltpu.make_async_copy(weight, scalar_buffer.at[at], sems.at[0]))
    later = []
    for at, slot in enumerate(SLOTS):
        start = first_row(slot, depth)
        for side, weight in enumerate((key_w, value_w)):
            lanes = pl.ds(side * width, width)
            source = weight.at[pl.ds(start, depth), :]
            if at < 2:
                to = weight_buffer.at[pl.ds(at * depth, depth), lanes]
                first.append(pltpu.make_async_copy(source, to, sems.at[0]))
            else:
                to = rest_ref.at[pl.ds((at - 2) * depth, depth), lanes]
                later.append(pltpu.make_async_copy(source, to, sems.at[1]))
    for copy in first + later:
        copy.start()
    for copy in first:
        copy.wait()
    rows = [scalar_buffer[at, h : h + 1, :].astype(f32) for at in range(2) for h in range(2)]
    stacked_ref[...] = row_pack(rows, stacked_ref.shape[-1]).astype(bf16)
    total = gates = 0.0
    for at in range(2):
        rows = own_c[...].reshape(-1, depth) if at else joined(own_first, own_second)
        total = total + dot(rows, weight_buffer[at * depth : (at + 1) * depth, :])
        gates = gates + scalar_part(rows, stacked_ref, SLOTS[at])
    sum_ref[...] = total
    gate_ref[...] = gates
    for copy in later:
        copy.wait()


def add_pieces(pieces, from_slot, rest, stacked, total, gates):
    for at in range(len(pieces) // 2):
        rows = joined(*pieces[2 * at : 2 * at + 2])
        depth = rows.shape[-1]
        slot = from_slot + at
        total = total + dot(rows, rest[(slot - 2) * depth : (slot - 1) * depth, :])
        gates = gates + scalar_part(rows, stacked, SLOTS[slot])
    return total, gates


def middle_kernel(first_slot, *refs):
    pieces, (sum_in, gate_in, rest, stacked, sum_ref, gate_ref) = refs[:-6], refs[-6:]
    total, gates = add_pieces(pieces, first_slot, rest, stacked, sum_in[...], gate_in[...])
    sum_ref[...] = total
    gate_ref[...] = gates


def lane_pair(ref, first):
    lanes = iota((1, LANES), 1)
    pair = ref[...]
    return jnp.where(
        lanes == first, pair[:, 0:1], jnp.where(lanes == first + 1, pair[:, 1:2], 0.0)
    )


def local_kernel(bias_ref, rate_ref, *refs):
    pieces, (sum_in, gate_in, rest, stacked) = refs[:2], refs[2:6]
    outputs, buffers, sems = refs[6:12], refs[12:18], refs[18]
    send_ref, key_ref, fresh_ref, carry_ref, cols_ref, rows_ref = buffers
    copies = []

    def give(at, part=None):
        source, to = buffers[at], outputs[at]
        if part is not None:
            source, to = source.at[part], to.at[part]
        copies.append(pltpu.make_async_copy(source, to, sems.at[at]))
        copies[-1].start()

    span = pieces[0].shape[0]
    head = send_ref.shape[-1]
    total, gates = add_pieces(pieces, 7, rest, stacked, sum_in[...], gate_in[...])
    width = total.shape[-1] // 2
    key_rows = total[:, :width].astype(bf16)
    value_rows = total[:, width:].astype(bf16)
    key_ref[...] = key_rows
    give(1)
    strength = jax.nn.sigmoid(gates + lane_pair(bias_ref, 0))
    decays = -jnp.exp(lane_pair(rate_ref, 2)) * jax.nn.softplus(gates)
    wide = cols_ref.shape[1]
    lanes = iota((wide, head), 1)
    causal_wide = (iota((wide, wide), 0) >= iota((wide, wide), 1)).astype(bf16)
    for seq in range(2):
        take = slice(seq * span, (seq + 1) * span)
        padded = jnp.concatenate([decays[take], jnp.zeros((wide - span, head), f32)], axis=0)
        cumulative = sum(dot(causal_wide, part) for part in thirds(padded))
        table = jnp.where((lanes == 2) | (lanes == 3), cumulative, 0.0)
        for h in range(2):
            keys = key_rows[take, h * head : (h + 1) * head].astype(f32)
            unit = jnp.concatenate(
                [rms_scale(keys, unit_floor, False), jnp.zeros((wide - span, 1), f32)], axis=0
            )
            beta = jnp.concatenate(
                [strength[take, h : h + 1], jnp.zeros((wide - span, 1), f32)], axis=0
            )
            table = jnp.where(lanes == h, beta, table)
            table = jnp.where(lanes == 4 + h, unit, table)
        cols_ref[seq] = table
        rows_ref[seq] = table.T
    give(4)
    give(5)
    half = head // 2
    t = iota((head, head), 0)
    s = iota((head, head), 1)
    apart = t ^ s
    upper, lower = slice(0, head), slice(head, span)
    blocks = []
    for pair in range(4):
        seq, h = divmod(pair, 2)
        keys = key_rows[seq * span : (seq + 1) * span, h * head : (h + 1) * head]

        def alike(of, with_, mask):
            col = lambda at: cols_ref[seq, of, at + h : at + h + 1]
            row = lambda at: rows_ref[seq, at + h : at + h + 1, with_]
            spread = col(2) - row(2)
            if mask is not None:
                spread = jnp.where(mask, spread, 0.0)
            product = dot(keys[of], keys[with_], ROWS)
            product = product * (col(0) * col(4)) * row(4) * jnp.exp(spread)
            return product if mask is None else jnp.where(mask, product, 0.0)

        def started(block):
            size = block.shape[0]
            near, same = apart[:size, :size] < 2, (t == s)[:size, :size]
            return jnp.where(same, 1.0, jnp.where(near, -block, 0.0)).astype(bf16)

        first = alike(upper, upper, t > s)
        second = alike(lower, lower, (t > s)[:half, :half])
        across = alike(lower, upper, None)
        blocks.append(
            [first.astype(bf16), second.astype(bf16), across.astype(bf16)]
            + [started(first), started(second)]
        )
    size = 2
    while size < half:
        mask = jnp.where((apart >= size) & (apart < 2 * size), 1.0, 0.0).astype(bf16)
        steps = []
        for first, second, _, x_first, x_second in blocks:
            step = dot(first * mask, x_first).astype(bf16)
            steps.append((step, dot(second * mask[:half, :half], x_second).astype(bf16)))
        for block, (step_first, step_second) in zip(blocks, steps):
            block[3] = block[3] - dot(block[3], step_first).astype(bf16)
            block[4] = block[4] - dot(block[4], step_second).astype(bf16)
        size *= 2
    left = jnp.where(iota((half, head), 1) < half, 1.0, 0.0).astype(bf16)
    blank = jnp.zeros((half, head), bf16)
    steps = [dot(block[0][half:] * left, block[3]).astype(bf16) for block in blocks]
    for block, step in zip(blocks, steps):
        change = dot(block[3][half:], jnp.concatenate([blank, step], axis=0)).astype(bf16)
        block[3] = jnp.concatenate([block[3][:half], block[3][half:] - change], axis=0)
    steps = [dot(block[2], block[3]).astype(bf16) for block in blocks]
    for pair in range(4):
        seq, h = divmod(pair, 2)
        take = slice(seq * span, (seq + 1) * span)
        keys = key_rows[take, h * head : (h + 1) * head]
        values = value_rows[take, h * head : (h + 1) * head]
        col = lambda at: cols_ref[seq, :span, at + h : at + h + 1]
        row = lambda at: rows_ref[seq, at + h : at + h + 1, :span]
        off_first = jnp.where(t == s, 0.0, blocks[pair][3].astype(f32))
        off_second = jnp.where((t == s)[:half, :half], 0.0, blocks[pair][4].astype(f32))
        off_across = -dot(blocks[pair][4], steps[pair])

        def applied(weight, right):
            top = dot(off_first * weight[:, upper], right[upper])
            low = dot(off_across * weight[:, upper], right[upper])
            low = low + dot(off_second * weight[:, lower], right[lower])
            return jnp.concatenate([top, low], axis=0)

        fresh = col(0) * values.astype(f32) + applied(row(0), values)
        carry = (col(0) * col(4) * jnp.exp(col(2))) * keys.astype(f32) + applied(
            row(0) * row(4) * jnp.exp(row(2)), keys
        )
        last = cols_ref[seq, span - 1 : span, 2 + h : 3 + h]
        late = col(4) * jnp.exp(last - col(2))
        reach = dot(carry * late, keys, COLS)
        gain = dot(fresh * late, keys, COLS)
        fresh_ref[pair] = fresh.astype(bf16)
        carry_ref[pair] = carry.astype(bf16)
        give(2, pair)
        give(3, pair)
        factor = row_pack(thirds(jnp.broadcast_to(jnp.exp(last), (1, head))), head)
        for side in range(2):
            to = 2 * pair + side
            send_ref[to, :head, :] = reach.astype(bf16)
            send_ref[to, head : head + half, :] = gain[side * half : (side + 1) * half].astype(bf16)
            send_ref[to, head + half :, :] = factor.astype(bf16)
        give(0, pl.ds(2 * pair, 2))
    for copy in copies:
        copy.wait()


def window_kernel(*refs):
    pieces, refs = refs[:14], refs[14:]
    query_w, gate_w, gain_ref, shared, refs = refs[0], refs[1], refs[2], refs[3:8], refs[8:]
    outputs, refs = refs[:3], refs[3:]
    token_buffer, query_buffer, gate_buffer, sems, more_sems = refs[:5]
    shared_buffers, output_buffers = refs[5:10], refs[10:]
    key_ref, fresh_ref, carry_ref, cols_ref, rows_ref = shared_buffers
    out_ref, reach_ref, silu_ref = output_buffers
    span, depth = token_buffer.shape[2:]
    head = fresh_ref.shape[-1]
    weights = ((query_w, query_buffer), (gate_w, gate_buffer))
    copies = []
    for at, slot in enumerate(SLOTS):
        if at < 2:
            parts = [(pieces[at], token_buffer.at[at])]
        else:
            parts = [(pieces[2 * at - 2 + seq], token_buffer.at[at, seq]) for seq in range(2)]
        for weight, buffer in weights:
            parts.append((weight.at[pl.ds(first_row(slot, depth), depth), :], buffer.at[at]))
        copies.append([pltpu.make_async_copy(a, b, sems.at[at]) for a, b in parts])
        for copy in copies[at]:
            copy.start()
    given = [
        pltpu.make_async_copy(a, b, more_sems.at[at])
        for at, (a, b) in enumerate(zip(shared, shared_buffers))
    ]
    for copy in given:
        copy.start()
    query_total = gate_total = 0.0
    for at in range(8):
        for copy in copies[at]:
            copy.wait()
        rows = token_buffer[at].reshape(-1, depth)
        query_total = query_total + dot(rows, query_buffer[at])
        gate_total = gate_total + dot(rows, gate_buffer[at])
    for copy in given:
        copy.wait()
    query_rows = query_total.astype(bf16)
    gate_rows = gate_total.astype(bf16).astype(f32)
    t = iota((span, span), 0)
    s = iota((span, span), 1)
    taken = []
    for pair in range(4):
        seq, h = divmod(pair, 2)
        take = slice(seq * span, (seq + 1) * span)
        part = slice(h * head, (h + 1) * head)
        col = lambda at: cols_ref[seq, :span, at + h : at + h + 1]
        row = lambda at: rows_ref[seq, at + h : at + h + 1, :span]
        queries = query_rows[take, part]
        unit = rms_scale(queries.astype(f32), unit_floor, False)
        spread = jnp.where(t >= s, col(2) - row(2), 0.0)
        scores = dot(queries, key_ref[take, part], ROWS) * unit * row(4) * jnp.exp(spread)
        scores = jnp.where(t >= s, scores, 0.0).astype(bf16)
        out_ref[pair] = dot(scores, fresh_ref[pair])
        reach = (unit * jnp.exp(col(2))) * queries.astype(f32) - dot(scores, carry_ref[pair])
        reach_ref[pair] = reach.astype(bf16)
        gate = gate_rows[take, part]
        silu_ref[pair] = gain_ref[...] * gate * jax.nn.sigmoid(gate)
        for at, (a, b) in enumerate(zip(output_buffers, outputs)):
            taken.append(pltpu.make_async_copy(a.at[pair], b.at[pair], more_sems.at[5 + at]))
            taken[-1].start()
    for copy in taken:
        copy.wait()


def unpack_factor(block):
    block = block.astype(f32)
    return block[0:1] + block[1:2] + block[2:3]


def load_member(in_ref, at):
    body = in_ref.shape[1] - PACK
    return in_ref[at, :body, :].astype(f32), unpack_factor(in_ref[at, body:, :])


def join(first, second):
    both, factor = first
    later, later_factor = second
    head = later.shape[-1]
    tail = jnp.concatenate([factor * later[:head], later[head:]], axis=0)
    return later_factor * both - dot(both, later[:head]) + tail, factor * later_factor


def total_kernel(in_ref, total_ref):
    parts = [load_member(in_ref, at) for at in range(in_ref.shape[0])]
    while len(parts) > 1:
        parts = [join(parts[at], parts[at + 1]) for at in range(0, len(parts), 2)]
    both, factor = parts[0]
    body, head = both.shape
    total_ref[:body, :] = both.astype(bf16)
    total_ref[body:, :] = row_pack(thirds(factor), head).astype(bf16)


def prefix_kernel(_, in_ref, out_in, reach_in, silu_in, *refs):
    maps_ref, adds_ref, factors_ref, out_ref, reach_ref, silu_ref, sems = refs
    moved = ((out_in, out_ref), (reach_in, reach_ref), (silu_in, silu_ref))
    copies = [pltpu.make_async_copy(a, b, sems.at[at]) for at, (a, b) in enumerate(moved)]
    for copy in copies:
        copy.start()
    count, _, head = in_ref.shape
    member = [load_member(in_ref, at) for at in range(count - 1)]
    c23, c45 = (join(member[at], member[at + 1]) for at in (2, 4))
    upto = [None, member[0], join(member[0], member[1])]
    c456 = join(c45, member[6])
    upto.append(join(upto[2], member[2]))
    upto.append(join(upto[2], c23))
    upto.append(join(upto[4], member[4]))
    upto.append(join(upto[4], c45))
    upto.append(join(upto[4], c456))
    for at in range(1, count):
        both, factor = upto[at]
        maps_ref[at - 1] = both[:head].astype(bf16)
        adds_ref[at - 1] = both[head:]
        factors_ref[at - 1] = jnp.broadcast_to(factor, (8, head))
    for copy in copies:
        copy.wait()


def spread_kernel(
    beta_ref, decay_ref, own, back1, back2, back3, maps_ref, adds_ref, factors_ref,
    query_ref, key_ref, value_ref, send_ref, groups_ref, wide_ref, turned_ref,
):
    _, head = own.shape
    half = head // 2
    far = lax.axis_index("zh")
    near = lax.axis_index("zl") * 4 + lax.axis_index("x")
    pair = near // 2
    side = near % 2

    def scalar(ref):
        total = jnp.zeros((1, 1), f32)
        for at in range(4):
            entry = ref[at // 2 : at // 2 + 1, at % 2 : at % 2 + 1]
            total = jnp.where(pair == at, entry, total)
        return total

    def chosen(ref):
        total = jnp.zeros((1, head), f32)
        for at in range(4):
            row = ref[at // 2, at % 2 : at % 2 + 1, :].astype(f32)
            total = jnp.where(pair == at, row, total)
        return total

    for slot, ref in enumerate((own, back1, back2, back3)):
        groups_ref[slot] = ref[...]
    state = jnp.zeros((half, head), f32)
    begin = state
    for group in range(4):
        begin = jnp.where(far == group, state, begin)
        block = groups_ref[lax.bitwise_xor(far, group)]
        added = block[head : head + half].astype(f32)
        if group:
            state = unpack_factor(block[head + half :]) * state - dot(state, block[:head]) + added
        else:
            state = added
    final = state.astype(bf16).astype(f32)
    wide_ref[...] = jnp.zeros((head, head), f32)
    wide_ref[pl.ds(pl.multiple_of(side * half, half), half), :] = final
    padded = wide_ref[...]
    turned_ref[...] = padded.T
    mine = turned_ref[pl.ds(pl.multiple_of(far * 32, 32), 32), :]
    query = chosen(query_ref)
    key = chosen(key_ref)
    query = query * rms_scale(query, unit_floor, False)
    key = key * rms_scale(key, unit_floor, False)
    hits = dot(row_pack(thirds(query) + thirds(key), head), padded, ROWS)
    recall = hits[0:1] + hits[1:2] + hits[2:3]
    retrieve = hits[3:4] + hits[4:5] + hits[5:6]
    decay = scalar(decay_ref)
    intersect = jnp.sum(key * query, axis=-1, keepdims=True)
    fresh = chosen(value_ref) - decay * retrieve
    read = decay * recall + (scalar(beta_ref) * intersect) * fresh
    read = jnp.where(iota((1, head), 1) // half == side, read, 0.0)
    zero = jnp.zeros((1, head), f32)
    extra = row_pack((zero, zero, zero, zero) + thirds(read), head)
    pick_row = iota((PACK, 32), 0)
    pick_col = iota((PACK, 32), 1)
    for member in range(8):
        if member:
            at = member - 1
            entry = factors_ref[at, 0:1, :] * begin - dot(begin, maps_ref[at]) + adds_ref[at]
        else:
            entry = begin
        send_ref[member, :half, :] = entry.astype(bf16)
        pick = ((pick_row < 4) & (pick_col == 4 * member + pick_row)).astype(bf16)
        send_ref[member, half:, :] = (dot(pick, mine) + extra).astype(bf16)


def finish_kernel(in_ref, out_ref, reach_ref, silu_ref, gain_ref, mixed_ref, cache_ref, read_ref):
    head = in_ref.shape[-1]
    half = head // 2
    for pair in range(4):
        seq, h = divmod(pair, 2)
        incoming = jnp.concatenate([in_ref[2 * pair, :half, :], in_ref[2 * pair + 1, :half, :]], 0)
        whole = out_ref[pair] + dot(reach_ref[pair], incoming, ROWS)
        mixed = whole * rms_scale(whole, norm_floor, True) * silu_ref[pair]
        mixed_ref[seq, :, h * head : (h + 1) * head] = mixed.astype(bf16)
        extra = in_ref[2 * pair, half:, :].astype(f32) + in_ref[2 * pair + 1, half:, :].astype(f32)
        cache_ref[seq, h] = extra[:4].astype(bf16)
        read = extra[4:5] + extra[5:6] + extra[6:7]
        read = read * rms_scale(read, norm_floor, True) * gain_ref[...]
        read_ref[seq : seq + 1, h * head : (h + 1) * head] = read


def vmem():
    return pl.BlockSpec(memory_space=pltpu.VMEM)


def smem():
    return pl.BlockSpec(memory_space=pltpu.SMEM)


def kernel(body, outputs, kinds, args, scratch=(), limit=16):
    given = {"s": smem, "v": vmem, "p": vmem, "h": lambda: pl.BlockSpec(memory_space=pl.ANY)}
    placed = [
        arg
        if kind == "s"
        else pltpu.with_memory_space_constraint(arg, pltpu.VMEM if kind == "p" else pltpu.HBM)
        for kind, arg in zip(kinds, args, strict=True)
    ]
    plain = lambda out: pltpu.HBM(out.shape, out.dtype)
    return pl.pallas_call(
        body,
        out_shape=tuple(out if kind == "p" else plain(out) for kind, out in outputs),
        in_specs=[given[kind]() for kind in kinds],
        out_specs=tuple(given[kind]() for kind, _ in outputs),
        scratch_shapes=list(scratch),
        compiler_params=pltpu.CompilerParams(vmem_limit_bytes=limit * 1024 * 1024),
    )(*placed)


def shift(value, axis, by):
    length = lax.axis_size(axis)
    return lax.ppermute(value, axis, [(at, (at + by) % length) for at in range(length)])


def shards(
    tokens, query_weight, key_weight, value_weight, gate_weight, beta_weight, decay_weight,
    beta_bias, rate_log, out_gain, new_query, new_key, new_value, new_beta, new_decay,
):
    _, span, depth = tokens.shape
    head = out_gain.shape[0]
    half = head // 2
    wide = 256
    width = query_weight.shape[1]
    rows = head + half + PACK
    on, dma = pltpu.VMEM, pltpu.SemaphoreType.DMA
    depth = tokens.shape[2]
    swap = lambda value: shift(value, "c", 1)
    tokens_c = swap(tokens)
    half_span = ("p", on((span, depth), bf16))
    first, second = kernel(split_kernel, [half_span, half_span], "h", (tokens,), (dma((2,)),))
    up0 = shift(first, "y", 1)
    down1 = shift(second, "y", -1)
    sums = [("p", on((2 * span, 2 * width), f32)), ("p", on((2 * span, head), f32))]
    early = kernel(
        early_kernel,
        sums + [("p", on((6 * depth, 2 * width), bf16)), ("p", on((PACK, 8 * depth), bf16))],
        "ppphhhh",
        (first, second, tokens_c, beta_weight.T, decay_weight.T, key_weight, value_weight),
        (
            on((2 * depth, 2 * width), bf16),
            on((2, 2, 8 * depth), bf16),
            dma((2,)),
        ),
    )
    early = list(early)
    first, second, *early[:2] = lax.optimization_barrier((first, second, *early[:2]))
    up1 = shift(second, "y", 1)
    down0 = shift(first, "y", -1)
    rest = early[2:]
    far0 = shift(up0, "y", 1)
    far1 = shift(down1, "y", -1)
    near = (up0, up1, down0, down1)
    swapped = []
    for value in near:
        swapped.append(swap(value))
    middle = kernel(
        functools.partial(middle_kernel, 2), sums, "p" * 12, (*near, *swapped, *early[:2], *rest)
    )
    far0, far1, *middle = lax.optimization_barrier((far0, far1, *middle))
    last = [far0, far1, swap(far0), swap(far1)]
    middle = kernel(
        functools.partial(middle_kernel, 6), sums, "p" * 6, (far0, far1, *middle, *rest)
    )
    far_c0, far_c1, *middle = lax.optimization_barrier((*last[2:], *middle))
    last[2:] = [far_c0, far_c1]
    local_shapes = [
        on((8, rows, head), bf16),
        on((2 * span, width), bf16),
        on((4, span, head), bf16),
        on((4, span, head), bf16),
        on((2, wide, head), f32),
        on((2, head, wide), f32),
    ]
    send, *shared = kernel(
        local_kernel,
        [("h", out) for out in local_shapes],
        "p" * 8,
        (beta_bias[None], rate_log[None], *last[2:], *middle, *rest),
        (*local_shapes, dma((6,))),
    )
    arrived = lax.all_to_all(send, NEAR, 0, 0, tiled=True)
    gain = out_gain[None]
    finals = [on((4, span, head), f32), on((4, span, head), bf16), on((4, span, head), f32)]
    local_out, reach, silu = kernel(
        window_kernel,
        [("h", out) for out in finals],
        "h" * 16 + "v" + "h" * 5,
        (tokens, tokens_c, *near, *swapped, *last, query_weight, gate_weight, gain, *shared),
        (
            on((8, 2, span, depth), bf16),
            on((8, depth, width), bf16),
            on((8, depth, width), bf16),
            dma((8,)),
            dma((8,)),
            *local_shapes[1:],
            *finals,
        ),
        24,
    )
    arrived, local_out = lax.optimization_barrier((arrived, local_out))
    (total,) = kernel(total_kernel, [("p", on((rows, head), bf16))], "p", (arrived,))
    others = [
        lax.ppermute(total, "zh", [(at, at ^ by) for at in range(4)]) for by in (1, 2, 3)
    ]
    maps, adds, factors, *finals_in = kernel(
        prefix_kernel,
        [
            ("p", on((7, head, head), bf16)),
            ("p", on((7, half, head), f32)),
            ("p", on((7, 8, head), f32)),
            *(("p", out) for out in finals),
        ],
        "pphhh",
        (total, arrived, local_out, reach, silu),
        (dma((3,)),),
    )
    *others, maps = lax.optimization_barrier((*others, maps))
    (back,) = kernel(
        spread_kernel,
        [("p", on((8, half + PACK, head), bf16))],
        "p" * 12,
        (
            new_beta, new_decay, total, *others, maps, adds, factors,
            new_query, new_key, new_value,
        ),
        (on((4, rows, head), bf16), on((head, head), f32), on((head, head), f32)),
    )
    returned = lax.all_to_all(back, NEAR, 0, 0, tiled=True)
    return kernel(
        finish_kernel,
        [
            ("v", on((2, span, width), bf16)),
            ("v", on((2, 2, 4, head), bf16)),
            ("v", on((2, width), f32)),
        ],
        "ppppp",
        (returned, *finals_in, gain),
    )


def solution(mesh):
    torus = Mesh(mesh.devices.reshape(4, 2, 4, 4, 2), AXES + ("y", "c"))
    sp, tp = AXES, ("y", "c")
    weight = P(None, tp)
    in_specs = (
        P(None, sp, tp),
        weight, weight, weight, weight, weight, weight,
        P(tp), P(tp), P(),
        P(None, tp, None), P(None, tp, None), P(None, tp, None),
        P(None, tp), P(None, tp),
    )
    out_specs = (P(None, sp, tp), P(None, tp, sp, None), P(None, tp))

    return jax.shard_map(
        shards, mesh=torus, in_specs=in_specs, out_specs=out_specs, check_vma=False
    )
```

```python
import functools

import jax
import jax.numpy as jnp
from jax import lax
from jax.experimental import pallas as pl
from jax.experimental.pallas import tpu as pltpu
from jax.sharding import Mesh
from jax.sharding import PartitionSpec as P


NEAR = ("zl", "x")
AXES = ("zh", "zl", "x")
PACK = 16
LANES = 128
unit_floor = 1.0
norm_floor = 0.001
bf16 = jnp.bfloat16
f32 = jnp.float32


def dot(left, right, dims=((1,), (0,))):
    return lax.dot_general(
        left.astype(bf16), right.astype(bf16), (dims, ((), ())), preferred_element_type=f32
    )


ROWS = ((1,), (1,))
COLS = ((0,), (0,))


def thirds(value):
    high = value.astype(bf16).astype(f32)
    rest = value - high
    mid = rest.astype(bf16).astype(f32)
    return high, mid, rest - mid


def iota(shape, dim):
    return lax.broadcasted_iota(jnp.int32, shape, dim)


def row_pack(values, width):
    rows = iota((PACK, width), 0)
    packed = jnp.zeros((PACK, width), f32)
    for at, value in enumerate(values):
        packed = jnp.where(rows == at, value, packed)
    return packed


def rms_scale(values, floor, mean):
    total = jnp.sum(values * values, axis=-1, keepdims=True)
    return lax.rsqrt((total / values.shape[-1] if mean else total) + floor)


def shard_index(ahead, swapped):
    core = lax.axis_index("c")
    core = 1 - core if swapped else core
    return lax.rem(lax.axis_index("y") + ahead, 4) * 2 + core


def first_row(slot, depth):
    return pl.multiple_of(shard_index(*slot) * depth, depth)


def joined(first, second):
    return jnp.concatenate([first[...], second[...]], axis=0)


def scalar_part(rows, stacked, slot):
    depth = rows.shape[-1]
    weight = stacked[:, pl.ds(first_row(slot, depth), depth)]
    weight = jnp.concatenate([weight, jnp.zeros((LANES - PACK, depth), bf16)], axis=0)
    return dot(rows, weight, ROWS)


SLOTS = (
    (0, False), (0, True), (3, False), (1, False), (3, True), (1, True), (2, False), (2, True),
)


def split_kernel(source, first, second, sems):
    copies = [
        pltpu.make_async_copy(source.at[at], to, sems.at[at]) for at, to in enumerate((first, second))
    ]
    for copy in copies:
        copy.start()
    for copy in copies:
        copy.wait()


def early_kernel(
    own_first, own_second, own_c, beta_w, decay_w, key_w, value_w, sum_ref, gate_ref, rest_ref, stacked_ref,
    weight_buffer, scalar_buffer, sems,
):
    depth = own_c.shape[-1]
    width = key_w.shape[-1]
    first = []
    for at, weight in enumerate((beta_w, decay_w)):
        first.append(pltpu.make_async_copy(weight, scalar_buffer.at[at], sems.at[0]))
    later = []
    for at, slot in enumerate(SLOTS):
        start = first_row(slot, depth)
        for side, weight in enumerate((key_w, value_w)):
            lanes = pl.ds(side * width, width)
            source = weight.at[pl.ds(start, depth), :]
            if at < 2:
                to = weight_buffer.at[pl.ds(at * depth, depth), lanes]
                first.append(pltpu.make_async_copy(source, to, sems.at[0]))
            else:
                to = rest_ref.at[pl.ds((at - 2) * depth, depth), lanes]
                later.append(pltpu.make_async_copy(source, to, sems.at[1]))
    for copy in first + later:
        copy.start()
    for copy in first:
        copy.wait()
    rows = [scalar_buffer[at, h : h + 1, :].astype(f32) for at in range(2) for h in range(2)]
    stacked_ref[...] = row_pack(rows, stacked_ref.shape[-1]).astype(bf16)
    total = gates = 0.0
    for at in range(2):
        rows = own_c[...].reshape(-1, depth) if at else joined(own_first, own_second)
        total = total + dot(rows, weight_buffer[at * depth : (at + 1) * depth, :])
        gates = gates + scalar_part(rows, stacked_ref, SLOTS[at])
    sum_ref[...] = total
    gate_ref[...] = gates
    for copy in later:
        copy.wait()


def add_pieces(pieces, from_slot, rest, stacked, total, gates):
    for at in range(len(pieces) // 2):
        rows = joined(*pieces[2 * at : 2 * at + 2])
        depth = rows.shape[-1]
        slot = from_slot + at
        total = total + dot(rows, rest[(slot - 2) * depth : (slot - 1) * depth, :])
        gates = gates + scalar_part(rows, stacked, SLOTS[slot])
    return total, gates


def middle_kernel(first_slot, *refs):
    pieces, (sum_in, gate_in, rest, stacked, sum_ref, gate_ref) = refs[:-6], refs[-6:]
    total, gates = add_pieces(pieces, first_slot, rest, stacked, sum_in[...], gate_in[...])
    sum_ref[...] = total
    gate_ref[...] = gates


def lane_pair(ref, first):
    lanes = iota((1, LANES), 1)
    pair = ref[...]
    return jnp.where(
        lanes == first, pair[:, 0:1], jnp.where(lanes == first + 1, pair[:, 1:2], 0.0)
    )


def local_kernel(bias_ref, rate_ref, *refs):
    pieces, (sum_in, gate_in, rest, stacked) = refs[:2], refs[2:6]
    outputs, buffers, sems = refs[6:12], refs[12:18], refs[18]
    send_ref, key_ref, fresh_ref, carry_ref, cols_ref, rows_ref = buffers
    copies = []

    def give(at, part=None):
        source, to = buffers[at], outputs[at]
        if part is not None:
            source, to = source.at[part], to.at[part]
        copies.append(pltpu.make_async_copy(source, to, sems.at[at]))
        copies[-1].start()

    span = pieces[0].shape[0]
    head = send_ref.shape[-1]
    total, gates = add_pieces(pieces, 7, rest, stacked, sum_in[...], gate_in[...])
    width = total.shape[-1] // 2
    key_rows = total[:, :width].astype(bf16)
    value_rows = total[:, width:].astype(bf16)
    key_ref[...] = key_rows
    give(1)
    strength = jax.nn.sigmoid(gates + lane_pair(bias_ref, 0))
    decays = -jnp.exp(lane_pair(rate_ref, 2)) * jax.nn.softplus(gates)
    wide = cols_ref.shape[1]
    lanes = iota((wide, head), 1)
    causal_wide = (iota((wide, wide), 0) >= iota((wide, wide), 1)).astype(bf16)
    for seq in range(2):
        take = slice(seq * span, (seq + 1) * span)
        padded = jnp.concatenate([decays[take], jnp.zeros((wide - span, head), f32)], axis=0)
        cumulative = sum(dot(causal_wide, part) for part in thirds(padded))
        table = jnp.where((lanes == 2) | (lanes == 3), cumulative, 0.0)
        for h in range(2):
            keys = key_rows[take, h * head : (h + 1) * head].astype(f32)
            unit = jnp.concatenate(
                [rms_scale(keys, unit_floor, False), jnp.zeros((wide - span, 1), f32)], axis=0
            )
            beta = jnp.concatenate(
                [strength[take, h : h + 1], jnp.zeros((wide - span, 1), f32)], axis=0
            )
            table = jnp.where(lanes == h, beta, table)
            table = jnp.where(lanes == 4 + h, unit, table)
        cols_ref[seq] = table
        rows_ref[seq] = table.T
    give(4)
    give(5)
    half = head // 2
    t = iota((head, head), 0)
    s = iota((head, head), 1)
    apart = t ^ s
    upper, lower = slice(0, head), slice(head, span)
    blocks = []
    for pair in range(4):
        seq, h = divmod(pair, 2)
        keys = key_rows[seq * span : (seq + 1) * span, h * head : (h + 1) * head]

        def alike(of, with_, mask):
            col = lambda at: cols_ref[seq, of, at + h : at + h + 1]
            row = lambda at: rows_ref[seq, at + h : at + h + 1, with_]
            spread = col(2) - row(2)
            if mask is not None:
                spread = jnp.where(mask, spread, 0.0)
            product = dot(keys[of], keys[with_], ROWS)
            product = product * (col(0) * col(4)) * row(4) * jnp.exp(spread)
            return product if mask is None else jnp.where(mask, product, 0.0)

        def started(block):
            size = block.shape[0]
            near, same = apart[:size, :size] < 2, (t == s)[:size, :size]
            return jnp.where(same, 1.0, jnp.where(near, -block, 0.0)).astype(bf16)

        first = alike(upper, upper, t > s)
        second = alike(lower, lower, (t > s)[:half, :half])
        across = alike(lower, upper, None)
        blocks.append(
            [first.astype(bf16), second.astype(bf16), across.astype(bf16)]
            + [started(first), started(second)]
        )
    size = 2
    while size < half:
        mask = jnp.where((apart >= size) & (apart < 2 * size), 1.0, 0.0).astype(bf16)
        steps = []
        for first, second, _, x_first, x_second in blocks:
            step = dot(first * mask, x_first).astype(bf16)
            steps.append((step, dot(second * mask[:half, :half], x_second).astype(bf16)))
        for block, (step_first, step_second) in zip(blocks, steps):
            block[3] = block[3] - dot(block[3], step_first).astype(bf16)
            block[4] = block[4] - dot(block[4], step_second).astype(bf16)
        size *= 2
    left = jnp.where(iota((half, head), 1) < half, 1.0, 0.0).astype(bf16)
    blank = jnp.zeros((half, head), bf16)
    steps = [dot(block[0][half:] * left, block[3]).astype(bf16) for block in blocks]
    for block, step in zip(blocks, steps):
        change = dot(block[3][half:], jnp.concatenate([blank, step], axis=0)).astype(bf16)
        block[3] = jnp.concatenate([block[3][:half], block[3][half:] - change], axis=0)
    steps = [dot(block[2], block[3]).astype(bf16) for block in blocks]
    for pair in range(4):
        seq, h = divmod(pair, 2)
        take = slice(seq * span, (seq + 1) * span)
        keys = key_rows[take, h * head : (h + 1) * head]
        values = value_rows[take, h * head : (h + 1) * head]
        col = lambda at: cols_ref[seq, :span, at + h : at + h + 1]
        row = lambda at: rows_ref[seq, at + h : at + h + 1, :span]
        off_first = jnp.where(t == s, 0.0, blocks[pair][3].astype(f32))
        off_second = jnp.where((t == s)[:half, :half], 0.0, blocks[pair][4].astype(f32))
        off_across = -dot(blocks[pair][4], steps[pair])

        def applied(weight, right):
            top = dot(off_first * weight[:, upper], right[upper])
            low = dot(off_across * weight[:, upper], right[upper])
            low = low + dot(off_second * weight[:, lower], right[lower])
            return jnp.concatenate([top, low], axis=0)

        fresh = col(0) * values.astype(f32) + applied(row(0), values)
        carry = (col(0) * col(4) * jnp.exp(col(2))) * keys.astype(f32) + applied(
            row(0) * row(4) * jnp.exp(row(2)), keys
        )
        last = cols_ref[seq, span - 1 : span, 2 + h : 3 + h]
        late = col(4) * jnp.exp(last - col(2))
        reach = dot(carry * late, keys, COLS)
        gain = dot(fresh * late, keys, COLS)
        fresh_ref[pair] = fresh.astype(bf16)
        carry_ref[pair] = carry.astype(bf16)
        give(2, pair)
        give(3, pair)
        factor = row_pack(thirds(jnp.broadcast_to(jnp.exp(last), (1, head))), head)
        for side in range(2):
            to = 2 * pair + side
            send_ref[to, :head, :] = reach.astype(bf16)
            send_ref[to, head : head + half, :] = gain[side * half : (side + 1) * half].astype(bf16)
            send_ref[to, head + half :, :] = factor.astype(bf16)
        give(0, pl.ds(2 * pair, 2))
    for copy in copies:
        copy.wait()


def window_kernel(*refs):
    pieces, refs = refs[:14], refs[14:]
    query_w, gate_w, gain_ref, shared, refs = refs[0], refs[1], refs[2], refs[3:8], refs[8:]
    outputs, refs = refs[:3], refs[3:]
    token_buffer, query_buffer, gate_buffer, sems, more_sems = refs[:5]
    shared_buffers, output_buffers = refs[5:10], refs[10:]
    key_ref, fresh_ref, carry_ref, cols_ref, rows_ref = shared_buffers
    out_ref, reach_ref, silu_ref = output_buffers
    span, depth = token_buffer.shape[2:]
    head = fresh_ref.shape[-1]
    weights = ((query_w, query_buffer), (gate_w, gate_buffer))
    copies = []
    for at, slot in enumerate(SLOTS):
        if at < 2:
            parts = [(pieces[at], token_buffer.at[at])]
        else:
            parts = [(pieces[2 * at - 2 + seq], token_buffer.at[at, seq]) for seq in range(2)]
        for weight, buffer in weights:
            parts.append((weight.at[pl.ds(first_row(slot, depth), depth), :], buffer.at[at]))
        copies.append([pltpu.make_async_copy(a, b, sems.at[at]) for a, b in parts])
        for copy in copies[at]:
            copy.start()
    given = [
        pltpu.make_async_copy(a, b, more_sems.at[at])
        for at, (a, b) in enumerate(zip(shared, shared_buffers))
    ]
    for copy in given:
        copy.start()
    query_total = gate_total = 0.0
    for at in range(8):
        for copy in copies[at]:
            copy.wait()
        rows = token_buffer[at].reshape(-1, depth)
        query_total = query_total + dot(rows, query_buffer[at])
        gate_total = gate_total + dot(rows, gate_buffer[at])
    for copy in given:
        copy.wait()
    query_rows = query_total.astype(bf16)
    gate_rows = gate_total.astype(bf16).astype(f32)
    t = iota((span, span), 0)
    s = iota((span, span), 1)
    taken = []
    for pair in range(4):
        seq, h = divmod(pair, 2)
        take = slice(seq * span, (seq + 1) * span)
        part = slice(h * head, (h + 1) * head)
        col = lambda at: cols_ref[seq, :span, at + h : at + h + 1]
        row = lambda at: rows_ref[seq, at + h : at + h + 1, :span]
        queries = query_rows[take, part]
        unit = rms_scale(queries.astype(f32), unit_floor, False)
        spread = jnp.where(t >= s, col(2) - row(2), 0.0)
        scores = dot(queries, key_ref[take, part], ROWS) * unit * row(4) * jnp.exp(spread)
        scores = jnp.where(t >= s, scores, 0.0).astype(bf16)
        out_ref[pair] = dot(scores, fresh_ref[pair])
        reach = (unit * jnp.exp(col(2))) * queries.astype(f32) - dot(scores, carry_ref[pair])
        reach_ref[pair] = reach.astype(bf16)
        gate = gate_rows[take, part]
        silu_ref[pair] = gain_ref[...] * gate * jax.nn.sigmoid(gate)
        for at, (a, b) in enumerate(zip(output_buffers, outputs)):
            taken.append(pltpu.make_async_copy(a.at[pair], b.at[pair], more_sems.at[5 + at]))
            taken[-1].start()
    for copy in taken:
        copy.wait()


def unpack_factor(block):
    block = block.astype(f32)
    return block[0:1] + block[1:2] + block[2:3]


def load_member(in_ref, at):
    body = in_ref.shape[1] - PACK
    return in_ref[at, :body, :].astype(f32), unpack_factor(in_ref[at, body:, :])


def join(first, second):
    both, factor = first
    later, later_factor = second
    head = later.shape[-1]
    tail = jnp.concatenate([factor * later[:head], later[head:]], axis=0)
    return later_factor * both - dot(both, later[:head]) + tail, factor * later_factor


def total_kernel(in_ref, total_ref):
    parts = [load_member(in_ref, at) for at in range(in_ref.shape[0])]
    while len(parts) > 1:
        parts = [join(parts[at], parts[at + 1]) for at in range(0, len(parts), 2)]
    both, factor = parts[0]
    body, head = both.shape
    total_ref[:body, :] = both.astype(bf16)
    total_ref[body:, :] = row_pack(thirds(factor), head).astype(bf16)


def prefix_kernel(_, in_ref, out_in, reach_in, silu_in, *refs):
    maps_ref, adds_ref, factors_ref, out_ref, reach_ref, silu_ref, sems = refs
    moved = ((out_in, out_ref), (reach_in, reach_ref), (silu_in, silu_ref))
    copies = [pltpu.make_async_copy(a, b, sems.at[at]) for at, (a, b) in enumerate(moved)]
    for copy in copies:
        copy.start()
    count, _, head = in_ref.shape
    member = [load_member(in_ref, at) for at in range(count - 1)]
    c23, c45 = (join(member[at], member[at + 1]) for at in (2, 4))
    upto = [None, member[0], join(member[0], member[1])]
    c456 = join(c45, member[6])
    upto.append(join(upto[2], member[2]))
    upto.append(join(upto[2], c23))
    upto.append(join(upto[4], member[4]))
    upto.append(join(upto[4], c45))
    upto.append(join(upto[4], c456))
    for at in range(1, count):
        both, factor = upto[at]
        maps_ref[at - 1] = both[:head].astype(bf16)
        adds_ref[at - 1] = both[head:]
        factors_ref[at - 1] = jnp.broadcast_to(factor, (8, head))
    for copy in copies:
        copy.wait()


def split_total(ref):
    body = ref.shape[0] - PACK
    return ref[:body, :].astype(f32), unpack_factor(ref[body:, :])


def chosen_total(flag, first, second):
    return tuple(jnp.where(flag, a, b) for a, b in zip(first, second))


def pair_kernel(own_ref, near_ref, pair_ref):
    odd = lax.axis_index("zh") % 2 == 1
    own, near = split_total(own_ref), split_total(near_ref)
    both, factor = join(chosen_total(odd, near, own), chosen_total(odd, own, near))
    body, head = both.shape
    pair_ref[:body, :] = both.astype(bf16)
    pair_ref[body:, :] = row_pack(thirds(factor), head).astype(bf16)


def spread_kernel(
    beta_ref, decay_ref, near_ref, pair_ref, other_ref, maps_ref, adds_ref, factors_ref,
    query_ref, key_ref, value_ref, send_ref, wide_ref, turned_ref,
):
    head = pair_ref.shape[1]
    half = head // 2
    far = lax.axis_index("zh")
    near = lax.axis_index("zl") * 4 + lax.axis_index("x")
    pair = near // 2
    side = near % 2

    def scalar(ref):
        total = jnp.zeros((1, 1), f32)
        for at in range(4):
            entry = ref[at // 2 : at // 2 + 1, at % 2 : at % 2 + 1]
            total = jnp.where(pair == at, entry, total)
        return total

    def chosen(ref):
        total = jnp.zeros((1, head), f32)
        for at in range(4):
            row = ref[at // 2, at % 2 : at % 2 + 1, :].astype(f32)
            total = jnp.where(pair == at, row, total)
        return total

    def after(step, state):
        both, factor = step
        return factor * state - dot(state, both[:head]) + both[head:]

    low = far < 2
    mine, theirs = split_total(pair_ref), split_total(other_ref)
    begin = jnp.where(low, 0.0, theirs[0][head:])
    begin = jnp.where(far % 2 == 1, after(split_total(near_ref), begin), begin)
    first, last = chosen_total(low, mine, theirs), chosen_total(low, theirs, mine)
    state = after(last, first[0][head:])
    final = state.astype(bf16).astype(f32)
    wide_ref[...] = jnp.zeros((head, head), f32)
    wide_ref[pl.ds(pl.multiple_of(side * half, half), half), :] = final
    padded = wide_ref[...]
    turned_ref[...] = padded.T
    mine = turned_ref[pl.ds(pl.multiple_of(far * 32, 32), 32), :]
    query = chosen(query_ref)
    key = chosen(key_ref)
    query = query * rms_scale(query, unit_floor, False)
    key = key * rms_scale(key, unit_floor, False)
    hits = dot(row_pack(thirds(query) + thirds(key), head), padded, ROWS)
    recall = hits[0:1] + hits[1:2] + hits[2:3]
    retrieve = hits[3:4] + hits[4:5] + hits[5:6]
    decay = scalar(decay_ref)
    intersect = jnp.sum(key * query, axis=-1, keepdims=True)
    fresh = chosen(value_ref) - decay * retrieve
    read = decay * recall + (scalar(beta_ref) * intersect) * fresh
    read = jnp.where(iota((1, head), 1) // half == side, read, 0.0)
    zero = jnp.zeros((1, head), f32)
    extra = row_pack((zero, zero, zero, zero) + thirds(read), head)
    pick_row = iota((PACK, 32), 0)
    pick_col = iota((PACK, 32), 1)
    for member in range(8):
        if member:
            at = member - 1
            entry = factors_ref[at, 0:1, :] * begin - dot(begin, maps_ref[at]) + adds_ref[at]
        else:
            entry = begin
        send_ref[member, :half, :] = entry.astype(bf16)
        pick = ((pick_row < 4) & (pick_col == 4 * member + pick_row)).astype(bf16)
        send_ref[member, half:, :] = (dot(pick, mine) + extra).astype(bf16)


def finish_kernel(in_ref, out_ref, reach_ref, silu_ref, gain_ref, mixed_ref, cache_ref, read_ref):
    head = in_ref.shape[-1]
    half = head // 2
    for pair in range(4):
        seq, h = divmod(pair, 2)
        incoming = jnp.concatenate([in_ref[2 * pair, :half, :], in_ref[2 * pair + 1, :half, :]], 0)
        whole = out_ref[pair] + dot(reach_ref[pair], incoming, ROWS)
        mixed = whole * rms_scale(whole, norm_floor, True) * silu_ref[pair]
        mixed_ref[seq, :, h * head : (h + 1) * head] = mixed.astype(bf16)
        extra = in_ref[2 * pair, half:, :].astype(f32) + in_ref[2 * pair + 1, half:, :].astype(f32)
        cache_ref[seq, h] = extra[:4].astype(bf16)
        read = extra[4:5] + extra[5:6] + extra[6:7]
        read = read * rms_scale(read, norm_floor, True) * gain_ref[...]
        read_ref[seq : seq + 1, h * head : (h + 1) * head] = read


def vmem():
    return pl.BlockSpec(memory_space=pltpu.VMEM)


def smem():
    return pl.BlockSpec(memory_space=pltpu.SMEM)


def kernel(body, outputs, kinds, args, scratch=(), limit=16):
    given = {"s": smem, "v": vmem, "p": vmem, "h": lambda: pl.BlockSpec(memory_space=pl.ANY)}
    placed = [
        arg
        if kind == "s"
        else pltpu.with_memory_space_constraint(arg, pltpu.VMEM if kind == "p" else pltpu.HBM)
        for kind, arg in zip(kinds, args, strict=True)
    ]
    plain = lambda out: pltpu.HBM(out.shape, out.dtype)
    return pl.pallas_call(
        body,
        out_shape=tuple(out if kind == "p" else plain(out) for kind, out in outputs),
        in_specs=[given[kind]() for kind in kinds],
        out_specs=tuple(given[kind]() for kind, _ in outputs),
        scratch_shapes=list(scratch),
        compiler_params=pltpu.CompilerParams(vmem_limit_bytes=limit * 1024 * 1024),
    )(*placed)


def shift(value, axis, by):
    length = lax.axis_size(axis)
    return lax.ppermute(value, axis, [(at, (at + by) % length) for at in range(length)])


def shards(
    tokens, query_weight, key_weight, value_weight, gate_weight, beta_weight, decay_weight,
    beta_bias, rate_log, out_gain, new_query, new_key, new_value, new_beta, new_decay,
):
    _, span, depth = tokens.shape
    head = out_gain.shape[0]
    half = head // 2
    wide = 256
    width = query_weight.shape[1]
    rows = head + half + PACK
    on, dma = pltpu.VMEM, pltpu.SemaphoreType.DMA
    depth = tokens.shape[2]
    swap = lambda value: shift(value, "c", 1)
    tokens_c = swap(tokens)
    half_span = ("p", on((span, depth), bf16))
    first, second = kernel(split_kernel, [half_span, half_span], "h", (tokens,), (dma((2,)),))
    up0 = shift(first, "y", 1)
    down1 = shift(second, "y", -1)
    sums = [("p", on((2 * span, 2 * width), f32)), ("p", on((2 * span, head), f32))]
    early = kernel(
        early_kernel,
        sums + [("p", on((6 * depth, 2 * width), bf16)), ("p", on((PACK, 8 * depth), bf16))],
        "ppphhhh",
        (first, second, tokens_c, beta_weight.T, decay_weight.T, key_weight, value_weight),
        (
            on((2 * depth, 2 * width), bf16),
            on((2, 2, 8 * depth), bf16),
            dma((2,)),
        ),
    )
    early = list(early)
    first, second, *early[:2] = lax.optimization_barrier((first, second, *early[:2]))
    up1 = shift(second, "y", 1)
    down0 = shift(first, "y", -1)
    rest = early[2:]
    far0 = shift(up0, "y", 1)
    far1 = shift(down1, "y", -1)
    near = (up0, up1, down0, down1)
    swapped = []
    for value in near:
        swapped.append(swap(value))
    middle = kernel(
        functools.partial(middle_kernel, 2), sums, "p" * 12, (*near, *swapped, *early[:2], *rest)
    )
    far0, far1, *middle = lax.optimization_barrier((far0, far1, *middle))
    last = [far0, far1, swap(far0), swap(far1)]
    middle = kernel(
        functools.partial(middle_kernel, 6), sums, "p" * 6, (far0, far1, *middle, *rest)
    )
    far_c0, far_c1, *middle = lax.optimization_barrier((*last[2:], *middle))
    last[2:] = [far_c0, far_c1]
    local_shapes = [
        on((8, rows, head), bf16),
        on((2 * span, width), bf16),
        on((4, span, head), bf16),
        on((4, span, head), bf16),
        on((2, wide, head), f32),
        on((2, head, wide), f32),
    ]
    send, *shared = kernel(
        local_kernel,
        [("h", out) for out in local_shapes],
        "p" * 8,
        (beta_bias[None], rate_log[None], *last[2:], *middle, *rest),
        (*local_shapes, dma((6,))),
    )
    arrived = lax.all_to_all(send, NEAR, 0, 0, tiled=True)
    gain = out_gain[None]
    finals = [on((4, span, head), f32), on((4, span, head), bf16), on((4, span, head), f32)]
    local_out, reach, silu = kernel(
        window_kernel,
        [("h", out) for out in finals],
        "h" * 16 + "v" + "h" * 5,
        (tokens, tokens_c, *near, *swapped, *last, query_weight, gate_weight, gain, *shared),
        (
            on((8, 2, span, depth), bf16),
            on((8, depth, width), bf16),
            on((8, depth, width), bf16),
            dma((8,)),
            dma((8,)),
            *local_shapes[1:],
            *finals,
        ),
        24,
    )
    arrived, local_out = lax.optimization_barrier((arrived, local_out))
    (total,) = kernel(total_kernel, [("p", on((rows, head), bf16))], "p", (arrived,))
    exchange = lambda value, by: lax.ppermute(value, "zh", [(at, at ^ by) for at in range(4)])
    beside = exchange(total, 1)
    maps, adds, factors, *finals_in = kernel(
        prefix_kernel,
        [
            ("p", on((7, head, head), bf16)),
            ("p", on((7, half, head), f32)),
            ("p", on((7, 8, head), f32)),
            *(("p", out) for out in finals),
        ],
        "pphhh",
        (total, arrived, local_out, reach, silu),
        (dma((3,)),),
    )
    beside, maps = lax.optimization_barrier((beside, maps))
    (pair,) = kernel(pair_kernel, [("p", on((rows, head), bf16))], "pp", (total, beside))
    other = exchange(pair, 3)
    (back,) = kernel(
        spread_kernel,
        [("p", on((8, half + PACK, head), bf16))],
        "p" * 11,
        (
            new_beta, new_decay, beside, pair, other, maps, adds, factors,
            new_query, new_key, new_value,
        ),
        (on((head, head), f32), on((head, head), f32)),
    )
    returned = lax.all_to_all(back, NEAR, 0, 0, tiled=True)
    return kernel(
        finish_kernel,
        [
            ("v", on((2, span, width), bf16)),
            ("v", on((2, 2, 4, head), bf16)),
            ("v", on((2, width), f32)),
        ],
        "ppppp",
        (returned, *finals_in, gain),
    )


def solution(mesh):
    torus = Mesh(mesh.devices.reshape(4, 2, 4, 4, 2), AXES + ("y", "c"))
    sp, tp = AXES, ("y", "c")
    weight = P(None, tp)
    in_specs = (
        P(None, sp, tp),
        weight, weight, weight, weight, weight, weight,
        P(tp), P(tp), P(),
        P(None, tp, None), P(None, tp, None), P(None, tp, None),
        P(None, tp), P(None, tp),
    )
    out_specs = (P(None, sp, tp), P(None, tp, sp, None), P(None, tp))

    return jax.shard_map(
        shards, mesh=torus, in_specs=in_specs, out_specs=out_specs, check_vma=False
    )
```

```python
import functools

import jax
import jax.numpy as jnp
from jax import lax
from jax.experimental import pallas as pl
from jax.experimental.pallas import tpu as pltpu
from jax.sharding import Mesh
from jax.sharding import PartitionSpec as P


NEAR = ("zl", "x")
AXES = ("zh", "zl", "x")
PACK = 8
LANES = 128
unit_floor = 1.0
norm_floor = 0.001
bf16 = jnp.bfloat16
f32 = jnp.float32


def dot(left, right, dims=((1,), (0,))):
    return lax.dot_general(
        left.astype(bf16), right.astype(bf16), (dims, ((), ())), preferred_element_type=f32
    )


ROWS = ((1,), (1,))
COLS = ((0,), (0,))


def thirds(value):
    high = value.astype(bf16).astype(f32)
    rest = value - high
    mid = rest.astype(bf16).astype(f32)
    return high, mid, rest - mid


def iota(shape, dim):
    return lax.broadcasted_iota(jnp.int32, shape, dim)


def row_pack(values, width):
    rows = iota((PACK, width), 0)
    packed = jnp.zeros((PACK, width), f32)
    for at, value in enumerate(values):
        packed = jnp.where(rows == at, value, packed)
    return packed


def rms_scale(values, floor, mean):
    total = jnp.sum(values * values, axis=-1, keepdims=True)
    return lax.rsqrt((total / values.shape[-1] if mean else total) + floor)


def shard_index(ahead, swapped):
    core = lax.axis_index("c")
    core = 1 - core if swapped else core
    return lax.rem(lax.axis_index("y") + ahead, 4) * 2 + core


def first_row(slot, depth):
    return pl.multiple_of(shard_index(*slot) * depth, depth)


def joined(first, second):
    return jnp.concatenate([first[...], second[...]], axis=0)


def scalar_part(rows, stacked, slot):
    depth = rows.shape[-1]
    weight = stacked[:, pl.ds(first_row(slot, depth), depth)]
    weight = jnp.concatenate([weight, jnp.zeros((LANES - 16, depth), bf16)], axis=0)
    return dot(rows, weight, ROWS)


SLOTS = (
    (0, False), (0, True), (3, False), (1, False), (3, True), (1, True), (2, False), (2, True),
)


def split_kernel(source, first, second, sems):
    copies = [
        pltpu.make_async_copy(source.at[at], to, sems.at[at]) for at, to in enumerate((first, second))
    ]
    for copy in copies:
        copy.start()
    for copy in copies:
        copy.wait()


def early_kernel(
    own_first, own_second, own_c, beta_w, decay_w, key_w, value_w, sum_ref, gate_ref, rest_ref, stacked_ref,
    weight_buffer, scalar_buffer, sems,
):
    depth = own_c.shape[-1]
    width = key_w.shape[-1]
    first = []
    for at, weight in enumerate((beta_w, decay_w)):
        first.append(pltpu.make_async_copy(weight, scalar_buffer.at[at], sems.at[0]))
    later = []
    for at, slot in enumerate(SLOTS):
        start = first_row(slot, depth)
        for side, weight in enumerate((key_w, value_w)):
            lanes = pl.ds(side * width, width)
            source = weight.at[pl.ds(start, depth), :]
            if at < 2:
                to = weight_buffer.at[pl.ds(at * depth, depth), lanes]
                first.append(pltpu.make_async_copy(source, to, sems.at[0]))
            else:
                to = rest_ref.at[pl.ds((at - 2) * depth, depth), lanes]
                later.append(pltpu.make_async_copy(source, to, sems.at[1]))
    for copy in first + later:
        copy.start()
    for copy in first:
        copy.wait()
    rows = [scalar_buffer[at, h : h + 1, :].astype(f32) for at in range(2) for h in range(2)]
    stacked_ref[...] = jnp.concatenate([row_pack(rows, stacked_ref.shape[-1]), jnp.zeros((8, stacked_ref.shape[-1]), f32)], axis=0).astype(bf16)
    total = gates = 0.0
    for at in range(2):
        rows = own_c[...].reshape(-1, depth) if at else joined(own_first, own_second)
        total = total + dot(rows, weight_buffer[at * depth : (at + 1) * depth, :])
        gates = gates + scalar_part(rows, stacked_ref, SLOTS[at])
    sum_ref[...] = total
    gate_ref[...] = gates
    for copy in later:
        copy.wait()


def add_pieces(pieces, from_slot, rest, stacked, total, gates):
    for at in range(len(pieces) // 2):
        rows = joined(*pieces[2 * at : 2 * at + 2])
        depth = rows.shape[-1]
        slot = from_slot + at
        total = total + dot(rows, rest[(slot - 2) * depth : (slot - 1) * depth, :])
        gates = gates + scalar_part(rows, stacked, SLOTS[slot])
    return total, gates


def middle_kernel(first_slot, *refs):
    pieces, (sum_in, gate_in, rest, stacked, sum_ref, gate_ref) = refs[:-6], refs[-6:]
    total, gates = add_pieces(pieces, first_slot, rest, stacked, sum_in[...], gate_in[...])
    sum_ref[...] = total
    gate_ref[...] = gates


def lane_pair(ref, first):
    lanes = iota((1, LANES), 1)
    pair = ref[...]
    return jnp.where(
        lanes == first, pair[:, 0:1], jnp.where(lanes == first + 1, pair[:, 1:2], 0.0)
    )


def local_kernel(bias_ref, rate_ref, *refs):
    pieces, (sum_in, gate_in, rest, stacked) = refs[:2], refs[2:6]
    outputs, buffers, sems = refs[6:12], refs[12:18], refs[18]
    send_ref, key_ref, fresh_ref, carry_ref, cols_ref, rows_ref = buffers
    copies = []

    def give(at, part=None):
        source, to = buffers[at], outputs[at]
        if part is not None:
            source, to = source.at[part], to.at[part]
        copies.append(pltpu.make_async_copy(source, to, sems.at[at]))
        copies[-1].start()

    span = pieces[0].shape[0]
    head = send_ref.shape[-1]
    total, gates = add_pieces(pieces, 7, rest, stacked, sum_in[...], gate_in[...])
    width = total.shape[-1] // 2
    key_rows = total[:, :width].astype(bf16)
    value_rows = total[:, width:].astype(bf16)
    key_ref[...] = key_rows
    give(1)
    strength = jax.nn.sigmoid(gates + lane_pair(bias_ref, 0))
    decays = -jnp.exp(lane_pair(rate_ref, 2)) * jax.nn.softplus(gates)
    wide = cols_ref.shape[1]
    lanes = iota((wide, head), 1)
    causal_wide = (iota((wide, wide), 0) >= iota((wide, wide), 1)).astype(bf16)
    for seq in range(2):
        take = slice(seq * span, (seq + 1) * span)
        padded = jnp.concatenate([decays[take], jnp.zeros((wide - span, head), f32)], axis=0)
        cumulative = sum(dot(causal_wide, part) for part in thirds(padded))
        table = jnp.where((lanes == 2) | (lanes == 3), cumulative, 0.0)
        for h in range(2):
            keys = key_rows[take, h * head : (h + 1) * head].astype(f32)
            unit = jnp.concatenate(
                [rms_scale(keys, unit_floor, False), jnp.zeros((wide - span, 1), f32)], axis=0
            )
            beta = jnp.concatenate(
                [strength[take, h : h + 1], jnp.zeros((wide - span, 1), f32)], axis=0
            )
            table = jnp.where(lanes == h, beta, table)
            table = jnp.where(lanes == 4 + h, unit, table)
        cols_ref[seq] = table
        rows_ref[seq] = table.T
    give(4)
    give(5)
    half = head // 2
    t = iota((head, head), 0)
    s = iota((head, head), 1)
    apart = t ^ s
    upper, lower = slice(0, head), slice(head, span)
    blocks = []
    for pair in range(4):
        seq, h = divmod(pair, 2)
        keys = key_rows[seq * span : (seq + 1) * span, h * head : (h + 1) * head]

        def alike(of, with_, mask):
            col = lambda at: cols_ref[seq, of, at + h : at + h + 1]
            row = lambda at: rows_ref[seq, at + h : at + h + 1, with_]
            spread = col(2) - row(2)
            if mask is not None:
                spread = jnp.where(mask, spread, 0.0)
            product = dot(keys[of], keys[with_], ROWS)
            product = product * (col(0) * col(4)) * row(4) * jnp.exp(spread)
            return product if mask is None else jnp.where(mask, product, 0.0)

        def started(block):
            size = block.shape[0]
            near, same = apart[:size, :size] < 2, (t == s)[:size, :size]
            return jnp.where(same, 1.0, jnp.where(near, -block, 0.0)).astype(bf16)

        first = alike(upper, upper, t > s)
        second = alike(lower, lower, (t > s)[:half, :half])
        across = alike(lower, upper, None)
        blocks.append(
            [first.astype(bf16), second.astype(bf16), across.astype(bf16)]
            + [started(first), started(second)]
        )
    size = 2
    while size < half:
        mask = jnp.where((apart >= size) & (apart < 2 * size), 1.0, 0.0).astype(bf16)
        steps = []
        for first, second, _, x_first, x_second in blocks:
            step = dot(first * mask, x_first).astype(bf16)
            steps.append((step, dot(second * mask[:half, :half], x_second).astype(bf16)))
        for block, (step_first, step_second) in zip(blocks, steps):
            block[3] = block[3] - dot(block[3], step_first).astype(bf16)
            block[4] = block[4] - dot(block[4], step_second).astype(bf16)
        size *= 2
    left = jnp.where(iota((half, head), 1) < half, 1.0, 0.0).astype(bf16)
    blank = jnp.zeros((half, head), bf16)
    steps = [dot(block[0][half:] * left, block[3]).astype(bf16) for block in blocks]
    for block, step in zip(blocks, steps):
        change = dot(block[3][half:], jnp.concatenate([blank, step], axis=0)).astype(bf16)
        block[3] = jnp.concatenate([block[3][:half], block[3][half:] - change], axis=0)
    steps = [dot(block[2], block[3]).astype(bf16) for block in blocks]
    for pair in range(4):
        seq, h = divmod(pair, 2)
        take = slice(seq * span, (seq + 1) * span)
        keys = key_rows[take, h * head : (h + 1) * head]
        values = value_rows[take, h * head : (h + 1) * head]
        col = lambda at: cols_ref[seq, :span, at + h : at + h + 1]
        row = lambda at: rows_ref[seq, at + h : at + h + 1, :span]
        off_first = jnp.where(t == s, 0.0, blocks[pair][3].astype(f32))
        off_second = jnp.where((t == s)[:half, :half], 0.0, blocks[pair][4].astype(f32))
        off_across = -dot(blocks[pair][4], steps[pair])

        def applied(weight, right):
            top = dot(off_first * weight[:, upper], right[upper])
            low = dot(off_across * weight[:, upper], right[upper])
            low = low + dot(off_second * weight[:, lower], right[lower])
            return jnp.concatenate([top, low], axis=0)

        fresh = col(0) * values.astype(f32) + applied(row(0), values)
        carry = (col(0) * col(4) * jnp.exp(col(2))) * keys.astype(f32) + applied(
            row(0) * row(4) * jnp.exp(row(2)), keys
        )
        last = cols_ref[seq, span - 1 : span, 2 + h : 3 + h]
        late = col(4) * jnp.exp(last - col(2))
        reach = dot(carry * late, keys, COLS)
        gain = dot(fresh * late, keys, COLS)
        fresh_ref[pair] = fresh.astype(bf16)
        carry_ref[pair] = carry.astype(bf16)
        give(2, pair)
        give(3, pair)
        factor = row_pack(thirds(jnp.broadcast_to(jnp.exp(last), (1, head))), head)
        for side in range(2):
            to = 2 * pair + side
            send_ref[to, :head, :] = reach.astype(bf16)
            send_ref[to, head : head + half, :] = gain[side * half : (side + 1) * half].astype(bf16)
            send_ref[to, head + half :, :] = factor.astype(bf16)
        give(0, pl.ds(2 * pair, 2))
    for copy in copies:
        copy.wait()


def window_kernel(*refs):
    pieces, refs = refs[:14], refs[14:]
    query_w, gate_w, gain_ref, shared, refs = refs[0], refs[1], refs[2], refs[3:8], refs[8:]
    outputs, refs = refs[:3], refs[3:]
    token_buffer, query_buffer, gate_buffer, sems, more_sems = refs[:5]
    shared_buffers, output_buffers = refs[5:10], refs[10:]
    key_ref, fresh_ref, carry_ref, cols_ref, rows_ref = shared_buffers
    out_ref, reach_ref, silu_ref = output_buffers
    span, depth = token_buffer.shape[2:]
    head = fresh_ref.shape[-1]
    weights = ((query_w, query_buffer), (gate_w, gate_buffer))
    copies = []
    for at, slot in enumerate(SLOTS):
        if at < 2:
            parts = [(pieces[at], token_buffer.at[at])]
        else:
            parts = [(pieces[2 * at - 2 + seq], token_buffer.at[at, seq]) for seq in range(2)]
        for weight, buffer in weights:
            parts.append((weight.at[pl.ds(first_row(slot, depth), depth), :], buffer.at[at]))
        copies.append([pltpu.make_async_copy(a, b, sems.at[at]) for a, b in parts])
        for copy in copies[at]:
            copy.start()
    given = [
        pltpu.make_async_copy(a, b, more_sems.at[at])
        for at, (a, b) in enumerate(zip(shared, shared_buffers))
    ]
    for copy in given:
        copy.start()
    query_total = gate_total = 0.0
    for at in range(8):
        for copy in copies[at]:
            copy.wait()
        rows = token_buffer[at].reshape(-1, depth)
        query_total = query_total + dot(rows, query_buffer[at])
        gate_total = gate_total + dot(rows, gate_buffer[at])
    for copy in given:
        copy.wait()
    query_rows = query_total.astype(bf16)
    gate_rows = gate_total.astype(bf16).astype(f32)
    t = iota((span, span), 0)
    s = iota((span, span), 1)
    taken = []
    for pair in range(4):
        seq, h = divmod(pair, 2)
        take = slice(seq * span, (seq + 1) * span)
        part = slice(h * head, (h + 1) * head)
        col = lambda at: cols_ref[seq, :span, at + h : at + h + 1]
        row = lambda at: rows_ref[seq, at + h : at + h + 1, :span]
        queries = query_rows[take, part]
        unit = rms_scale(queries.astype(f32), unit_floor, False)
        spread = jnp.where(t >= s, col(2) - row(2), 0.0)
        scores = dot(queries, key_ref[take, part], ROWS) * unit * row(4) * jnp.exp(spread)
        scores = jnp.where(t >= s, scores, 0.0).astype(bf16)
        out_ref[pair] = dot(scores, fresh_ref[pair])
        reach = (unit * jnp.exp(col(2))) * queries.astype(f32) - dot(scores, carry_ref[pair])
        reach_ref[pair] = reach.astype(bf16)
        gate = gate_rows[take, part]
        silu_ref[pair] = gain_ref[...] * gate * jax.nn.sigmoid(gate)
        for at, (a, b) in enumerate(zip(output_buffers, outputs)):
            taken.append(pltpu.make_async_copy(a.at[pair], b.at[pair], more_sems.at[5 + at]))
            taken[-1].start()
    for copy in taken:
        copy.wait()


def unpack_factor(block):
    block = block.astype(f32)
    return block[0:1] + block[1:2] + block[2:3]


def load_member(in_ref, at):
    body = in_ref.shape[1] - PACK
    return in_ref[at, :body, :].astype(f32), unpack_factor(in_ref[at, body:, :])


def join(first, second):
    both, factor = first
    later, later_factor = second
    head = later.shape[-1]
    tail = jnp.concatenate([factor * later[:head], later[head:]], axis=0)
    return later_factor * both - dot(both, later[:head]) + tail, factor * later_factor


def total_kernel(in_ref, total_ref):
    parts = [load_member(in_ref, at) for at in range(in_ref.shape[0])]
    while len(parts) > 1:
        parts = [join(parts[at], parts[at + 1]) for at in range(0, len(parts), 2)]
    both, factor = parts[0]
    body, head = both.shape
    total_ref[:body, :] = both.astype(bf16)
    total_ref[body:, :] = row_pack(thirds(factor), head).astype(bf16)


def prefix_kernel(_, in_ref, out_in, reach_in, silu_in, *refs):
    maps_ref, adds_ref, factors_ref, out_ref, reach_ref, silu_ref, sems = refs
    moved = ((out_in, out_ref), (reach_in, reach_ref), (silu_in, silu_ref))
    copies = [pltpu.make_async_copy(a, b, sems.at[at]) for at, (a, b) in enumerate(moved)]
    for copy in copies:
        copy.start()
    count, _, head = in_ref.shape
    member = [load_member(in_ref, at) for at in range(count - 1)]
    c23, c45 = (join(member[at], member[at + 1]) for at in (2, 4))
    upto = [None, member[0], join(member[0], member[1])]
    c456 = join(c45, member[6])
    upto.append(join(upto[2], member[2]))
    upto.append(join(upto[2], c23))
    upto.append(join(upto[4], member[4]))
    upto.append(join(upto[4], c45))
    upto.append(join(upto[4], c456))
    for at in range(1, count):
        both, factor = upto[at]
        maps_ref[at - 1] = both[:head].astype(bf16)
        adds_ref[at - 1] = both[head:]
        factors_ref[at - 1] = jnp.broadcast_to(factor, (8, head))
    for copy in copies:
        copy.wait()


def split_total(ref):
    body = ref.shape[0] - PACK
    return ref[:body, :].astype(f32), unpack_factor(ref[body:, :])


def chosen_total(flag, first, second):
    return tuple(jnp.where(flag, a, b) for a, b in zip(first, second))


def pair_kernel(own_ref, near_ref, pair_ref):
    odd = lax.axis_index("zh") % 2 == 1
    own, near = split_total(own_ref), split_total(near_ref)
    both, factor = join(chosen_total(odd, near, own), chosen_total(odd, own, near))
    body, head = both.shape
    pair_ref[:body, :] = both.astype(bf16)
    pair_ref[body:, :] = row_pack(thirds(factor), head).astype(bf16)


def spread_kernel(
    beta_ref, decay_ref, near_ref, pair_ref, other_ref, maps_ref, adds_ref, factors_ref,
    query_ref, key_ref, value_ref, send_ref, wide_ref, turned_ref,
):
    head = pair_ref.shape[1]
    half = head // 2
    far = lax.axis_index("zh")
    near = lax.axis_index("zl") * 4 + lax.axis_index("x")
    pair = near // 2
    side = near % 2

    def scalar(ref):
        total = jnp.zeros((1, 1), f32)
        for at in range(4):
            entry = ref[at // 2 : at // 2 + 1, at % 2 : at % 2 + 1]
            total = jnp.where(pair == at, entry, total)
        return total

    def chosen(ref):
        total = jnp.zeros((1, head), f32)
        for at in range(4):
            row = ref[at // 2, at % 2 : at % 2 + 1, :].astype(f32)
            total = jnp.where(pair == at, row, total)
        return total

    def after(step, state):
        both, factor = step
        return factor * state - dot(state, both[:head]) + both[head:]

    low = far < 2
    mine, theirs = split_total(pair_ref), split_total(other_ref)
    begin = jnp.where(low, 0.0, theirs[0][head:])
    begin = jnp.where(far % 2 == 1, after(split_total(near_ref), begin), begin)
    first, last = chosen_total(low, mine, theirs), chosen_total(low, theirs, mine)
    state = after(last, first[0][head:])
    final = state.astype(bf16).astype(f32)
    wide_ref[...] = jnp.zeros((head, head), f32)
    wide_ref[pl.ds(pl.multiple_of(side * half, half), half), :] = final
    padded = wide_ref[...]
    turned_ref[...] = padded.T
    mine = turned_ref[pl.ds(pl.multiple_of(far * 32, 32), 32), :]
    query = chosen(query_ref)
    key = chosen(key_ref)
    query = query * rms_scale(query, unit_floor, False)
    key = key * rms_scale(key, unit_floor, False)
    hits = dot(row_pack(thirds(query) + thirds(key), head), padded, ROWS)
    recall = hits[0:1] + hits[1:2] + hits[2:3]
    retrieve = hits[3:4] + hits[4:5] + hits[5:6]
    decay = scalar(decay_ref)
    intersect = jnp.sum(key * query, axis=-1, keepdims=True)
    fresh = chosen(value_ref) - decay * retrieve
    read = decay * recall + (scalar(beta_ref) * intersect) * fresh
    read = jnp.where(iota((1, head), 1) // half == side, read, 0.0)
    zero = jnp.zeros((1, head), f32)
    extra = row_pack((zero, zero, zero, zero) + thirds(read), head)
    pick_row = iota((PACK, 32), 0)
    pick_col = iota((PACK, 32), 1)
    for member in range(8):
        if member:
            at = member - 1
            entry = factors_ref[at, 0:1, :] * begin - dot(begin, maps_ref[at]) + adds_ref[at]
        else:
            entry = begin
        send_ref[member, :half, :] = entry.astype(bf16)
        pick = ((pick_row < 4) & (pick_col == 4 * member + pick_row)).astype(bf16)
        send_ref[member, half:, :] = (dot(pick, mine) + extra).astype(bf16)


def finish_kernel(in_ref, out_ref, reach_ref, silu_ref, gain_ref, mixed_ref, cache_ref, read_ref):
    head = in_ref.shape[-1]
    half = head // 2
    for pair in range(4):
        seq, h = divmod(pair, 2)
        incoming = jnp.concatenate([in_ref[2 * pair, :half, :], in_ref[2 * pair + 1, :half, :]], 0)
        whole = out_ref[pair] + dot(reach_ref[pair], incoming, ROWS)
        mixed = whole * rms_scale(whole, norm_floor, True) * silu_ref[pair]
        mixed_ref[seq, :, h * head : (h + 1) * head] = mixed.astype(bf16)
        extra = in_ref[2 * pair, half:, :].astype(f32) + in_ref[2 * pair + 1, half:, :].astype(f32)
        cache_ref[seq, h] = extra[:4].astype(bf16)
        read = extra[4:5] + extra[5:6] + extra[6:7]
        read = read * rms_scale(read, norm_floor, True) * gain_ref[...]
        read_ref[seq : seq + 1, h * head : (h + 1) * head] = read


def vmem():
    return pl.BlockSpec(memory_space=pltpu.VMEM)


def smem():
    return pl.BlockSpec(memory_space=pltpu.SMEM)


def kernel(body, outputs, kinds, args, scratch=(), limit=16):
    given = {"s": smem, "v": vmem, "p": vmem, "h": lambda: pl.BlockSpec(memory_space=pl.ANY)}
    placed = [
        arg
        if kind == "s"
        else pltpu.with_memory_space_constraint(arg, pltpu.VMEM if kind == "p" else pltpu.HBM)
        for kind, arg in zip(kinds, args, strict=True)
    ]
    plain = lambda out: pltpu.HBM(out.shape, out.dtype)
    return pl.pallas_call(
        body,
        out_shape=tuple(out if kind == "p" else plain(out) for kind, out in outputs),
        in_specs=[given[kind]() for kind in kinds],
        out_specs=tuple(given[kind]() for kind, _ in outputs),
        scratch_shapes=list(scratch),
        compiler_params=pltpu.CompilerParams(vmem_limit_bytes=limit * 1024 * 1024),
    )(*placed)


def shift(value, axis, by):
    length = lax.axis_size(axis)
    return lax.ppermute(value, axis, [(at, (at + by) % length) for at in range(length)])


def shards(
    tokens, query_weight, key_weight, value_weight, gate_weight, beta_weight, decay_weight,
    beta_bias, rate_log, out_gain, new_query, new_key, new_value, new_beta, new_decay,
):
    _, span, depth = tokens.shape
    head = out_gain.shape[0]
    half = head // 2
    wide = 256
    width = query_weight.shape[1]
    rows = head + half + PACK
    on, dma = pltpu.VMEM, pltpu.SemaphoreType.DMA
    depth = tokens.shape[2]
    swap = lambda value: shift(value, "c", 1)
    tokens_c = swap(tokens)
    half_span = ("p", on((span, depth), bf16))
    first, second = kernel(split_kernel, [half_span, half_span], "h", (tokens,), (dma((2,)),))
    up0 = shift(first, "y", 1)
    down1 = shift(second, "y", -1)
    sums = [("p", on((2 * span, 2 * width), f32)), ("p", on((2 * span, head), f32))]
    early = kernel(
        early_kernel,
        sums + [("p", on((6 * depth, 2 * width), bf16)), ("p", on((16, 8 * depth), bf16))],
        "ppphhhh",
        (first, second, tokens_c, beta_weight.T, decay_weight.T, key_weight, value_weight),
        (
            on((2 * depth, 2 * width), bf16),
            on((2, 2, 8 * depth), bf16),
            dma((2,)),
        ),
    )
    early = list(early)
    first, second, *early[:2] = lax.optimization_barrier((first, second, *early[:2]))
    up1 = shift(second, "y", 1)
    down0 = shift(first, "y", -1)
    rest = early[2:]
    far0 = shift(up0, "y", 1)
    far1 = shift(down1, "y", -1)
    near = (up0, up1, down0, down1)
    swapped = []
    for value in near:
        swapped.append(swap(value))
    middle = kernel(
        functools.partial(middle_kernel, 2), sums, "p" * 12, (*near, *swapped, *early[:2], *rest)
    )
    far0, far1, *middle = lax.optimization_barrier((far0, far1, *middle))
    last = [far0, far1, swap(far0), swap(far1)]
    middle = kernel(
        functools.partial(middle_kernel, 6), sums, "p" * 6, (far0, far1, *middle, *rest)
    )
    far_c0, far_c1, *middle = lax.optimization_barrier((*last[2:], *middle))
    last[2:] = [far_c0, far_c1]
    local_shapes = [
        on((8, rows, head), bf16),
        on((2 * span, width), bf16),
        on((4, span, head), bf16),
        on((4, span, head), bf16),
        on((2, wide, head), f32),
        on((2, head, wide), f32),
    ]
    send, *shared = kernel(
        local_kernel,
        [("h", out) for out in local_shapes],
        "p" * 8,
        (beta_bias[None], rate_log[None], *last[2:], *middle, *rest),
        (*local_shapes, dma((6,))),
    )
    arrived = lax.all_to_all(send, NEAR, 0, 0, tiled=True)
    gain = out_gain[None]
    finals = [on((4, span, head), f32), on((4, span, head), bf16), on((4, span, head), f32)]
    local_out, reach, silu = kernel(
        window_kernel,
        [("h", out) for out in finals],
        "h" * 16 + "v" + "h" * 5,
        (tokens, tokens_c, *near, *swapped, *last, query_weight, gate_weight, gain, *shared),
        (
            on((8, 2, span, depth), bf16),
            on((8, depth, width), bf16),
            on((8, depth, width), bf16),
            dma((8,)),
            dma((8,)),
            *local_shapes[1:],
            *finals,
        ),
        24,
    )
    arrived, local_out = lax.optimization_barrier((arrived, local_out))
    (total,) = kernel(total_kernel, [("p", on((rows, head), bf16))], "p", (arrived,))
    exchange = lambda value, by: lax.ppermute(value, "zh", [(at, at ^ by) for at in range(4)])
    beside = exchange(total, 1)
    maps, adds, factors, *finals_in = kernel(
        prefix_kernel,
        [
            ("p", on((7, head, head), bf16)),
            ("p", on((7, half, head), f32)),
            ("p", on((7, 8, head), f32)),
            *(("p", out) for out in finals),
        ],
        "pphhh",
        (total, arrived, local_out, reach, silu),
        (dma((3,)),),
    )
    beside, maps = lax.optimization_barrier((beside, maps))
    (pair,) = kernel(pair_kernel, [("p", on((rows, head), bf16))], "pp", (total, beside))
    other = exchange(pair, 3)
    (back,) = kernel(
        spread_kernel,
        [("p", on((8, half + PACK, head), bf16))],
        "p" * 11,
        (
            new_beta, new_decay, beside, pair, other, maps, adds, factors,
            new_query, new_key, new_value,
        ),
        (on((head, head), f32), on((head, head), f32)),
    )
    returned = lax.all_to_all(back, NEAR, 0, 0, tiled=True)
    return kernel(
        finish_kernel,
        [
            ("v", on((2, span, width), bf16)),
            ("v", on((2, 2, 4, head), bf16)),
            ("v", on((2, width), f32)),
        ],
        "ppppp",
        (returned, *finals_in, gain),
    )


def solution(mesh):
    torus = Mesh(mesh.devices.reshape(4, 2, 4, 4, 2), AXES + ("y", "c"))
    sp, tp = AXES, ("y", "c")
    weight = P(None, tp)
    in_specs = (
        P(None, sp, tp),
        weight, weight, weight, weight, weight, weight,
        P(tp), P(tp), P(),
        P(None, tp, None), P(None, tp, None), P(None, tp, None),
        P(None, tp), P(None, tp),
    )
    out_specs = (P(None, sp, tp), P(None, tp, sp, None), P(None, tp))

    return jax.shard_map(
        shards, mesh=torus, in_specs=in_specs, out_specs=out_specs, check_vma=False
    )
```

```python
import functools

import jax
import jax.numpy as jnp
from jax import lax
from jax.experimental import pallas as pl
from jax.experimental.pallas import tpu as pltpu
from jax.sharding import Mesh
from jax.sharding import PartitionSpec as P


NEAR = ("zl", "x")
AXES = ("zh", "zl", "x")
PACK = 8
LANES = 128
unit_floor = 1.0
norm_floor = 0.001
bf16 = jnp.bfloat16
f32 = jnp.float32


def dot(left, right, dims=((1,), (0,))):
    return lax.dot_general(
        left.astype(bf16), right.astype(bf16), (dims, ((), ())), preferred_element_type=f32
    )


ROWS = ((1,), (1,))
COLS = ((0,), (0,))


def thirds(value):
    high = value.astype(bf16).astype(f32)
    rest = value - high
    mid = rest.astype(bf16).astype(f32)
    return high, mid, rest - mid


def iota(shape, dim):
    return lax.broadcasted_iota(jnp.int32, shape, dim)


def row_pack(values, width):
    rows = iota((PACK, width), 0)
    packed = jnp.zeros((PACK, width), f32)
    for at, value in enumerate(values):
        packed = jnp.where(rows == at, value, packed)
    return packed


def rms_scale(values, floor, mean):
    total = jnp.sum(values * values, axis=-1, keepdims=True)
    return lax.rsqrt((total / values.shape[-1] if mean else total) + floor)


def shard_index(ahead, swapped):
    core = lax.axis_index("c")
    core = 1 - core if swapped else core
    return lax.rem(lax.axis_index("y") + ahead, 4) * 2 + core


def first_row(slot, depth):
    return pl.multiple_of(shard_index(*slot) * depth, depth)


def joined(first, second):
    return jnp.concatenate([first[...], second[...]], axis=0)


def scalar_part(rows, stacked, slot):
    depth = rows.shape[-1]
    weight = stacked[:, pl.ds(first_row(slot, depth), depth)]
    weight = jnp.concatenate([weight, jnp.zeros((LANES - 16, depth), bf16)], axis=0)
    return dot(rows, weight, ROWS)


SLOTS = (
    (0, False), (0, True), (3, False), (1, False), (3, True), (1, True), (2, False), (2, True),
)


def split_kernel(source, first, second, sems):
    copies = [
        pltpu.make_async_copy(source.at[at], to, sems.at[at]) for at, to in enumerate((first, second))
    ]
    for copy in copies:
        copy.start()
    for copy in copies:
        copy.wait()


def early_kernel(
    own_first, own_second, own_c, beta_w, decay_w, key_w, value_w, sum_ref, gate_ref, rest_ref, stacked_ref,
    weight_buffer, scalar_buffer, sems,
):
    depth = own_c.shape[-1]
    width = key_w.shape[-1]
    first = []
    for at, weight in enumerate((beta_w, decay_w)):
        first.append(pltpu.make_async_copy(weight, scalar_buffer.at[at], sems.at[0]))
    later = []
    for at, slot in enumerate(SLOTS):
        start = first_row(slot, depth)
        for side, weight in enumerate((key_w, value_w)):
            lanes = pl.ds(side * width, width)
            source = weight.at[pl.ds(start, depth), :]
            if at < 2:
                to = weight_buffer.at[pl.ds(at * depth, depth), lanes]
                first.append(pltpu.make_async_copy(source, to, sems.at[0]))
            else:
                to = rest_ref.at[pl.ds((at - 2) * depth, depth), lanes]
                later.append(pltpu.make_async_copy(source, to, sems.at[1]))
    for copy in first + later:
        copy.start()
    for copy in first:
        copy.wait()
    rows = [scalar_buffer[at, h : h + 1, :].astype(f32) for at in range(2) for h in range(2)]
    stacked_ref[...] = jnp.concatenate([row_pack(rows, stacked_ref.shape[-1]), jnp.zeros((8, stacked_ref.shape[-1]), f32)], axis=0).astype(bf16)
    total = gates = 0.0
    for at in range(2):
        rows = own_c[...].reshape(-1, depth) if at else joined(own_first, own_second)
        total = total + dot(rows, weight_buffer[at * depth : (at + 1) * depth, :])
        gates = gates + scalar_part(rows, stacked_ref, SLOTS[at])
    sum_ref[...] = total
    gate_ref[...] = gates
    for copy in later:
        copy.wait()


def add_pieces(pieces, from_slot, rest, stacked, total, gates):
    for at in range(len(pieces) // 2):
        rows = joined(*pieces[2 * at : 2 * at + 2])
        depth = rows.shape[-1]
        slot = from_slot + at
        total = total + dot(rows, rest[(slot - 2) * depth : (slot - 1) * depth, :])
        gates = gates + scalar_part(rows, stacked, SLOTS[slot])
    return total, gates


def middle_kernel(first_slot, *refs):
    pieces, (sum_in, gate_in, rest, stacked, sum_ref, gate_ref) = refs[:-6], refs[-6:]
    total, gates = add_pieces(pieces, first_slot, rest, stacked, sum_in[...], gate_in[...])
    sum_ref[...] = total
    gate_ref[...] = gates


def lane_pair(ref, first):
    lanes = iota((1, LANES), 1)
    pair = ref[...]
    return jnp.where(
        lanes == first, pair[:, 0:1], jnp.where(lanes == first + 1, pair[:, 1:2], 0.0)
    )


def local_kernel(bias_ref, rate_ref, *refs):
    pieces, (sum_in, gate_in, rest, stacked) = refs[:2], refs[2:6]
    outputs, buffers, sems = refs[6:12], refs[12:18], refs[18]
    send_ref, key_ref, fresh_ref, carry_ref, cols_ref, rows_ref = buffers
    copies = []

    def give(at, part=None):
        source, to = buffers[at], outputs[at]
        if part is not None:
            source, to = source.at[part], to.at[part]
        copies.append(pltpu.make_async_copy(source, to, sems.at[at]))
        copies[-1].start()

    span = pieces[0].shape[0]
    head = send_ref.shape[-1]
    total, gates = add_pieces(pieces, 7, rest, stacked, sum_in[...], gate_in[...])
    width = total.shape[-1] // 2
    key_rows = total[:, :width].astype(bf16)
    value_rows = total[:, width:].astype(bf16)
    key_ref[...] = key_rows
    give(1)
    strength = jax.nn.sigmoid(gates + lane_pair(bias_ref, 0))
    decays = -jnp.exp(lane_pair(rate_ref, 2)) * jax.nn.softplus(gates)
    wide = cols_ref.shape[1]
    lanes = iota((wide, head), 1)
    causal_wide = (iota((wide, wide), 0) >= iota((wide, wide), 1)).astype(bf16)
    for seq in range(2):
        take = slice(seq * span, (seq + 1) * span)
        cumulative = sum(dot(causal_wide, part) for part in thirds(decays[take]))
        table = jnp.where((lanes == 2) | (lanes == 3), cumulative, 0.0)
        for h in range(2):
            keys = key_rows[take, h * head : (h + 1) * head].astype(f32)
            unit = rms_scale(keys, unit_floor, False)
            beta = strength[take, h : h + 1]
            table = jnp.where(lanes == h, beta, table)
            table = jnp.where(lanes == 4 + h, unit, table)
        cols_ref[seq] = table
        rows_ref[seq] = table.T
    give(4)
    give(5)
    half = head // 2
    t = iota((head, head), 0)
    s = iota((head, head), 1)
    apart = t ^ s
    upper, lower = slice(0, head), slice(head, span)
    blocks = []
    for pair in range(4):
        seq, h = divmod(pair, 2)
        keys = key_rows[seq * span : (seq + 1) * span, h * head : (h + 1) * head]

        def alike(of, with_, mask):
            col = lambda at: cols_ref[seq, of, at + h : at + h + 1]
            row = lambda at: rows_ref[seq, at + h : at + h + 1, with_]
            spread = col(2) - row(2)
            if mask is not None:
                spread = jnp.where(mask, spread, 0.0)
            product = dot(keys[of], keys[with_], ROWS)
            product = product * (col(0) * col(4)) * row(4) * jnp.exp(spread)
            return product if mask is None else jnp.where(mask, product, 0.0)

        def started(block):
            size = block.shape[0]
            near, same = apart[:size, :size] < 2, (t == s)[:size, :size]
            return jnp.where(same, 1.0, jnp.where(near, -block, 0.0)).astype(bf16)

        first = alike(upper, upper, t > s)
        second = alike(lower, lower, (t > s)[:half, :half])
        across = alike(lower, upper, None)
        blocks.append(
            [first.astype(bf16), second.astype(bf16), across.astype(bf16)]
            + [started(first), started(second)]
        )
    size = 2
    while size < half:
        mask = jnp.where((apart >= size) & (apart < 2 * size), 1.0, 0.0).astype(bf16)
        steps = []
        for first, second, _, x_first, x_second in blocks:
            step = dot(first * mask, x_first).astype(bf16)
            steps.append((step, dot(second * mask[:half, :half], x_second).astype(bf16)))
        for block, (step_first, step_second) in zip(blocks, steps):
            block[3] = block[3] - dot(block[3], step_first).astype(bf16)
            block[4] = block[4] - dot(block[4], step_second).astype(bf16)
        size *= 2
    left = jnp.where(iota((half, head), 1) < half, 1.0, 0.0).astype(bf16)
    blank = jnp.zeros((half, head), bf16)
    steps = [dot(block[0][half:] * left, block[3]).astype(bf16) for block in blocks]
    for block, step in zip(blocks, steps):
        change = dot(block[3][half:], jnp.concatenate([blank, step], axis=0)).astype(bf16)
        block[3] = jnp.concatenate([block[3][:half], block[3][half:] - change], axis=0)
    steps = [dot(block[2], block[3]).astype(bf16) for block in blocks]
    for pair in range(4):
        seq, h = divmod(pair, 2)
        take = slice(seq * span, (seq + 1) * span)
        keys = key_rows[take, h * head : (h + 1) * head]
        values = value_rows[take, h * head : (h + 1) * head]
        col = lambda at: cols_ref[seq, :span, at + h : at + h + 1]
        row = lambda at: rows_ref[seq, at + h : at + h + 1, :span]
        off_first = jnp.where(t == s, 0.0, blocks[pair][3].astype(f32))
        off_second = jnp.where((t == s)[:half, :half], 0.0, blocks[pair][4].astype(f32))
        off_across = -dot(blocks[pair][4], steps[pair])

        def applied(weight, right):
            top = dot(off_first * weight[:, upper], right[upper])
            low = dot(off_across * weight[:, upper], right[upper])
            low = low + dot(off_second * weight[:, lower], right[lower])
            return jnp.concatenate([top, low], axis=0)

        fresh = col(0) * values.astype(f32) + applied(row(0), values)
        carry = (col(0) * col(4) * jnp.exp(col(2))) * keys.astype(f32) + applied(
            row(0) * row(4) * jnp.exp(row(2)), keys
        )
        last = cols_ref[seq, span - 1 : span, 2 + h : 3 + h]
        late = col(4) * jnp.exp(last - col(2))
        reach = dot(carry * late, keys, COLS)
        gain = dot(fresh * late, keys, COLS)
        fresh_ref[pair] = fresh.astype(bf16)
        carry_ref[pair] = carry.astype(bf16)
        give(2, pair)
        give(3, pair)
        factor = row_pack(thirds(jnp.broadcast_to(jnp.exp(last), (1, head))), head)
        for side in range(2):
            to = 2 * pair + side
            send_ref[to, :head, :] = reach.astype(bf16)
            send_ref[to, head : head + half, :] = gain[side * half : (side + 1) * half].astype(bf16)
            send_ref[to, head + half :, :] = factor.astype(bf16)
        give(0, pl.ds(2 * pair, 2))
    for copy in copies:
        copy.wait()


def window_kernel(*refs):
    pieces, refs = refs[:14], refs[14:]
    query_w, gate_w, gain_ref, shared, refs = refs[0], refs[1], refs[2], refs[3:8], refs[8:]
    outputs, refs = refs[:3], refs[3:]
    token_buffer, query_buffer, gate_buffer, sems, more_sems = refs[:5]
    shared_buffers, output_buffers = refs[5:10], refs[10:]
    key_ref, fresh_ref, carry_ref, cols_ref, rows_ref = shared_buffers
    out_ref, reach_ref, silu_ref = output_buffers
    span, depth = token_buffer.shape[2:]
    head = fresh_ref.shape[-1]
    weights = ((query_w, query_buffer), (gate_w, gate_buffer))
    copies = []
    for at, slot in enumerate(SLOTS):
        if at < 2:
            parts = [(pieces[at], token_buffer.at[at])]
        else:
            parts = [(pieces[2 * at - 2 + seq], token_buffer.at[at, seq]) for seq in range(2)]
        for weight, buffer in weights:
            parts.append((weight.at[pl.ds(first_row(slot, depth), depth), :], buffer.at[at]))
        copies.append([pltpu.make_async_copy(a, b, sems.at[at]) for a, b in parts])
        for copy in copies[at]:
            copy.start()
    given = [
        pltpu.make_async_copy(a, b, more_sems.at[at])
        for at, (a, b) in enumerate(zip(shared, shared_buffers))
    ]
    for copy in given:
        copy.start()
    query_total = gate_total = 0.0
    for at in range(8):
        for copy in copies[at]:
            copy.wait()
        rows = token_buffer[at].reshape(-1, depth)
        query_total = query_total + dot(rows, query_buffer[at])
        gate_total = gate_total + dot(rows, gate_buffer[at])
    for copy in given:
        copy.wait()
    query_rows = query_total.astype(bf16)
    gate_rows = gate_total.astype(bf16).astype(f32)
    t = iota((span, span), 0)
    s = iota((span, span), 1)
    taken = []
    for pair in range(4):
        seq, h = divmod(pair, 2)
        take = slice(seq * span, (seq + 1) * span)
        part = slice(h * head, (h + 1) * head)
        col = lambda at: cols_ref[seq, :span, at + h : at + h + 1]
        row = lambda at: rows_ref[seq, at + h : at + h + 1, :span]
        queries = query_rows[take, part]
        unit = rms_scale(queries.astype(f32), unit_floor, False)
        spread = jnp.where(t >= s, col(2) - row(2), 0.0)
        scores = dot(queries, key_ref[take, part], ROWS) * unit * row(4) * jnp.exp(spread)
        scores = jnp.where(t >= s, scores, 0.0).astype(bf16)
        out_ref[pair] = dot(scores, fresh_ref[pair])
        reach = (unit * jnp.exp(col(2))) * queries.astype(f32) - dot(scores, carry_ref[pair])
        reach_ref[pair] = reach.astype(bf16)
        gate = gate_rows[take, part]
        silu_ref[pair] = gain_ref[...] * gate * jax.nn.sigmoid(gate)
        for at, (a, b) in enumerate(zip(output_buffers, outputs)):
            taken.append(pltpu.make_async_copy(a.at[pair], b.at[pair], more_sems.at[5 + at]))
            taken[-1].start()
    for copy in taken:
        copy.wait()


def unpack_factor(block):
    block = block.astype(f32)
    return block[0:1] + block[1:2] + block[2:3]


def load_member(in_ref, at):
    body = in_ref.shape[1] - PACK
    return in_ref[at, :body, :].astype(f32), unpack_factor(in_ref[at, body:, :])


def join(first, second):
    both, factor = first
    later, later_factor = second
    head = later.shape[-1]
    tail = jnp.concatenate([factor * later[:head], later[head:]], axis=0)
    return later_factor * both - dot(both, later[:head]) + tail, factor * later_factor


def total_kernel(in_ref, total_ref):
    parts = [load_member(in_ref, at) for at in range(in_ref.shape[0])]
    while len(parts) > 1:
        parts = [join(parts[at], parts[at + 1]) for at in range(0, len(parts), 2)]
    both, factor = parts[0]
    body, head = both.shape
    total_ref[:body, :] = both.astype(bf16)
    total_ref[body:, :] = row_pack(thirds(factor), head).astype(bf16)


def prefix_kernel(_, in_ref, out_in, reach_in, silu_in, *refs):
    maps_ref, adds_ref, factors_ref, out_ref, reach_ref, silu_ref, sems = refs
    moved = ((out_in, out_ref), (reach_in, reach_ref), (silu_in, silu_ref))
    copies = [pltpu.make_async_copy(a, b, sems.at[at]) for at, (a, b) in enumerate(moved)]
    for copy in copies:
        copy.start()
    count, _, head = in_ref.shape
    member = [load_member(in_ref, at) for at in range(count - 1)]
    c23, c45 = (join(member[at], member[at + 1]) for at in (2, 4))
    upto = [None, member[0], join(member[0], member[1])]
    c456 = join(c45, member[6])
    upto.append(join(upto[2], member[2]))
    upto.append(join(upto[2], c23))
    upto.append(join(upto[4], member[4]))
    upto.append(join(upto[4], c45))
    upto.append(join(upto[4], c456))
    for at in range(1, count):
        both, factor = upto[at]
        maps_ref[at - 1] = both[:head].astype(bf16)
        adds_ref[at - 1] = both[head:]
        factors_ref[at - 1] = jnp.broadcast_to(factor, (8, head))
    for copy in copies:
        copy.wait()


def split_total(ref):
    body = ref.shape[0] - PACK
    return ref[:body, :].astype(f32), unpack_factor(ref[body:, :])


def chosen_total(flag, first, second):
    return tuple(jnp.where(flag, a, b) for a, b in zip(first, second))


def pair_kernel(own_ref, near_ref, pair_ref):
    odd = lax.axis_index("zh") % 2 == 1
    own, near = split_total(own_ref), split_total(near_ref)
    both, factor = join(chosen_total(odd, near, own), chosen_total(odd, own, near))
    body, head = both.shape
    pair_ref[:body, :] = both.astype(bf16)
    pair_ref[body:, :] = row_pack(thirds(factor), head).astype(bf16)


def spread_kernel(
    beta_ref, decay_ref, near_ref, pair_ref, other_ref, maps_ref, adds_ref, factors_ref,
    query_ref, key_ref, value_ref, send_ref, wide_ref, turned_ref,
):
    head = pair_ref.shape[1]
    half = head // 2
    far = lax.axis_index("zh")
    near = lax.axis_index("zl") * 4 + lax.axis_index("x")
    pair = near // 2
    side = near % 2

    def scalar(ref):
        total = jnp.zeros((1, 1), f32)
        for at in range(4):
            entry = ref[at // 2 : at // 2 + 1, at % 2 : at % 2 + 1]
            total = jnp.where(pair == at, entry, total)
        return total

    def chosen(ref):
        total = jnp.zeros((1, head), f32)
        for at in range(4):
            row = ref[at // 2, at % 2 : at % 2 + 1, :].astype(f32)
            total = jnp.where(pair == at, row, total)
        return total

    def after(step, state):
        both, factor = step
        return factor * state - dot(state, both[:head]) + both[head:]

    low = far < 2
    mine, theirs = split_total(pair_ref), split_total(other_ref)
    begin = jnp.where(low, 0.0, theirs[0][head:])
    begin = jnp.where(far % 2 == 1, after(split_total(near_ref), begin), begin)
    first, last = chosen_total(low, mine, theirs), chosen_total(low, theirs, mine)
    state = after(last, first[0][head:])
    final = state.astype(bf16).astype(f32)
    wide_ref[...] = jnp.zeros((head, head), f32)
    wide_ref[pl.ds(pl.multiple_of(side * half, half), half), :] = final
    padded = wide_ref[...]
    turned_ref[...] = padded.T
    mine = turned_ref[pl.ds(pl.multiple_of(far * 32, 32), 32), :]
    query = chosen(query_ref)
    key = chosen(key_ref)
    query = query * rms_scale(query, unit_floor, False)
    key = key * rms_scale(key, unit_floor, False)
    hits = dot(row_pack(thirds(query) + thirds(key), head), padded, ROWS)
    recall = hits[0:1] + hits[1:2] + hits[2:3]
    retrieve = hits[3:4] + hits[4:5] + hits[5:6]
    decay = scalar(decay_ref)
    intersect = jnp.sum(key * query, axis=-1, keepdims=True)
    fresh = chosen(value_ref) - decay * retrieve
    read = decay * recall + (scalar(beta_ref) * intersect) * fresh
    read = jnp.where(iota((1, head), 1) // half == side, read, 0.0)
    zero = jnp.zeros((1, head), f32)
    extra = row_pack((zero, zero, zero, zero) + thirds(read), head)
    pick_row = iota((PACK, 32), 0)
    pick_col = iota((PACK, 32), 1)
    for member in range(8):
        if member:
            at = member - 1
            entry = factors_ref[at, 0:1, :] * begin - dot(begin, maps_ref[at]) + adds_ref[at]
        else:
            entry = begin
        send_ref[member, :half, :] = entry.astype(bf16)
        pick = ((pick_row < 4) & (pick_col == 4 * member + pick_row)).astype(bf16)
        send_ref[member, half:, :] = (dot(pick, mine) + extra).astype(bf16)


def finish_kernel(in_ref, out_ref, reach_ref, silu_ref, gain_ref, mixed_ref, cache_ref, read_ref):
    head = in_ref.shape[-1]
    half = head // 2
    for pair in range(4):
        seq, h = divmod(pair, 2)
        incoming = jnp.concatenate([in_ref[2 * pair, :half, :], in_ref[2 * pair + 1, :half, :]], 0)
        whole = out_ref[pair] + dot(reach_ref[pair], incoming, ROWS)
        mixed = whole * rms_scale(whole, norm_floor, True) * silu_ref[pair]
        mixed_ref[seq, :, h * head : (h + 1) * head] = mixed.astype(bf16)
        extra = in_ref[2 * pair, half:, :].astype(f32) + in_ref[2 * pair + 1, half:, :].astype(f32)
        cache_ref[seq, h] = extra[:4].astype(bf16)
        read = extra[4:5] + extra[5:6] + extra[6:7]
        read = read * rms_scale(read, norm_floor, True) * gain_ref[...]
        read_ref[seq : seq + 1, h * head : (h + 1) * head] = read


def vmem():
    return pl.BlockSpec(memory_space=pltpu.VMEM)


def smem():
    return pl.BlockSpec(memory_space=pltpu.SMEM)


def kernel(body, outputs, kinds, args, scratch=(), limit=16):
    given = {"s": smem, "v": vmem, "p": vmem, "h": lambda: pl.BlockSpec(memory_space=pl.ANY)}
    placed = [
        arg
        if kind == "s"
        else pltpu.with_memory_space_constraint(arg, pltpu.VMEM if kind == "p" else pltpu.HBM)
        for kind, arg in zip(kinds, args, strict=True)
    ]
    plain = lambda out: pltpu.HBM(out.shape, out.dtype)
    return pl.pallas_call(
        body,
        out_shape=tuple(out if kind == "p" else plain(out) for kind, out in outputs),
        in_specs=[given[kind]() for kind in kinds],
        out_specs=tuple(given[kind]() for kind, _ in outputs),
        scratch_shapes=list(scratch),
        compiler_params=pltpu.CompilerParams(vmem_limit_bytes=limit * 1024 * 1024),
    )(*placed)


def shift(value, axis, by):
    length = lax.axis_size(axis)
    return lax.ppermute(value, axis, [(at, (at + by) % length) for at in range(length)])


def shards(
    tokens, query_weight, key_weight, value_weight, gate_weight, beta_weight, decay_weight,
    beta_bias, rate_log, out_gain, new_query, new_key, new_value, new_beta, new_decay,
):
    _, span, depth = tokens.shape
    head = out_gain.shape[0]
    half = head // 2
    wide = span
    width = query_weight.shape[1]
    rows = head + half + PACK
    on, dma = pltpu.VMEM, pltpu.SemaphoreType.DMA
    depth = tokens.shape[2]
    swap = lambda value: shift(value, "c", 1)
    tokens_c = swap(tokens)
    half_span = ("p", on((span, depth), bf16))
    first, second = kernel(split_kernel, [half_span, half_span], "h", (tokens,), (dma((2,)),))
    up0 = shift(first, "y", 1)
    down1 = shift(second, "y", -1)
    sums = [("p", on((2 * span, 2 * width), f32)), ("p", on((2 * span, head), f32))]
    early = kernel(
        early_kernel,
        sums + [("p", on((6 * depth, 2 * width), bf16)), ("p", on((16, 8 * depth), bf16))],
        "ppphhhh",
        (first, second, tokens_c, beta_weight.T, decay_weight.T, key_weight, value_weight),
        (
            on((2 * depth, 2 * width), bf16),
            on((2, 2, 8 * depth), bf16),
            dma((2,)),
        ),
    )
    early = list(early)
    first, second, *early[:2] = lax.optimization_barrier((first, second, *early[:2]))
    up1 = shift(second, "y", 1)
    down0 = shift(first, "y", -1)
    rest = early[2:]
    far0 = shift(up0, "y", 1)
    far1 = shift(down1, "y", -1)
    near = (up0, up1, down0, down1)
    swapped = []
    for value in near:
        swapped.append(swap(value))
    middle = kernel(
        functools.partial(middle_kernel, 2), sums, "p" * 12, (*near, *swapped, *early[:2], *rest)
    )
    far0, far1, *middle = lax.optimization_barrier((far0, far1, *middle))
    last = [far0, far1, swap(far0), swap(far1)]
    middle = kernel(
        functools.partial(middle_kernel, 6), sums, "p" * 6, (far0, far1, *middle, *rest)
    )
    far_c0, far_c1, *middle = lax.optimization_barrier((*last[2:], *middle))
    last[2:] = [far_c0, far_c1]
    local_shapes = [
        on((8, rows, head), bf16),
        on((2 * span, width), bf16),
        on((4, span, head), bf16),
        on((4, span, head), bf16),
        on((2, wide, head), f32),
        on((2, head, wide), f32),
    ]
    send, *shared = kernel(
        local_kernel,
        [("h", out) for out in local_shapes],
        "p" * 8,
        (beta_bias[None], rate_log[None], *last[2:], *middle, *rest),
        (*local_shapes, dma((6,))),
    )
    arrived = lax.all_to_all(send, NEAR, 0, 0, tiled=True)
    gain = out_gain[None]
    finals = [on((4, span, head), f32), on((4, span, head), bf16), on((4, span, head), f32)]
    local_out, reach, silu = kernel(
        window_kernel,
        [("h", out) for out in finals],
        "h" * 16 + "v" + "h" * 5,
        (tokens, tokens_c, *near, *swapped, *last, query_weight, gate_weight, gain, *shared),
        (
            on((8, 2, span, depth), bf16),
            on((8, depth, width), bf16),
            on((8, depth, width), bf16),
            dma((8,)),
            dma((8,)),
            *local_shapes[1:],
            *finals,
        ),
        24,
    )
    arrived, local_out = lax.optimization_barrier((arrived, local_out))
    (total,) = kernel(total_kernel, [("p", on((rows, head), bf16))], "p", (arrived,))
    exchange = lambda value, by: lax.ppermute(value, "zh", [(at, at ^ by) for at in range(4)])
    beside = exchange(total, 1)
    maps, adds, factors, *finals_in = kernel(
        prefix_kernel,
        [
            ("p", on((7, head, head), bf16)),
            ("p", on((7, half, head), f32)),
            ("p", on((7, 8, head), f32)),
            *(("p", out) for out in finals),
        ],
        "pphhh",
        (total, arrived, local_out, reach, silu),
        (dma((3,)),),
    )
    beside, maps = lax.optimization_barrier((beside, maps))
    (pair,) = kernel(pair_kernel, [("p", on((rows, head), bf16))], "pp", (total, beside))
    other = exchange(pair, 3)
    (back,) = kernel(
        spread_kernel,
        [("p", on((8, half + PACK, head), bf16))],
        "p" * 11,
        (
            new_beta, new_decay, beside, pair, other, maps, adds, factors,
            new_query, new_key, new_value,
        ),
        (on((head, head), f32), on((head, head), f32)),
    )
    returned = lax.all_to_all(back, NEAR, 0, 0, tiled=True)
    return kernel(
        finish_kernel,
        [
            ("v", on((2, span, width), bf16)),
            ("v", on((2, 2, 4, head), bf16)),
            ("v", on((2, width), f32)),
        ],
        "ppppp",
        (returned, *finals_in, gain),
    )


def solution(mesh):
    torus = Mesh(mesh.devices.reshape(4, 2, 4, 4, 2), AXES + ("y", "c"))
    sp, tp = AXES, ("y", "c")
    weight = P(None, tp)
    in_specs = (
        P(None, sp, tp),
        weight, weight, weight, weight, weight, weight,
        P(tp), P(tp), P(),
        P(None, tp, None), P(None, tp, None), P(None, tp, None),
        P(None, tp), P(None, tp),
    )
    out_specs = (P(None, sp, tp), P(None, tp, sp, None), P(None, tp))

    return jax.shard_map(
        shards, mesh=torus, in_specs=in_specs, out_specs=out_specs, check_vma=False
    )
```
